32 devices in a mesh: ep: 8 (over z, y), tp: 4 (over x, core).
Axes of the slice: x: 2, y: 2, z: 4, core: 2. Of those that a mesh axis runs over, the one named last changes fastest.
Arguments:
- query_rows: bfloat16 [4096, 1024], P('ep', 'tp'), may hold values from -10 to 10
- key_rows: bfloat16 [4096, 1024], P('ep', 'tp'), may hold values from -10 to 10
- value_rows: bfloat16 [4096, 1024], P('ep', 'tp'), may hold values from -6 to 6
- key_bias: float32 [4096, 16], P(None, 'tp'), may hold values from -30 to 0
- out_weight: bfloat16 [1024, 2048], P('tp'), may hold values from -0.5625 to 0.5625
- moe_input: bfloat16 [4096, 2048], P(('ep', 'tp')), may hold values from -6 to 6
- moe_gain: float32 [2048], replicated, may hold values from 0.1 to 1.9
- expert_pick: int32 [4096, 2], P(('ep', 'tp')), may hold values from 0 to 7, as said below
- route_weight: float32 [4096, 2], P(('ep', 'tp')), may hold values from 0.1 to 1
- w_gate: bfloat16 [8, 2048, 1024], P('ep', None, 'tp'), may hold values from -0.125 to 0.125
- w_up: bfloat16 [8, 2048, 1024], P('ep', None, 'tp'), may hold values from -0.125 to 0.125
- w_down: bfloat16 [8, 1024, 2048], P('ep', 'tp'), may hold values from -0.1875 to 0.1875
Outputs:
- mixer_out: bfloat16 [4096, 2048], P(('ep', 'tp'))
- routed_out: bfloat16 [4096, 2048], P(('ep', 'tp'))
The draws below stay inside these ranges and needn't reach their ends.
Inputs may be any that keep to these rules, and one draw needn't show every extreme that they name: `expert_pick`: each row names two different experts of one group, expert e belonging to group e // 2; the rows of one device name no expert more than 64 times, and in every draw each expert of some group is named exactly 64 times by the rows of every device.
All inputs are finite; a program needn't handle non-finite values.
Results may differ from the reference program's by a relative error of at most 0.013.
Values may be sent and summed in bfloat16 or wider, within the bound.
A program may use at most 128 MiB of HBM per device.

```python
import math
import jax
import jax.numpy as jnp
from jax import lax

D = 2048
ATTENTION_HEADS = 16
HEAD_DIM = 64
FF = 1024
GROUPS = 4
TOPK = 2
SEQ_DEV = 512
TOK2_DEV = 128
EXPERTS = 8
FIRST_TOKENS1 = 4096
SEQ_BLOCKS = 8
TOKENS2 = 4096
CAP = 64
N_TP = 4


def draw_key_bias(key, part):
    flow_lanes = jax.random.split(jax.random.fold_in(key, 101), 5)
    fast_heads = jax.random.uniform(flow_lanes[0], (ATTENTION_HEADS,)) < 0.5
    jitter = jnp.clip(0.5 * jax.random.normal(flow_lanes[2], (FIRST_TOKENS1, ATTENTION_HEADS)), -1.0, 1.0)
    base_level = jnp.where(fast_heads, -jnp.log(4000.0), -jnp.log(130.0 * FIRST_TOKENS1))
    block_count = FIRST_TOKENS1 // SEQ_DEV
    shifts = jax.random.uniform(flow_lanes[1], (block_count, 1, ATTENTION_HEADS), minval=-0.75, maxval=0.75)
    shifts = jnp.broadcast_to(shifts, (block_count, SEQ_DEV, ATTENTION_HEADS)).reshape(FIRST_TOKENS1, ATTENTION_HEADS)
    bias_terms = base_level[None, :] + shifts + jitter
    slot_places = jax.random.randint(flow_lanes[3], (3, ATTENTION_HEADS), 0, FIRST_TOKENS1, dtype=jnp.int32)
    token_positions = jnp.arange(FIRST_TOKENS1, dtype=jnp.int32)[:, None]
    spike_mask = (token_positions == slot_places[0][None, :]) | (token_positions == slot_places[1][None, :]) | (token_positions == slot_places[2][None, :])
    spike_level = jax.random.uniform(flow_lanes[4], (FIRST_TOKENS1, ATTENTION_HEADS), minval=-2.0, maxval=-1.0)
    return jnp.where(spike_mask, spike_level, bias_terms).astype(jnp.float32)


def draw_expert_pick(key, part):
    base_key = jax.random.fold_in(key, 202)
    group_size = EXPERTS // GROUPS
    half_rows = TOK2_DEV // 2
    block_count = TOKENS2 // TOK2_DEV
    favored = jax.random.randint(jax.random.fold_in(base_key, 1), (), 0, GROUPS, dtype=jnp.int32)

    def one_block(block_key):
        flow_lanes = jax.random.split(block_key, 4)
        cut_points = jnp.sort(jax.random.randint(flow_lanes[0], (GROUPS - 2,), 0, half_rows + 1, dtype=jnp.int32))
        bounds = jnp.concatenate([jnp.zeros((1,), jnp.int32), cut_points, jnp.full((1,), half_rows, jnp.int32)])
        others = (favored + 1 + jnp.arange(GROUPS - 1, dtype=jnp.int32)) % GROUPS
        counts = jnp.zeros((GROUPS,), jnp.int32).at[favored].set(half_rows).at[others].set(bounds[1:] - bounds[:-1])
        group_ends = jnp.cumsum(counts)
        starts = group_ends - counts
        token_positions = jnp.arange(TOK2_DEV, dtype=jnp.int32)
        group_id = jnp.sum((token_positions[:, None] >= group_ends[None, :]).astype(jnp.int32), axis=1)
        group_rank = token_positions - starts[group_id]
        rotation = jax.random.randint(flow_lanes[1], (GROUPS,), 0, group_size, dtype=jnp.int32)
        offset = jax.random.randint(flow_lanes[2], (GROUPS,), 1, group_size, dtype=jnp.int32)
        first_pick = (group_rank + rotation[group_id]) % group_size
        second = (group_rank + rotation[group_id] + offset[group_id]) % group_size
        picked = jnp.stack([group_id * group_size + first_pick, group_id * group_size + second], axis=1)
        return picked[jax.random.permutation(flow_lanes[3], TOK2_DEV)]
    blocks = jax.vmap(one_block)(jax.random.split(base_key, block_count))
    return blocks.reshape(TOKENS2, TOPK).astype(jnp.int32)


def shard_levels(own_key, shape, cuts, least, top_value):
    gain = 1.0
    for dim, parts in cuts:
        heights = jax.random.uniform(jax.random.fold_in(jax.random.fold_in(own_key, 6), dim), (parts,), jnp.float32, least / len(cuts), top_value / len(cuts))
        gain = gain * jnp.repeat(jnp.exp(heights), shape[dim] // parts).reshape((-1,) + (1,) * (len(shape) - 1 - dim))
    return gain


def bell_draw(key, extent, spread, bound, shards=(), kind=jnp.bfloat16):
    drawn = jax.random.normal(key, extent, jnp.float32) * spread
    if len(shards) > 0:
        drawn = shard_levels(key, extent, shards, -0.22, 0.18) * drawn
    return jnp.clip(drawn, min=-bound, max=bound).astype(kind)


def setup_inputs(seed: int = 0) -> dict:
    keys = jax.random.split(jax.random.key(seed), 13)
    return {
        "query_rows": bell_draw(keys[0], (FIRST_TOKENS1, ATTENTION_HEADS * HEAD_DIM), 1.7, 10.0, ((0, 8), (1, 4))),
        "key_rows": bell_draw(keys[1], (FIRST_TOKENS1, ATTENTION_HEADS * HEAD_DIM), 1.7, 10.0, ((0, 8), (1, 4))),
        "value_rows": bell_draw(keys[2], (FIRST_TOKENS1, ATTENTION_HEADS * HEAD_DIM), 1.0, 6.0, ((0, 8), (1, 4))),
        "key_bias": draw_key_bias(jax.random.fold_in(keys[12], 71), 0),
        "out_weight": bell_draw(keys[4], (ATTENTION_HEADS * HEAD_DIM, D), (3.0 * (ATTENTION_HEADS * HEAD_DIM) ** -0.5), 0.5625, ((0, 4),)),
        "moe_input": bell_draw(keys[5], (TOKENS2, D), 1.0, 6.0, ((0, 32),)),
        "moe_gain": jnp.clip(1.0 + 0.18 * jax.random.normal(keys[6], (D,), jnp.float32), 0.1, 1.9),
        "expert_pick": draw_expert_pick(jax.random.fold_in(keys[12], 71), 0),
        "route_weight": jnp.clip(jnp.exp(math.log(1.0) - 2.3025851 * jax.random.uniform(keys[8], (TOKENS2, TOPK), jnp.float32) ** shard_levels(keys[8], (TOKENS2, TOPK), ((0, 32),), -0.2, 0.2)), 0.1, 1.0),
        "w_gate": bell_draw(keys[9], (EXPERTS, D, FF), D ** -0.5, 0.125, ((0, 8), (2, 4))),
        "w_up": bell_draw(keys[10], (EXPERTS, D, FF), D ** -0.5, 0.125, ((0, 8), (2, 4))),
        "w_down": bell_draw(keys[11], (EXPERTS, FF, D), FF ** -0.5, 0.1875, ((0, 8), (1, 4))),
    }


def block_values(query_heads, query_first, key_heads, value_heads, bias_heads, key_first, running):
    scores = jnp.einsum('hqd,hkd->hqk', query_heads.astype(jnp.float32), key_heads.astype(jnp.float32))
    scores = scores * HEAD_DIM ** (-0.5) + bias_heads[:, None, :]
    query_pos = query_first + jnp.arange(query_heads.shape[1], dtype=jnp.int32)
    key_pos = key_first + jnp.arange(key_heads.shape[1], dtype=jnp.int32)
    causal = (key_pos[None, :] < query_pos[:, None])[None]
    failure = jnp.where(causal, jax.nn.log_sigmoid(-scores), 0.0)
    remainder = lax.cumsum(failure, axis=2, reverse=True) - failure + running[:, :, None]
    stick_weight = jnp.where(causal, jnp.exp(jax.nn.log_sigmoid(scores) + remainder), 0.0).astype(jnp.bfloat16)
    portion = jnp.einsum('hqk,hkd->hqd', stick_weight.astype(jnp.float32), value_heads.astype(jnp.float32))
    return (portion, running + lax.optimization_barrier(jnp.sum(failure, axis=2)))

def mixer(query_rows, key_rows, value_rows, key_bias, out_weight):
    block_count = FIRST_TOKENS1 // SEQ_DEV

    def split_heads(rows):
        return jnp.transpose(rows.reshape(block_count, SEQ_DEV, ATTENTION_HEADS, HEAD_DIM), (0, 2, 1, 3))
    query_heads = split_heads(query_rows)
    key_heads = split_heads(key_rows)
    value_heads = split_heads(value_rows)
    bias_heads = jnp.transpose(key_bias.reshape(block_count, SEQ_DEV, ATTENTION_HEADS), (0, 2, 1))

    def one_block(block_index):

        def visit(step_index, carried):
            source = block_index - step_index
            portion, running = block_values(query_heads[block_index], block_index * SEQ_DEV, key_heads[source], value_heads[source], bias_heads[source], source * SEQ_DEV, carried[1])
            return (carried[0] + portion, running)
        start_state = (jnp.zeros((ATTENTION_HEADS, SEQ_DEV, HEAD_DIM), jnp.float32), jnp.zeros((ATTENTION_HEADS, SEQ_DEV), jnp.float32))
        steps_here = block_index % SEQ_BLOCKS + 1
        return lax.fori_loop(0, steps_here, visit, start_state)[0].astype(jnp.bfloat16)
    attended = lax.map(one_block, jnp.arange(block_count, dtype=jnp.int32))
    attended = jnp.transpose(attended, (0, 2, 1, 3)).reshape(FIRST_TOKENS1, ATTENTION_HEADS * HEAD_DIM)
    group_width = ATTENTION_HEADS * HEAD_DIM // N_TP
    summed = jnp.zeros((FIRST_TOKENS1, D), jnp.float32)
    for group in range(N_TP):
        columns = attended[:, group * group_width:(group + 1) * group_width]
        weights = out_weight[group * group_width:(group + 1) * group_width]
        rounded = jnp.dot(columns, weights, preferred_element_type=jnp.float32).astype(jnp.bfloat16)
        summed = summed + lax.optimization_barrier(rounded).astype(jnp.float32)
    return summed.astype(jnp.bfloat16)

def experts(moe_input, moe_gain, expert_pick, route_weight, w_gate, w_up, w_down):
    widened = moe_input.astype(jnp.float32)
    normed = (widened * lax.rsqrt(lax.optimization_barrier(jnp.mean(widened * widened, axis=1, keepdims=True)) + 1e-06) * moe_gain).astype(jnp.bfloat16)
    block_count = TOKENS2 // TOK2_DEV
    picks = expert_pick.reshape(block_count, TOK2_DEV * TOPK)
    matches = (picks[:, :, None] == jnp.arange(EXPERTS, dtype=jnp.int32)[None, None, :]).astype(jnp.int32)
    ranks = lax.optimization_barrier(jnp.sum((jnp.cumsum(matches, axis=1) - matches) * matches, axis=2))
    block_ids = jnp.arange(block_count, dtype=jnp.int32)[:, None]
    slots = picks * (block_count * CAP) + block_ids * CAP + ranks
    owners = block_ids * TOK2_DEV + jnp.arange(TOK2_DEV * TOPK, dtype=jnp.int32)[None, :] // TOPK
    table = jnp.full((EXPERTS * block_count * CAP,), TOKENS2, jnp.int32)
    table = table.at[slots.reshape(-1)].set(owners.reshape(-1)).reshape(EXPERTS, block_count * CAP)
    padded = jnp.concatenate([normed, jnp.zeros((1, D), jnp.bfloat16)], axis=0)

    def serve(expert):
        rows = padded[table[expert]]
        gate_in = jnp.dot(rows, w_gate[expert], preferred_element_type=jnp.float32)
        up_in = jnp.dot(rows, w_up[expert], preferred_element_type=jnp.float32)
        hidden = (jax.nn.silu(gate_in) * up_in).astype(jnp.bfloat16)
        return jnp.dot(hidden, w_down[expert], preferred_element_type=jnp.float32).astype(jnp.bfloat16)
    served = lax.map(serve, jnp.arange(EXPERTS, dtype=jnp.int32))
    chosen = served.reshape(EXPERTS * block_count * CAP, D)[slots.reshape(-1)]
    chosen = chosen.reshape(TOKENS2, TOPK, D).astype(jnp.float32)
    return lax.optimization_barrier(jnp.sum(chosen * route_weight[:, :, None], axis=1)).astype(jnp.bfloat16)

def reference(query_rows, key_rows, value_rows, key_bias, out_weight, moe_input, moe_gain, expert_pick, route_weight, w_gate, w_up, w_down):
    return (mixer(query_rows, key_rows, value_rows, key_bias, out_weight), experts(moe_input, moe_gain, expert_pick, route_weight, w_gate, w_up, w_down))
```

```python
import jax
import jax.numpy as jnp
from jax import lax
from jax.experimental import pallas as pl
from jax.experimental.pallas import tpu as pltpu
from jax.sharding import PartitionSpec as P

HEAD_DIM = 64
GROUPS = 4
TOPK = 2
PAIR = 2


norm_eps = 1e-06


def attend_kernel(tops_ref, query_ref, bias_ref, *rest):
    block_refs = rest[:-4]
    out_ref, acc_ref, kv_ref, sems = rest[-4:]

    @pl.when(pl.program_id(0) == 0)
    def _():
        copies = [
            pltpu.make_async_copy(ref, kv_ref.at[slot], sems.at[slot])
            for slot, ref in enumerate(block_refs)
        ]
        for copy in copies:
            copy.start()
        for copy in copies:
            copy.wait()

    tile = query_ref.shape[1]
    width = query_ref.shape[2]
    heads = width // HEAD_DIM
    slots = kv_ref.shape[0]
    per_block = kv_ref.shape[1] // tile
    top = tops_ref[pl.program_id(0)]
    own = tops_ref[2]
    turned = jnp.transpose(query_ref[0].astype(jnp.float32) * HEAD_DIM ** (-0.5))
    row_head = lax.broadcasted_iota(jnp.int32, (width, tile), 0) // HEAD_DIM
    queries = [jnp.where(row_head == h, turned, 0.0).astype(jnp.bfloat16) for h in range(heads)]
    key_at = lax.broadcasted_iota(jnp.int32, (tile, tile), 0)
    query_at = lax.broadcasted_iota(jnp.int32, (tile, tile), 1)
    causal = key_at < query_at
    later = jnp.where(causal, 1.0, 0.0).astype(jnp.bfloat16)
    acc_ref[...] = jnp.zeros_like(acc_ref)

    def visit(index, running, masked):
        block = index // per_block
        away = lax.rem(own // PAIR - block // PAIR + slots // PAIR, slots // PAIR)
        slot = away * PAIR + lax.rem(own + block, PAIR)
        rows = pl.ds(pl.multiple_of((index - block * per_block) * tile, tile), tile)
        first = pl.multiple_of(index * tile, tile)
        keys = kv_ref[slot, rows, :width]
        values = jnp.transpose(kv_ref[slot, rows, width:])
        passed = []
        for h in range(heads):
            scores = jnp.dot(keys, queries[h], preferred_element_type=jnp.float32)
            scores = scores + bias_ref[pl.ds(first, tile), h : h + 1]
            tail = jnp.log(1.0 + jnp.exp(-jnp.abs(scores)))
            lost = jnp.maximum(scores, 0.0) + tail
            won = jnp.minimum(scores, 0.0) - tail
            if masked:
                lost = jnp.where(causal, lost, 0.0)
            lost = lost.astype(jnp.bfloat16)
            after = jnp.dot(later, lost, preferred_element_type=jnp.float32)
            weight = jnp.exp(won - (after + running[h]))
            if masked:
                weight = jnp.where(causal, weight, 0.0)
            span = slice(h * HEAD_DIM, (h + 1) * HEAD_DIM)
            acc_ref[span, :] += jnp.dot(
                values[span, :], weight.astype(jnp.bfloat16), preferred_element_type=jnp.float32
            )
            passed.append(running[h] + after[0:1, :] + lost[0:1, :].astype(jnp.float32))
        return tuple(passed)

    running = tuple(jnp.zeros((1, tile), jnp.float32) for _ in range(heads))
    running = visit(top, running, True)
    lax.fori_loop(0, top, lambda step, carried: visit(top - 1 - step, carried, False), running)
    out_ref[0] = jnp.transpose(acc_ref[...]).astype(jnp.bfloat16)


def attend(tops, queries, blocks, bias):
    parts, tile, width = queries.shape
    held = (len(blocks),) + blocks[0].shape
    pairs = parts * tile * held[0] * held[1] * width // HEAD_DIM // 2
    return pl.pallas_call(
        attend_kernel,
        out_shape=jax.ShapeDtypeStruct(queries.shape, jnp.bfloat16),
        grid_spec=pltpu.PrefetchScalarGridSpec(
            num_scalar_prefetch=1,
            grid=(parts,),
            in_specs=[
                pl.BlockSpec((1, tile, width), lambda c, tops: (c, 0, 0)),
                pl.BlockSpec(memory_space=pltpu.VMEM),
            ]
            + [pl.BlockSpec(memory_space=pl.ANY)] * len(blocks),
            out_specs=pl.BlockSpec((1, tile, width), lambda c, tops: (c, 0, 0)),
            scratch_shapes=[
                pltpu.VMEM((width, tile), jnp.float32),
                pltpu.VMEM(held, blocks[0].dtype),
                pltpu.SemaphoreType.DMA((len(blocks),)),
            ],
        ),
        cost_estimate=pl.CostEstimate(
            flops=pairs * 1000, bytes_accessed=len(blocks) * blocks[0].size * 2, transcendentals=pairs * 3
        ),
        compiler_params=pltpu.CompilerParams(vmem_limit_bytes=58 * 1024 * 1024),
    )(tops, queries, bias, *blocks)


def gather_blocks(own, count):
    ring = count // PAIR
    swap = [(i, i // PAIR * PAIR + (i + 1) % PAIR) for i in range(count)]
    ahead = [(i, (i + PAIR) % count) for i in range(count)]
    behind = [(j, i) for i, j in ahead]
    near = [own, lax.ppermute(own, "ep", swap)]
    far = {}
    for member in range(PAIR):
        reach = (ring - 1 + (member == 0)) // 2
        held = near[member]
        for step in range(1, reach + 1):
            held = lax.ppermute(held, "ep", ahead)
            far[step, member] = held
        held = near[member]
        for step in range(ring - 1, reach, -1):
            held = lax.ppermute(held, "ep", behind)
            far[step, member] = held
    return near + [far[step, member] for step in range(1, ring) for member in range(PAIR)]


def expand(arrived, gate_weights, up_weights):
    gate_in = jnp.einsum(
        "necm,emf->necf", arrived, gate_weights, preferred_element_type=jnp.float32
    )
    up_in = jnp.einsum("necm,emf->necf", arrived, up_weights, preferred_element_type=jnp.float32)
    return (jax.nn.silu(gate_in) * up_in).astype(jnp.bfloat16)


def contract(hidden, down_weights):
    return jnp.einsum("necf,efm->necm", hidden, down_weights, preferred_element_type=jnp.float32)


def local(
    query_rows,
    key_rows,
    value_rows,
    key_bias,
    out_weight,
    moe_input,
    moe_gain,
    expert_pick,
    route_weight,
    w_gate,
    w_up,
    w_down,
):
    block_rows = query_rows.shape[0]
    half_rows = block_rows // 2
    ep_index = lax.axis_index("ep")
    ep_count = lax.axis_size("ep")
    own_kv = jnp.concatenate([key_rows, value_rows], axis=1)
    mirror = [(i, ep_count - 1 - i) for i in range(ep_count)]
    far_query = lax.ppermute(query_rows[half_rows:], "ep", mirror)
    blocks = gather_blocks(own_kv, ep_count)
    tops = jnp.stack(
        [2 * ep_index, 2 * (ep_count - 1 - ep_index) + 1, ep_index]
    ).astype(jnp.int32)
    near, far = attend(
        tops, jnp.stack([query_rows[:half_rows], far_query]), blocks, key_bias
    )
    attended = jnp.concatenate([near, lax.ppermute(far, "ep", mirror)], axis=0)
    mixer_out = lax.psum_scatter(
        jnp.dot(attended, out_weight, preferred_element_type=jnp.float32).astype(jnp.bfloat16),
        "tp",
        scatter_dimension=0,
        tiled=True,
    )
    token_count = moe_input.shape[0]
    widened = moe_input.astype(jnp.float32)
    normed = (
        widened
        * lax.rsqrt(jnp.mean(widened * widened, axis=1, keepdims=True) + norm_eps)
        * moe_gain
    ).astype(jnp.bfloat16)
    local_experts = w_gate.shape[0]
    expert_total = local_experts * ep_count
    capacity = GROUPS * token_count // expert_total
    picks = expert_pick.reshape(-1)
    matches = (picks[:, None] == jnp.arange(expert_total, dtype=jnp.int32)[None, :]).astype(
        jnp.int32
    )
    ranks = jnp.sum((jnp.cumsum(matches, axis=0) - matches) * matches, axis=1)
    slots = picks * capacity + ranks
    owners = jnp.arange(picks.shape[0], dtype=jnp.int32) // TOPK
    table = jnp.full((expert_total * capacity,), token_count, jnp.int32).at[slots].set(owners)
    padded = jnp.concatenate([normed, jnp.zeros((1, normed.shape[1]), jnp.bfloat16)], axis=0)
    outgoing = padded[table].reshape(ep_count, local_experts, capacity, normed.shape[1])
    outgoing = lax.optimization_barrier((outgoing, far_query, *blocks))[0]
    arrived = lax.all_to_all(outgoing, "ep", split_axis=0, concat_axis=0, tiled=True)
    gate_all, up_all, down_all = (
        lax.all_gather(w_gate, "tp", axis=2, tiled=True),
        lax.all_gather(w_up, "tp", axis=2, tiled=True),
        lax.all_gather(w_down, "tp", axis=1, tiled=True),
    )
    served = contract(expand(arrived, gate_all, up_all), down_all).astype(jnp.bfloat16)
    returned = lax.all_to_all(served, "ep", split_axis=0, concat_axis=0, tiled=True)
    flat = returned.reshape(expert_total * capacity, returned.shape[3])
    chosen = flat[slots].reshape(token_count, TOPK, flat.shape[1]).astype(jnp.float32)
    routed_out = jnp.sum(chosen * route_weight[:, :, None], axis=1).astype(jnp.bfloat16)
    return (mixer_out, routed_out)


MESH = pl.DeviceIdType.MESH
CHUNKS = 4


def remote(src, dst, send, recv, device):
    return pltpu.make_async_remote_copy(
        src_ref=src,
        dst_ref=dst,
        send_sem=send,
        recv_sem=recv,
        device_id=device,
        device_id_type=MESH,
    )


def split_parts(values):
    high = values.astype(jnp.bfloat16).astype(jnp.float32)
    rest = values - high
    middle = rest.astype(jnp.bfloat16).astype(jnp.float32)
    return high, middle, rest - middle


def fused_kernel(
    q_ref,
    k_ref,
    v_ref,
    bias_ref,
    out_weight_ref,
    moe_ref,
    gain_ref,
    pick_ref,
    route_ref,
    gate_ref,
    up_ref,
    down_ref,
    mixer_ref,
    routed_ref,
    q_send,
    q_recv,
    kv_send,
    kv_recv,
    keys,
    acc,
    att_send,
    att_recv,
    project,
    mix_send,
    mix_recv,
    rows_send,
    rows_recv,
    placed,
    gate_all,
    up_all,
    down_all,
    hidden,
    part_send,
    part_recv,
    part_own,
    back_send,
    back_recv,
    local_sem,
    over_send,
    over_recv,
    die_send,
    die_recv,
    pass_send,
    pass_recv,
    project_send,
    project_recv,
    q_out,
    q_in,
    kv_out,
    kv_pass,
    kv_in,
    rows_out,
    rows_pass,
    rows_in,
    att_out,
    att_in,
    mix_out,
    mix_in,
    part_out,
    part_in,
    back_out,
    back_in,
):
    ep_count = q_recv.shape[0]
    lines = ep_count // PAIR
    e, t = lax.axis_index("ep"), lax.axis_index("tp")
    z, y = lax.div(e, PAIR), lax.rem(e, PAIR)
    chip, core = lax.div(t, PAIR), lax.rem(t, PAIR)
    die = PAIR * chip + 1 - core
    over = PAIR * (1 - chip) + core
    across = PAIR * (1 - chip) + 1 - core
    side = PAIR * z + 1 - y
    block_rows, width = q_ref.shape
    half = block_rows // PAIR
    quarter = half // PAIR
    tokens, model = moe_ref.shape
    slots = rows_send.shape[1]
    shard = gate_ref.shape[2]
    span = model // CHUNKS

    barrier = pltpu.get_barrier_semaphore()
    for step in range(1, ep_count):
        for other in range(PAIR):
            pl.semaphore_signal(
                barrier,
                inc=1,
                device_id=(lax.rem(e + step, ep_count), PAIR * chip + other),
                device_id_type=MESH,
            )
    for other in (die, over):
        pl.semaphore_signal(barrier, inc=1, device_id=(e, other), device_id_type=MESH)

    pieces = []
    own_rows = pl.ds(pl.multiple_of(t * shard, shard), shard)
    pieces.append((gate_ref.at[0], gate_all.at[t]))
    pieces.append((up_ref.at[0], up_all.at[t]))
    for chunk in range(CHUNKS):
        pieces.append(
            (
                down_ref.at[0, :, chunk * span : (chunk + 1) * span],
                down_all.at[chunk, own_rows, :],
            )
        )

    def held(index, owner):
        if index == 0:
            return gate_all.at[owner]
        if index == 1:
            return up_all.at[owner]
        rows = pl.ds(pl.multiple_of(owner * shard, shard), shard)
        return down_all.at[index - 2, rows, :]

    project_rows = pl.ds(pl.multiple_of(core * width, width), width)
    die_rows = pl.ds(pl.multiple_of((1 - core) * width, width), width)
    locals_ = [
        pltpu.make_async_copy(src, dst, local_sem.at[i]) for i, (src, dst) in enumerate(pieces)
    ]
    locals_.append(
        pltpu.make_async_copy(out_weight_ref, project.at[project_rows, :], local_sem.at[len(pieces)])
    )
    for copy in locals_:
        copy.start()

    keys_turned = jnp.transpose(k_ref[...].astype(jnp.float32)).astype(jnp.bfloat16)
    values_turned = jnp.transpose(v_ref[...].astype(jnp.float32)).astype(jnp.bfloat16)
    for h in range(lines):
        span_h = slice(h * HEAD_DIM, (h + 1) * HEAD_DIM)
        kv_send[h, :HEAD_DIM, :] = keys_turned[span_h, :]
        kv_send[h, HEAD_DIM:, :] = values_turned[span_h, :]
    pl.semaphore_wait(barrier, PAIR * (ep_count - 1) + 2)

    pending = []
    for i, (src, dst) in enumerate(pieces):
        copy = remote(src, dst, over_send.at[i], over_recv.at[i], (e, over))
        copy.start()
        pending.append(copy)
    for step in range(1, lines):
        there = lax.rem(z + step, lines)
        copy = remote(
            kv_send.at[there], kv_recv.at[e], kv_out.at[step], kv_in.at[e], (PAIR * there + y, t)
        )
        copy.start()
        pending.append(copy)
    copy = remote(kv_send.at[z], kv_recv.at[e], kv_pass.at[z], kv_in.at[e], (side, t))
    copy.start()
    pending.append(copy)
    kv_recv[e] = kv_send[z]

    q_turned = jnp.transpose(q_ref[...].astype(jnp.float32) * HEAD_DIM ** (-0.5))
    for h in range(lines):
        q_send[h] = q_turned[h * HEAD_DIM : (h + 1) * HEAD_DIM, :].astype(jnp.bfloat16)
    ones_at = lax.broadcasted_iota(jnp.int32, (HEAD_DIM, half), 0) < 3
    ones_rows = jnp.where(ones_at, 1.0, 0.0).astype(jnp.bfloat16)
    for i in range(ep_count):
        q_recv[i, HEAD_DIM:, :] = ones_rows
    for step in range(1, ep_count):
        there = lax.rem(e + step, ep_count)
        head, column = lax.div(there, PAIR), lax.rem(there, PAIR)
        lanes = pl.ds(pl.multiple_of(lax.rem(column + e, PAIR) * half, half), half)
        copy = remote(
            q_send.at[head, :, lanes],
            q_recv.at[e, :HEAD_DIM, :],
            q_out.at[step],
            q_in.at[e],
            (there, t),
        )
        copy.start()
        pending.append(copy)
    own_lanes = pl.ds(pl.multiple_of(lax.rem(y + e, PAIR) * half, half), half)
    q_recv[e, :HEAD_DIM, :] = q_send[z, :, own_lanes]

    for i, (src, dst) in enumerate(pieces):
        copy = remote(src, dst, die_send.at[i], die_recv.at[i], (e, die))
        copy.start()
        pending.append(copy)
    copy = remote(
        out_weight_ref, project.at[project_rows, :], project_send, project_recv, (e, die)
    )
    copy.start()
    pending.append(copy)

    widened = moe_ref[...].astype(jnp.float32)
    normed = (
        widened
        * lax.rsqrt(jnp.mean(widened * widened, axis=1, keepdims=True) + norm_eps)
        * gain_ref[...]
    ).astype(jnp.bfloat16)
    group_row = lax.shift_right_logical(pick_ref[0:1, :], 1)
    groups = lines
    group_at = lax.broadcasted_iota(jnp.int32, (8, tokens), 0)
    chosen = (group_at == group_row).astype(jnp.float32)
    earlier = (
        lax.broadcasted_iota(jnp.int32, (tokens, tokens), 0)
        < lax.broadcasted_iota(jnp.int32, (tokens, tokens), 1)
    ).astype(jnp.float32)
    ranks = jnp.dot(
        chosen.astype(jnp.bfloat16),
        earlier.astype(jnp.bfloat16),
        preferred_element_type=jnp.float32,
    )
    slot_row = jnp.sum(
        chosen * (ranks + group_at.astype(jnp.float32) * slots), axis=0, keepdims=True
    )
    slot_at = lax.broadcasted_iota(jnp.int32, (groups * slots, tokens), 0)
    picked = (slot_at == slot_row.astype(jnp.int32)).astype(jnp.float32)
    placed[...] = jnp.transpose(picked).astype(jnp.bfloat16)
    first_low = (pick_ref[0:1, :] & 1) == 0
    low_row = jnp.where(first_low, route_ref[0:1, :], route_ref[1:2, :])
    high_row = jnp.where(first_low, route_ref[1:2, :], route_ref[0:1, :])
    low = split_parts(jnp.sum(picked * low_row, axis=1, keepdims=True))
    high = split_parts(jnp.sum(picked * high_row, axis=1, keepdims=True))
    lane = lax.broadcasted_iota(jnp.int32, (groups * slots, 128), 1)
    shares = jnp.zeros((groups * slots, 128), jnp.float32)
    for i, part in enumerate(low + high):
        shares = jnp.where(lane == i, part, shares)
    rows_send[:, :, model:] = shares.astype(jnp.bfloat16).reshape(groups, slots, 128)
    picked = picked.astype(jnp.bfloat16)
    for first in range(0, model, span):
        rows_send[:, :, first : first + span] = (
            jnp.dot(picked, normed[:, first : first + span], preferred_element_type=jnp.float32)
            .astype(jnp.bfloat16)
            .reshape(groups, slots, span)
        )
    home = y * lines + z
    for step in range(1, lines):
        there = lax.rem(z + step, lines)
        copy = remote(
            rows_send.at[there],
            rows_recv.at[home],
            rows_out.at[step],
            rows_in.at[home],
            (PAIR * there + y, t),
        )
        copy.start()
        pending.append(copy)

    def pass_kv(step):
        source = PAIR * lax.rem(z + step, lines) + y
        arrived = kv_recv.at[source]
        remote(arrived, arrived, kv_out.at[0], kv_in.at[source], (side, t)).wait_recv()
        copy = remote(
            arrived, arrived, kv_pass.at[lax.div(source, PAIR)], kv_in.at[source], (side, t)
        )
        copy.start()
        pending.append(copy)

    for step in (1, 3, 2) if lines == 4 else range(1, lines):
        pass_kv(step)
    copy = remote(rows_send.at[z], rows_recv.at[home], rows_pass.at[z], rows_in.at[home], (side, t))
    copy.start()
    pending.append(copy)
    rows_recv[home] = rows_send[z]

    for i in range(lines):
        source = PAIR * i + 1 - y
        arrived = kv_recv.at[source]
        remote(arrived, arrived, kv_out.at[0], kv_in.at[source], (side, t)).wait_recv()
    for step in range(1, ep_count):
        source = lax.rem(e + step, ep_count)
        arrived = q_recv.at[source, :HEAD_DIM, :]
        remote(arrived, arrived, q_out.at[0], q_in.at[source], (side, t)).wait_recv()

    head_at = lax.broadcasted_iota(jnp.int32, (lines, block_rows), 0)
    aug_at = lax.broadcasted_iota(jnp.int32, (HEAD_DIM, block_rows), 0)

    def turn_keys(i, _):
        rows = pl.ds(pl.multiple_of(i * block_rows, block_rows), block_rows)
        bias = jnp.sum(
            jnp.where(head_at == z, bias_ref[:, rows], 0.0), axis=0, keepdims=True
        )
        extra = jnp.zeros((HEAD_DIM, block_rows), jnp.float32)
        for place, part in enumerate(split_parts(bias)):
            extra = jnp.where(aug_at == place, part, extra)
        stacked = jnp.concatenate([kv_recv[i, :HEAD_DIM, :].astype(jnp.float32), extra], axis=0)
        keys[rows, :] = jnp.transpose(stacked).astype(jnp.bfloat16)
        return 0

    lax.fori_loop(0, ep_count, turn_keys, 0)

    key_at = lax.broadcasted_iota(jnp.int32, (half, half), 0)
    query_at = lax.broadcasted_iota(jnp.int32, (half, half), 1)
    later = jnp.where(key_at < query_at, 1.0, 0.0).astype(jnp.bfloat16)

    def visit(block, queries, running, place):
        for sub in range(PAIR - 1, -1, -1):
            rows = pl.ds(pl.multiple_of(block * block_rows + sub * half, half), half)
            scores = jnp.dot(keys[rows, :], queries, preferred_element_type=jnp.float32)
            lost = jnp.maximum(scores, jnp.log(1.0 + jnp.exp(jnp.minimum(scores, 80.0))))
            won = scores - lost
            if place is not None:
                causal = key_at - query_at < (place - sub) * half
                lost = jnp.where(causal, lost, 0.0)
            lost = lost.astype(jnp.bfloat16)
            after = jnp.dot(later, lost, preferred_element_type=jnp.float32)
            weight = jnp.exp(won - (after + running))
            if place is not None:
                weight = jnp.where(causal, weight, 0.0)
            values = kv_recv[block, HEAD_DIM:, sub * half : (sub + 1) * half]
            acc[...] += jnp.dot(
                values, weight.astype(jnp.bfloat16), preferred_element_type=jnp.float32
            )
            running = running + after[0:1, :] + lost[0:1, :].astype(jnp.float32)
        return running

    def send_attended(i, other):
        place = lax.rem(y + i, PAIR)
        return remote(
            att_send.at[i, :, other * quarter : (other + 1) * quarter],
            att_recv.at[
                pl.ds(pl.multiple_of(core * width + z * HEAD_DIM, HEAD_DIM), HEAD_DIM),
                pl.ds(pl.multiple_of(place * quarter, quarter), quarter),
            ],
            att_out.at[i, other],
            att_in.at[core, e],
            (i, PAIR * chip + other),
        )

    def wait_rows(place):
        arrived = rows_recv.at[place]
        remote(arrived, arrived, rows_out.at[0], rows_in.at[place], (side, t)).wait_recv()

    def pass_rows(step):
        there = lax.rem(z + step, lines)
        place = y * lines + there
        wait_rows(place)
        arrived = rows_recv.at[place]
        return remote(arrived, arrived, rows_pass.at[there], rows_in.at[place], (side, t))

    def one_tile(i, _):
        place = lax.rem(y + i, PAIR)
        queries = q_recv[i]
        acc[...] = jnp.zeros_like(acc)
        running = visit(i, queries, jnp.zeros((1, half), jnp.float32), place)
        lax.fori_loop(0, i, lambda s, r: visit(i - 1 - s, queries, r, None), running)
        att_send[i] = acc[...].astype(jnp.bfloat16)
        for other in range(PAIR):
            here = jnp.logical_and(i == e, core == other)

            @pl.when(jnp.logical_not(here))
            def _():
                send_attended(i, other).start()

            @pl.when(here)
            def _():
                att_recv[
                    pl.ds(pl.multiple_of(core * width + z * HEAD_DIM, HEAD_DIM), HEAD_DIM),
                    pl.ds(pl.multiple_of(place * quarter, quarter), quarter),
                ] = att_send[i, :, other * quarter : (other + 1) * quarter]

        return 0

    lax.fori_loop(0, ep_count, one_tile, 0)

    for step in (1, 3, 2) if lines == 4 else range(1, lines):
        copy = pass_rows(step)
        copy.start()
        pending.append(copy)

    def pass_on(index):
        arrived = held(index, over)
        remote(arrived, arrived, over_send.at[index], over_recv.at[index], (e, over)).wait_recv()
        copy = remote(arrived, arrived, pass_send.at[index], pass_recv.at[index], (e, die))
        copy.start()
        pending.append(copy)

    def wait_die(index):
        arrived = held(index, die)
        remote(arrived, arrived, die_send.at[index], die_recv.at[index], (e, die)).wait_recv()

    def wait_across(index):
        arrived = held(index, across)
        remote(arrived, arrived, pass_send.at[index], pass_recv.at[index], (e, die)).wait_recv()

    def serve(owner):
        columns = pl.ds(pl.multiple_of(owner * shard, shard), shard)

        def part(m, _):
            rows = rows_recv[pl.ds(m * lines, lines), :, :model].reshape(lines * slots, model)
            gate_in = jnp.dot(rows, gate_all[owner], preferred_element_type=jnp.float32)
            up_in = jnp.dot(rows, up_all[owner], preferred_element_type=jnp.float32)
            target = pl.ds(pl.multiple_of(m * lines * slots, lines * slots), lines * slots)
            hidden[target, columns] = (gate_in / (1.0 + jnp.exp(-gate_in)) * up_in).astype(
                jnp.bfloat16
            )
            return 0

        lax.fori_loop(0, PAIR, part, 0)

    pass_on(0)
    for copy in locals_:
        copy.wait()
    for i in range(lines):
        wait_rows((1 - y) * lines + i)
    wait_die(0)
    wait_die(1)
    serve(t)
    serve(die)

    for source_core in range(PAIR):
        for i in range(ep_count):

            @pl.when(jnp.logical_not(jnp.logical_and(core == source_core, e == i)))
            def _():
                first = source_core * width + i // PAIR * HEAD_DIM
                place = lax.rem(i % PAIR + e, PAIR)
                lanes = pl.ds(pl.multiple_of(place * quarter, quarter), quarter)
                arrived = att_recv.at[first : first + HEAD_DIM, lanes]
                remote(
                    arrived, arrived, att_out.at[0, 0], att_in.at[source_core, i], (side, t)
                ).wait_recv()

    arrived = project.at[die_rows, :]
    remote(arrived, arrived, project_send, project_recv, (e, die)).wait_recv()

    def mixed(which):
        lanes = pl.ds(pl.multiple_of(which * quarter, quarter), quarter)
        attended = jnp.transpose(att_recv[:, lanes].astype(jnp.float32)).astype(jnp.bfloat16)
        return jnp.dot(attended, project[...], preferred_element_type=jnp.float32).astype(
            jnp.bfloat16
        )

    mix_send[...] = mixed(1 - chip)
    copy = remote(mix_send, mix_recv, mix_out, mix_in, (e, over))
    copy.start()
    pending.append(copy)
    mixer_ref[...] = mixed(chip)

    pass_on(1)
    serve(over)
    wait_across(0)
    wait_across(1)
    serve(across)

    share_lane = lax.broadcasted_iota(jnp.int32, (lines * slots, 128), 1)
    share_here = jnp.logical_and(share_lane >= 3 * y, share_lane < 3 * y + 3)

    def contract(chunk, which):
        rows = pl.ds(pl.multiple_of(which * lines * slots, lines * slots), lines * slots)
        shares = rows_recv[pl.ds(which * lines, lines), :, model:].reshape(lines * slots, 128)
        share = jnp.sum(
            jnp.where(share_here, shares.astype(jnp.float32), 0.0), axis=1, keepdims=True
        )
        return (
            jnp.dot(hidden[rows, :], down_all[chunk], preferred_element_type=jnp.float32) * share
        )

    def give_back(chunk):
        arrived = part_recv.at[chunk]
        remote(arrived, arrived, part_out.at[chunk], part_in.at[chunk], (side, t)).wait_recv()
        total = part_own[chunk] + part_recv[chunk].astype(jnp.float32)
        back_send[chunk] = total.astype(jnp.bfloat16).reshape(lines, slots, span)
        for step in range(1, lines):
            there = lax.rem(z + step, lines)
            copy = remote(
                back_send.at[chunk, there],
                back_recv.at[chunk, z],
                back_out.at[chunk, step],
                back_in.at[chunk, z],
                (PAIR * there + y, t),
            )
            copy.start()
            pending.append(copy)
        back_recv[chunk, z] = back_send[chunk, z]

    for chunk in range(CHUNKS):
        pass_on(2 + chunk)
        if chunk > 0:
            give_back(chunk - 1)
        wait_die(2 + chunk)
        wait_across(2 + chunk)
        part_send[chunk] = contract(chunk, 1 - y).astype(jnp.bfloat16)
        copy = remote(
            part_send.at[chunk],
            part_recv.at[chunk],
            part_out.at[chunk],
            part_in.at[chunk],
            (side, t),
        )
        copy.start()
        pending.append(copy)
        part_own[chunk] = contract(chunk, y)
    give_back(CHUNKS - 1)

    remote(mix_send, mix_recv, mix_out, mix_in, (e, over)).wait_recv()
    mixer_ref[...] = (
        mixer_ref[...].astype(jnp.float32) + mix_recv[...].astype(jnp.float32)
    ).astype(jnp.bfloat16)

    for chunk in range(CHUNKS):
        for step in range(1, lines):
            there = lax.rem(z + step, lines)
            arrived = back_recv.at[chunk, there]
            remote(
                arrived, arrived, back_out.at[chunk, 0], back_in.at[chunk, there], (side, t)
            ).wait_recv()
        routed_ref[:, chunk * span : (chunk + 1) * span] = jnp.dot(
            placed[...],
            back_recv[chunk].reshape(groups * slots, span),
            preferred_element_type=jnp.float32,
        ).astype(jnp.bfloat16)

    for copy in pending:
        copy.wait_send()

    def drain(i, _):
        for other in range(PAIR):

            @pl.when(jnp.logical_not(jnp.logical_and(i == e, core == other)))
            def _():
                send_attended(i, other).wait_send()

        return 0

    lax.fori_loop(0, ep_count, drain, 0)


def fused(
    query_rows,
    key_rows,
    value_rows,
    key_bias,
    out_weight,
    moe_input,
    moe_gain,
    expert_pick,
    route_weight,
    w_gate,
    w_up,
    w_down,
):
    ep_count = lax.axis_size("ep")
    tp_count = lax.axis_size("tp")
    lines = ep_count // PAIR
    block_rows, width = query_rows.shape
    half = block_rows // PAIR
    quarter = half // PAIR
    tokens, model = moe_input.shape
    slots = GROUPS * tokens // (w_gate.shape[0] * ep_count)
    shard = w_gate.shape[2]
    span = model // CHUNKS
    bf16, f32 = jnp.bfloat16, jnp.float32
    dma = pltpu.SemaphoreType.DMA
    vmem = pltpu.VMEM
    scratch = [
        vmem((lines, HEAD_DIM, block_rows), bf16),
        vmem((ep_count, 2 * HEAD_DIM, half), bf16),
        vmem((lines, 2 * HEAD_DIM, block_rows), bf16),
        vmem((ep_count, 2 * HEAD_DIM, block_rows), bf16),
        vmem((ep_count * block_rows, 2 * HEAD_DIM), bf16),
        vmem((HEAD_DIM, half), f32),
        vmem((ep_count, HEAD_DIM, half), bf16),
        vmem((PAIR * width, half), bf16),
        vmem((PAIR * width, model), bf16),
        vmem((quarter, model), bf16),
        vmem((quarter, model), bf16),
        vmem((lines, slots, model + 128), bf16),
        vmem((ep_count, slots, model + 128), bf16),
        vmem((tokens, lines * slots), bf16),
        vmem((tp_count, model, shard), bf16),
        vmem((tp_count, model, shard), bf16),
        vmem((CHUNKS, tp_count * shard, span), bf16),
        vmem((ep_count * slots, tp_count * shard), bf16),
        vmem((CHUNKS, lines * slots, span), bf16),
        vmem((CHUNKS, lines * slots, span), bf16),
        vmem((CHUNKS, lines * slots, span), f32),
        vmem((CHUNKS, lines, slots, span), bf16),
        vmem((CHUNKS, lines, slots, span), bf16),
        dma((CHUNKS + 3,)),
        dma((CHUNKS + 2,)),
        dma((CHUNKS + 2,)),
        dma((CHUNKS + 2,)),
        dma((CHUNKS + 2,)),
        dma((CHUNKS + 2,)),
        dma((CHUNKS + 2,)),
        dma,
        dma,
        dma((ep_count,)),
        dma((ep_count,)),
        dma((lines,)),
        dma((lines,)),
        dma((ep_count,)),
        dma((lines,)),
        dma((lines,)),
        dma((ep_count,)),
        dma((ep_count, PAIR)),
        dma((PAIR, ep_count)),
        dma,
        dma,
        dma((CHUNKS,)),
        dma((CHUNKS,)),
        dma((CHUNKS, lines)),
        dma((CHUNKS, lines)),
    ]
    in_vmem = pl.BlockSpec(memory_space=pltpu.VMEM)
    anywhere = pl.BlockSpec(memory_space=pl.ANY)
    return pl.pallas_call(
        fused_kernel,
        out_shape=(
            jax.ShapeDtypeStruct((quarter, model), bf16),
            jax.ShapeDtypeStruct((tokens, model), bf16),
        ),
        in_specs=[in_vmem] * 4 + [anywhere] + [in_vmem] * 4 + [anywhere] * 3,
        out_specs=(in_vmem, in_vmem),
        scratch_shapes=scratch,
        compiler_params=pltpu.CompilerParams(
            collective_id=0, has_side_effects=True, vmem_limit_bytes=60 * 1024 * 1024
        ),
    )(
        query_rows,
        key_rows,
        value_rows,
        jnp.transpose(key_bias),
        out_weight,
        moe_input,
        moe_gain.reshape(1, model),
        jnp.transpose(expert_pick),
        jnp.transpose(route_weight),
        w_gate,
        w_up,
        w_down,
    )


def fits(query_rows, w_gate):
    ep_count = lax.axis_size("ep")
    return (
        lax.axis_size("tp") == PAIR * PAIR
        and TOPK == PAIR
        and w_gate.shape[0] == 1
        and ep_count == GROUPS * TOPK
        and query_rows.shape[1] == GROUPS * HEAD_DIM
    )


def step(*args):
    return (fused if fits(args[0], args[9]) else local)(*args)


def solution(mesh):
    placed = (
        P("ep", "tp"),
        P("ep", "tp"),
        P("ep", "tp"),
        P(None, "tp"),
        P("tp", None),
        P(("ep", "tp"), None),
        P(),
        P(("ep", "tp"), None),
        P(("ep", "tp"), None),
        P("ep", None, "tp"),
        P("ep", None, "tp"),
        P("ep", "tp", None),
    )
    return jax.shard_map(
        step,
        mesh=mesh,
        in_specs=placed,
        out_specs=(P(("ep", "tp"), None), P(("ep", "tp"), None)),
        check_vma=False,
    )
```

```python
import jax
import jax.numpy as jnp
from jax import lax
from jax.experimental import pallas as pl
from jax.experimental.pallas import tpu as pltpu
from jax.sharding import PartitionSpec as P

HEAD_DIM = 64
GROUPS = 4
TOPK = 2
PAIR = 2


norm_eps = 1e-06


def attend_kernel(tops_ref, query_ref, bias_ref, *rest):
    block_refs = rest[:-4]
    out_ref, acc_ref, kv_ref, sems = rest[-4:]

    @pl.when(pl.program_id(0) == 0)
    def _():
        copies = [
            pltpu.make_async_copy(ref, kv_ref.at[slot], sems.at[slot])
            for slot, ref in enumerate(block_refs)
        ]
        for copy in copies:
            copy.start()
        for copy in copies:
            copy.wait()

    tile = query_ref.shape[1]
    width = query_ref.shape[2]
    heads = width // HEAD_DIM
    slots = kv_ref.shape[0]
    per_block = kv_ref.shape[1] // tile
    top = tops_ref[pl.program_id(0)]
    own = tops_ref[2]
    turned = jnp.transpose(query_ref[0].astype(jnp.float32) * HEAD_DIM ** (-0.5))
    row_head = lax.broadcasted_iota(jnp.int32, (width, tile), 0) // HEAD_DIM
    queries = [jnp.where(row_head == h, turned, 0.0).astype(jnp.bfloat16) for h in range(heads)]
    key_at = lax.broadcasted_iota(jnp.int32, (tile, tile), 0)
    query_at = lax.broadcasted_iota(jnp.int32, (tile, tile), 1)
    causal = key_at < query_at
    later = jnp.where(causal, 1.0, 0.0).astype(jnp.bfloat16)
    acc_ref[...] = jnp.zeros_like(acc_ref)

    def visit(index, running, masked):
        block = index // per_block
        away = lax.rem(own // PAIR - block // PAIR + slots // PAIR, slots // PAIR)
        slot = away * PAIR + lax.rem(own + block, PAIR)
        rows = pl.ds(pl.multiple_of((index - block * per_block) * tile, tile), tile)
        first = pl.multiple_of(index * tile, tile)
        keys = kv_ref[slot, rows, :width]
        values = jnp.transpose(kv_ref[slot, rows, width:])
        passed = []
        for h in range(heads):
            scores = jnp.dot(keys, queries[h], preferred_element_type=jnp.float32)
            scores = scores + bias_ref[pl.ds(first, tile), h : h + 1]
            tail = jnp.log(1.0 + jnp.exp(-jnp.abs(scores)))
            lost = jnp.maximum(scores, 0.0) + tail
            won = jnp.minimum(scores, 0.0) - tail
            if masked:
                lost = jnp.where(causal, lost, 0.0)
            lost = lost.astype(jnp.bfloat16)
            after = jnp.dot(later, lost, preferred_element_type=jnp.float32)
            weight = jnp.exp(won - (after + running[h]))
            if masked:
                weight = jnp.where(causal, weight, 0.0)
            span = slice(h * HEAD_DIM, (h + 1) * HEAD_DIM)
            acc_ref[span, :] += jnp.dot(
                values[span, :], weight.astype(jnp.bfloat16), preferred_element_type=jnp.float32
            )
            passed.append(running[h] + after[0:1, :] + lost[0:1, :].astype(jnp.float32))
        return tuple(passed)

    running = tuple(jnp.zeros((1, tile), jnp.float32) for _ in range(heads))
    running = visit(top, running, True)
    lax.fori_loop(0, top, lambda step, carried: visit(top - 1 - step, carried, False), running)
    out_ref[0] = jnp.transpose(acc_ref[...]).astype(jnp.bfloat16)


def attend(tops, queries, blocks, bias):
    parts, tile, width = queries.shape
    held = (len(blocks),) + blocks[0].shape
    pairs = parts * tile * held[0] * held[1] * width // HEAD_DIM // 2
    return pl.pallas_call(
        attend_kernel,
        out_shape=jax.ShapeDtypeStruct(queries.shape, jnp.bfloat16),
        grid_spec=pltpu.PrefetchScalarGridSpec(
            num_scalar_prefetch=1,
            grid=(parts,),
            in_specs=[
                pl.BlockSpec((1, tile, width), lambda c, tops: (c, 0, 0)),
                pl.BlockSpec(memory_space=pltpu.VMEM),
            ]
            + [pl.BlockSpec(memory_space=pl.ANY)] * len(blocks),
            out_specs=pl.BlockSpec((1, tile, width), lambda c, tops: (c, 0, 0)),
            scratch_shapes=[
                pltpu.VMEM((width, tile), jnp.float32),
                pltpu.VMEM(held, blocks[0].dtype),
                pltpu.SemaphoreType.DMA((len(blocks),)),
            ],
        ),
        cost_estimate=pl.CostEstimate(
            flops=pairs * 1000, bytes_accessed=len(blocks) * blocks[0].size * 2, transcendentals=pairs * 3
        ),
        compiler_params=pltpu.CompilerParams(vmem_limit_bytes=58 * 1024 * 1024),
    )(tops, queries, bias, *blocks)


def gather_blocks(own, count):
    ring = count // PAIR
    swap = [(i, i // PAIR * PAIR + (i + 1) % PAIR) for i in range(count)]
    ahead = [(i, (i + PAIR) % count) for i in range(count)]
    behind = [(j, i) for i, j in ahead]
    near = [own, lax.ppermute(own, "ep", swap)]
    far = {}
    for member in range(PAIR):
        reach = (ring - 1 + (member == 0)) // 2
        held = near[member]
        for step in range(1, reach + 1):
            held = lax.ppermute(held, "ep", ahead)
            far[step, member] = held
        held = near[member]
        for step in range(ring - 1, reach, -1):
            held = lax.ppermute(held, "ep", behind)
            far[step, member] = held
    return near + [far[step, member] for step in range(1, ring) for member in range(PAIR)]


def expand(arrived, gate_weights, up_weights):
    gate_in = jnp.einsum(
        "necm,emf->necf", arrived, gate_weights, preferred_element_type=jnp.float32
    )
    up_in = jnp.einsum("necm,emf->necf", arrived, up_weights, preferred_element_type=jnp.float32)
    return (jax.nn.silu(gate_in) * up_in).astype(jnp.bfloat16)


def contract(hidden, down_weights):
    return jnp.einsum("necf,efm->necm", hidden, down_weights, preferred_element_type=jnp.float32)


def local(
    query_rows,
    key_rows,
    value_rows,
    key_bias,
    out_weight,
    moe_input,
    moe_gain,
    expert_pick,
    route_weight,
    w_gate,
    w_up,
    w_down,
):
    block_rows = query_rows.shape[0]
    half_rows = block_rows // 2
    ep_index = lax.axis_index("ep")
    ep_count = lax.axis_size("ep")
    own_kv = jnp.concatenate([key_rows, value_rows], axis=1)
    mirror = [(i, ep_count - 1 - i) for i in range(ep_count)]
    far_query = lax.ppermute(query_rows[half_rows:], "ep", mirror)
    blocks = gather_blocks(own_kv, ep_count)
    tops = jnp.stack(
        [2 * ep_index, 2 * (ep_count - 1 - ep_index) + 1, ep_index]
    ).astype(jnp.int32)
    near, far = attend(
        tops, jnp.stack([query_rows[:half_rows], far_query]), blocks, key_bias
    )
    attended = jnp.concatenate([near, lax.ppermute(far, "ep", mirror)], axis=0)
    mixer_out = lax.psum_scatter(
        jnp.dot(attended, out_weight, preferred_element_type=jnp.float32).astype(jnp.bfloat16),
        "tp",
        scatter_dimension=0,
        tiled=True,
    )
    token_count = moe_input.shape[0]
    widened = moe_input.astype(jnp.float32)
    normed = (
        widened
        * lax.rsqrt(jnp.mean(widened * widened, axis=1, keepdims=True) + norm_eps)
        * moe_gain
    ).astype(jnp.bfloat16)
    local_experts = w_gate.shape[0]
    expert_total = local_experts * ep_count
    capacity = GROUPS * token_count // expert_total
    picks = expert_pick.reshape(-1)
    matches = (picks[:, None] == jnp.arange(expert_total, dtype=jnp.int32)[None, :]).astype(
        jnp.int32
    )
    ranks = jnp.sum((jnp.cumsum(matches, axis=0) - matches) * matches, axis=1)
    slots = picks * capacity + ranks
    owners = jnp.arange(picks.shape[0], dtype=jnp.int32) // TOPK
    table = jnp.full((expert_total * capacity,), token_count, jnp.int32).at[slots].set(owners)
    padded = jnp.concatenate([normed, jnp.zeros((1, normed.shape[1]), jnp.bfloat16)], axis=0)
    outgoing = padded[table].reshape(ep_count, local_experts, capacity, normed.shape[1])
    outgoing = lax.optimization_barrier((outgoing, far_query, *blocks))[0]
    arrived = lax.all_to_all(outgoing, "ep", split_axis=0, concat_axis=0, tiled=True)
    gate_all, up_all, down_all = (
        lax.all_gather(w_gate, "tp", axis=2, tiled=True),
        lax.all_gather(w_up, "tp", axis=2, tiled=True),
        lax.all_gather(w_down, "tp", axis=1, tiled=True),
    )
    served = contract(expand(arrived, gate_all, up_all), down_all).astype(jnp.bfloat16)
    returned = lax.all_to_all(served, "ep", split_axis=0, concat_axis=0, tiled=True)
    flat = returned.reshape(expert_total * capacity, returned.shape[3])
    chosen = flat[slots].reshape(token_count, TOPK, flat.shape[1]).astype(jnp.float32)
    routed_out = jnp.sum(chosen * route_weight[:, :, None], axis=1).astype(jnp.bfloat16)
    return (mixer_out, routed_out)


MESH = pl.DeviceIdType.MESH
CHUNKS = 4


def remote(src, dst, send, recv, device):
    return pltpu.make_async_remote_copy(
        src_ref=src,
        dst_ref=dst,
        send_sem=send,
        recv_sem=recv,
        device_id=device,
        device_id_type=MESH,
    )


def split_parts(values):
    high = values.astype(jnp.bfloat16).astype(jnp.float32)
    rest = values - high
    middle = rest.astype(jnp.bfloat16).astype(jnp.float32)
    return high, middle, rest - middle


def fused_kernel(
    q_ref,
    k_ref,
    v_ref,
    bias_ref,
    out_weight_ref,
    moe_ref,
    gain_ref,
    pick_ref,
    route_ref,
    gate_ref,
    up_ref,
    down_ref,
    mixer_ref,
    routed_ref,
    q_send,
    q_recv,
    kv_send,
    kv_recv,
    keys,
    scores_buf,
    won,
    weights,
    acc,
    att_send,
    att_recv,
    project,
    mix_send,
    mix_recv,
    rows_send,
    rows_recv,
    placed,
    gate_all,
    up_all,
    down_all,
    hidden,
    part_send,
    part_recv,
    part_own,
    back_send,
    back_recv,
    local_sem,
    over_send,
    over_recv,
    die_send,
    die_recv,
    pass_send,
    pass_recv,
    project_send,
    project_recv,
    q_out,
    q_in,
    kv_out,
    kv_pass,
    kv_in,
    rows_out,
    rows_pass,
    rows_in,
    att_out,
    att_in,
    mix_out,
    mix_in,
    part_out,
    part_in,
    back_out,
    back_in,
):
    ep_count = q_recv.shape[0]
    lines = ep_count // PAIR
    e, t = lax.axis_index("ep"), lax.axis_index("tp")
    z, y = lax.div(e, PAIR), lax.rem(e, PAIR)
    chip, core = lax.div(t, PAIR), lax.rem(t, PAIR)
    die = PAIR * chip + 1 - core
    over = PAIR * (1 - chip) + core
    across = PAIR * (1 - chip) + 1 - core
    side = PAIR * z + 1 - y
    block_rows, width = q_ref.shape
    half = block_rows // PAIR
    quarter = half // PAIR
    tokens, model = moe_ref.shape
    slots = rows_send.shape[1]
    shard = gate_ref.shape[2]
    span = model // CHUNKS

    upper = lax.div(z, PAIR)
    inner = lax.rem(z + upper, PAIR)

    def nearest(order):
        away = (1, 2 + inner, 3 - inner)[order]
        return lax.rem(z + away + upper * (2 * lines - 2 * away), lines)

    barrier = pltpu.get_barrier_semaphore()
    for step in range(1, ep_count):
        for other in range(PAIR):
            pl.semaphore_signal(
                barrier,
                inc=1,
                device_id=(lax.rem(e + step, ep_count), PAIR * chip + other),
                device_id_type=MESH,
            )
    for other in (die, over):
        pl.semaphore_signal(barrier, inc=1, device_id=(e, other), device_id_type=MESH)

    pieces = []
    own_rows = pl.ds(pl.multiple_of(t * shard, shard), shard)
    pieces.append((gate_ref.at[0], gate_all.at[t]))
    pieces.append((up_ref.at[0], up_all.at[t]))
    for chunk in range(CHUNKS):
        pieces.append(
            (
                down_ref.at[0, :, chunk * span : (chunk + 1) * span],
                down_all.at[chunk, own_rows, :],
            )
        )

    def held(index, owner):
        if index == 0:
            return gate_all.at[owner]
        if index == 1:
            return up_all.at[owner]
        rows = pl.ds(pl.multiple_of(owner * shard, shard), shard)
        return down_all.at[index - 2, rows, :]

    project_rows = pl.ds(pl.multiple_of(core * width, width), width)
    die_rows = pl.ds(pl.multiple_of((1 - core) * width, width), width)
    locals_ = [
        pltpu.make_async_copy(src, dst, local_sem.at[i]) for i, (src, dst) in enumerate(pieces)
    ]
    locals_.append(
        pltpu.make_async_copy(out_weight_ref, project.at[project_rows, :], local_sem.at[len(pieces)])
    )
    for copy in locals_:
        copy.start()

    keys_turned = jnp.transpose(k_ref[...].astype(jnp.float32)).astype(jnp.bfloat16)
    values_turned = jnp.transpose(v_ref[...].astype(jnp.float32)).astype(jnp.bfloat16)
    for h in range(lines):
        span_h = slice(h * HEAD_DIM, (h + 1) * HEAD_DIM)
        kv_send[h, :HEAD_DIM, :] = keys_turned[span_h, :]
        kv_send[h, HEAD_DIM:, :] = values_turned[span_h, :]
    pl.semaphore_wait(barrier, PAIR * (ep_count - 1) + 2)

    pending = []
    for i, (src, dst) in enumerate(pieces):
        copy = remote(src, dst, over_send.at[i], over_recv.at[i], (e, over))
        copy.start()
        pending.append(copy)
    for order in range(lines - 1):
        there = nearest(order)
        copy = remote(
            kv_send.at[there], kv_recv.at[e], kv_out.at[order], kv_in.at[e], (PAIR * there + y, t)
        )
        copy.start()
        pending.append(copy)
    copy = remote(kv_send.at[z], kv_recv.at[e], kv_pass.at[z], kv_in.at[e], (side, t))
    copy.start()
    pending.append(copy)
    kv_recv[e] = kv_send[z]

    q_turned = jnp.transpose(q_ref[...].astype(jnp.float32) * HEAD_DIM ** (-0.5))
    for h in range(lines):
        q_send[h] = q_turned[h * HEAD_DIM : (h + 1) * HEAD_DIM, :].astype(jnp.bfloat16)
    ones_at = lax.broadcasted_iota(jnp.int32, (HEAD_DIM, half), 0) < 3
    ones_rows = jnp.where(ones_at, 1.0, 0.0).astype(jnp.bfloat16)
    for i in range(ep_count):
        q_recv[i, HEAD_DIM:, :] = ones_rows
    for step in range(1, ep_count):
        head = z if step == ep_count - 1 else nearest((step - 1) // PAIR)
        column = 1 - y if step == ep_count - 1 else (step - 1) % PAIR
        there = PAIR * head + column
        lanes = pl.ds(pl.multiple_of(lax.rem(column + e, PAIR) * half, half), half)
        copy = remote(
            q_send.at[head, :, lanes],
            q_recv.at[e, :HEAD_DIM, :],
            q_out.at[step],
            q_in.at[e],
            (there, t),
        )
        copy.start()
        pending.append(copy)
    own_lanes = pl.ds(pl.multiple_of(lax.rem(y + e, PAIR) * half, half), half)
    q_recv[e, :HEAD_DIM, :] = q_send[z, :, own_lanes]

    for i, (src, dst) in enumerate(pieces):
        copy = remote(src, dst, die_send.at[i], die_recv.at[i], (e, die))
        copy.start()
        pending.append(copy)
    copy = remote(
        out_weight_ref, project.at[project_rows, :], project_send, project_recv, (e, die)
    )
    copy.start()
    pending.append(copy)

    widened = moe_ref[...].astype(jnp.float32)
    normed = (
        widened
        * lax.rsqrt(jnp.mean(widened * widened, axis=1, keepdims=True) + norm_eps)
        * gain_ref[...]
    ).astype(jnp.bfloat16)
    group_row = lax.shift_right_logical(pick_ref[0:1, :], 1)
    groups = lines
    group_at = lax.broadcasted_iota(jnp.int32, (8, tokens), 0)
    chosen = (group_at == group_row).astype(jnp.float32)
    earlier = (
        lax.broadcasted_iota(jnp.int32, (tokens, tokens), 0)
        < lax.broadcasted_iota(jnp.int32, (tokens, tokens), 1)
    ).astype(jnp.float32)
    ranks = jnp.dot(
        chosen.astype(jnp.bfloat16),
        earlier.astype(jnp.bfloat16),
        preferred_element_type=jnp.float32,
    )
    slot_row = jnp.sum(
        chosen * (ranks + group_at.astype(jnp.float32) * slots), axis=0, keepdims=True
    )
    slot_at = lax.broadcasted_iota(jnp.int32, (groups * slots, tokens), 0)
    picked = (slot_at == slot_row.astype(jnp.int32)).astype(jnp.float32)
    placed[...] = jnp.transpose(picked).astype(jnp.bfloat16)
    first_low = (pick_ref[0:1, :] & 1) == 0
    low_row = jnp.where(first_low, route_ref[0:1, :], route_ref[1:2, :])
    high_row = jnp.where(first_low, route_ref[1:2, :], route_ref[0:1, :])
    low = split_parts(jnp.sum(picked * low_row, axis=1, keepdims=True))
    high = split_parts(jnp.sum(picked * high_row, axis=1, keepdims=True))
    lane = lax.broadcasted_iota(jnp.int32, (groups * slots, 128), 1)
    shares = jnp.zeros((groups * slots, 128), jnp.float32)
    for i, part in enumerate(low + high):
        shares = jnp.where(lane == i, part, shares)
    rows_send[:, :, model:] = shares.astype(jnp.bfloat16).reshape(groups, slots, 128)
    picked = picked.astype(jnp.bfloat16)
    for first in range(0, model, span):
        rows_send[:, :, first : first + span] = (
            jnp.dot(picked, normed[:, first : first + span], preferred_element_type=jnp.float32)
            .astype(jnp.bfloat16)
            .reshape(groups, slots, span)
        )
    for order in range(lines - 1):
        there = nearest(order)
        source = PAIR * there + y
        arrived = kv_recv.at[source]
        remote(arrived, arrived, kv_out.at[0], kv_in.at[source], (side, t)).wait_recv()
        copy = remote(arrived, arrived, kv_pass.at[there], kv_in.at[source], (side, t))
        copy.start()
        pending.append(copy)
    home = y * lines + z
    for order in range(lines - 1):
        there = nearest(order)
        copy = remote(
            rows_send.at[there],
            rows_recv.at[home],
            rows_out.at[order],
            rows_in.at[home],
            (PAIR * there + y, t),
        )
        copy.start()
        pending.append(copy)

    copy = remote(rows_send.at[z], rows_recv.at[home], rows_pass.at[z], rows_in.at[home], (side, t))
    copy.start()
    pending.append(copy)
    rows_recv[home] = rows_send[z]

    for i in range(lines):
        source = PAIR * i + 1 - y
        arrived = kv_recv.at[source]
        remote(arrived, arrived, kv_out.at[0], kv_in.at[source], (side, t)).wait_recv()
    for step in range(1, ep_count):
        source = lax.rem(e + step, ep_count)
        arrived = q_recv.at[source, :HEAD_DIM, :]
        remote(arrived, arrived, q_out.at[0], q_in.at[source], (side, t)).wait_recv()

    head_at = lax.broadcasted_iota(jnp.int32, (lines, block_rows), 0)
    aug_at = lax.broadcasted_iota(jnp.int32, (HEAD_DIM, block_rows), 0)

    def turn_keys(i, _):
        rows = pl.ds(pl.multiple_of(i * block_rows, block_rows), block_rows)
        bias = jnp.sum(
            jnp.where(head_at == z, bias_ref[:, rows], 0.0), axis=0, keepdims=True
        )
        extra = jnp.zeros((HEAD_DIM, block_rows), jnp.float32)
        for place, part in enumerate(split_parts(bias)):
            extra = jnp.where(aug_at == place, part, extra)
        stacked = jnp.concatenate([kv_recv[i, :HEAD_DIM, :].astype(jnp.float32), extra], axis=0)
        keys[rows, :] = jnp.transpose(stacked).astype(jnp.bfloat16)
        return 0

    lax.fori_loop(0, ep_count, turn_keys, 0)

    key_at = lax.broadcasted_iota(jnp.int32, (half, half), 0)
    query_at = lax.broadcasted_iota(jnp.int32, (half, half), 1)
    later = jnp.where(key_at < query_at, 1.0, 0.0).astype(jnp.bfloat16)

    def score(block, queries):
        for sub in range(PAIR):
            rows = pl.ds(pl.multiple_of(block * block_rows + sub * half, half), half)
            scores_buf[sub] = jnp.dot(keys[rows, :], queries, preferred_element_type=jnp.float32)

    def gather_values(block):
        acc[...] += jnp.dot(
            kv_recv[block, HEAD_DIM:, :], weights[...], preferred_element_type=jnp.float32
        )

    def visit(following, queries, running, place):
        firsts, afters = {}, {}
        for sub in range(PAIR - 1, -1, -1):
            scores = scores_buf[sub]
            lost = jnp.maximum(scores, jnp.log(1.0 + jnp.exp(jnp.minimum(scores, 80.0))))
            won[sub] = scores - lost
            if place is not None:
                lost = jnp.where(key_at - query_at < (place - sub) * half, lost, 0.0)
            lost = lost.astype(jnp.bfloat16)
            firsts[sub] = lost[0:1, :].astype(jnp.float32)
            afters[sub] = jnp.dot(later, lost, preferred_element_type=jnp.float32)
        score(following, queries)
        for sub in range(PAIR - 1, -1, -1):
            weight = jnp.exp(won[sub] - (afters[sub] + running))
            if place is not None:
                weight = jnp.where(key_at - query_at < (place - sub) * half, weight, 0.0)
            weights[sub * half : (sub + 1) * half, :] = weight.astype(jnp.bfloat16)
            running = running + afters[sub][0:1, :] + firsts[sub]
        return running

    def send_attended(i, other):
        place = lax.rem(y + i, PAIR)
        return remote(
            att_send.at[i, :, other * quarter : (other + 1) * quarter],
            att_recv.at[
                pl.ds(pl.multiple_of(core * width + z * HEAD_DIM, HEAD_DIM), HEAD_DIM),
                pl.ds(pl.multiple_of(place * quarter, quarter), quarter),
            ],
            att_out.at[i, other],
            att_in.at[core, e],
            (i, PAIR * chip + other),
        )

    def wait_rows(place):
        arrived = rows_recv.at[place]
        remote(arrived, arrived, rows_out.at[0], rows_in.at[place], (side, t)).wait_recv()

    def pass_rows(order):
        there = nearest(order)
        place = y * lines + there
        arrived = rows_recv.at[place]
        return remote(arrived, arrived, rows_pass.at[there], rows_in.at[place], (side, t))

    def pass_rows_on(order):
        wait_rows(y * lines + nearest(order))
        pass_rows(order).start()

    def one_tile(i, _):
        for order in range(lines - 2):

            @pl.when(i == ep_count - lines + 2 + order)
            def _():
                pass_rows_on(order)

        place = lax.rem(y + i, PAIR)
        queries = q_recv[i]
        acc[...] = jnp.zeros_like(acc)
        score(i, queries)
        running = visit(
            jnp.maximum(i - 1, 0), queries, jnp.zeros((1, half), jnp.float32), place
        )

        def next_block(s, running):
            gather_values(i - s)
            return visit(jnp.maximum(i - 2 - s, 0), queries, running, None)

        lax.fori_loop(0, i, next_block, running)
        gather_values(0)
        att_send[i] = acc[...].astype(jnp.bfloat16)
        for other in range(PAIR):
            here = jnp.logical_and(i == e, core == other)

            @pl.when(jnp.logical_not(here))
            def _():
                send_attended(i, other).start()

            @pl.when(here)
            def _():
                att_recv[
                    pl.ds(pl.multiple_of(core * width + z * HEAD_DIM, HEAD_DIM), HEAD_DIM),
                    pl.ds(pl.multiple_of(place * quarter, quarter), quarter),
                ] = att_send[i, :, other * quarter : (other + 1) * quarter]

        return 0

    lax.fori_loop(0, ep_count, one_tile, 0)

    pass_rows_on(lines - 2)

    def pass_on(index):
        arrived = held(index, over)
        remote(arrived, arrived, over_send.at[index], over_recv.at[index], (e, over)).wait_recv()
        copy = remote(arrived, arrived, pass_send.at[index], pass_recv.at[index], (e, die))
        copy.start()
        pending.append(copy)

    def wait_die(index):
        arrived = held(index, die)
        remote(arrived, arrived, die_send.at[index], die_recv.at[index], (e, die)).wait_recv()

    def wait_across(index):
        arrived = held(index, across)
        remote(arrived, arrived, pass_send.at[index], pass_recv.at[index], (e, die)).wait_recv()

    def serve(owner, column):
        hidden_lanes = pl.ds(pl.multiple_of(owner * shard, shard), shard)
        rows = rows_recv[pl.ds(column * lines, lines), :, :model].reshape(lines * slots, model)
        gate_in = jnp.dot(rows, gate_all[owner], preferred_element_type=jnp.float32)
        up_in = jnp.dot(rows, up_all[owner], preferred_element_type=jnp.float32)
        target = pl.ds(pl.multiple_of(column * lines * slots, lines * slots), lines * slots)
        hidden[target, hidden_lanes] = (gate_in / (1.0 + jnp.exp(-gate_in)) * up_in).astype(
            jnp.bfloat16
        )

    def serve_near(column):
        def one(k, _):
            serve(PAIR * chip + lax.rem(core + k, PAIR), column)
            return 0

        lax.fori_loop(0, PAIR, one, 0)

    def serve_across(column, _):
        serve(across, column)
        return 0

    pass_on(0)
    for copy in locals_:
        copy.wait()
    wait_die(0)
    wait_die(1)
    serve_near(y)
    pass_on(1)
    serve(over, y)
    for i in range(lines):
        wait_rows((1 - y) * lines + i)
    serve_near(1 - y)
    serve(over, 1 - y)
    wait_across(0)
    wait_across(1)
    lax.fori_loop(0, PAIR, serve_across, 0)

    def mix():
        for source_core in range(PAIR):
            for i in range(ep_count):

                @pl.when(jnp.logical_not(jnp.logical_and(core == source_core, e == i)))
                def _():
                    first = source_core * width + i // PAIR * HEAD_DIM
                    place = lax.rem(i % PAIR + e, PAIR)
                    lanes = pl.ds(pl.multiple_of(place * quarter, quarter), quarter)
                    arrived = att_recv.at[first : first + HEAD_DIM, lanes]
                    remote(
                        arrived, arrived, att_out.at[0, 0], att_in.at[source_core, i], (side, t)
                    ).wait_recv()

        arrived = project.at[die_rows, :]
        remote(arrived, arrived, project_send, project_recv, (e, die)).wait_recv()

        def mixed(which):
            lanes = pl.ds(pl.multiple_of(which * quarter, quarter), quarter)
            attended = jnp.transpose(att_recv[:, lanes].astype(jnp.float32)).astype(jnp.bfloat16)
            return jnp.dot(attended, project[...], preferred_element_type=jnp.float32).astype(
                jnp.bfloat16
            )

        mix_send[...] = mixed(1 - chip)
        copy = remote(mix_send, mix_recv, mix_out, mix_in, (e, over))
        copy.start()
        pending.append(copy)
        mixer_ref[...] = mixed(chip)

    share_lane = lax.broadcasted_iota(jnp.int32, (lines * slots, 128), 1)
    share_here = jnp.logical_and(share_lane >= 3 * y, share_lane < 3 * y + 3)

    def contract(chunk, which):
        rows = pl.ds(pl.multiple_of(which * lines * slots, lines * slots), lines * slots)
        shares = rows_recv[pl.ds(which * lines, lines), :, model:].reshape(lines * slots, 128)
        share = jnp.sum(
            jnp.where(share_here, shares.astype(jnp.float32), 0.0), axis=1, keepdims=True
        )
        return (
            jnp.dot(hidden[rows, :], down_all[chunk], preferred_element_type=jnp.float32) * share
        )

    def give_back(chunk):
        arrived = part_recv.at[chunk]
        remote(arrived, arrived, part_out.at[chunk], part_in.at[chunk], (side, t)).wait_recv()
        total = part_own[chunk] + part_recv[chunk].astype(jnp.float32)
        back_send[chunk] = total.astype(jnp.bfloat16).reshape(lines, slots, span)
        for order in range(lines - 1):
            there = nearest(order)
            copy = remote(
                back_send.at[chunk, there],
                back_recv.at[chunk, z],
                back_out.at[chunk, order],
                back_in.at[chunk, z],
                (PAIR * there + y, t),
            )
            copy.start()
            pending.append(copy)
        back_recv[chunk, z] = back_send[chunk, z]

    for chunk in range(CHUNKS):
        pass_on(2 + chunk)
        wait_die(2 + chunk)
        wait_across(2 + chunk)
        part_send[chunk] = contract(chunk, 1 - y).astype(jnp.bfloat16)
        copy = remote(
            part_send.at[chunk],
            part_recv.at[chunk],
            part_out.at[chunk],
            part_in.at[chunk],
            (side, t),
        )
        copy.start()
        pending.append(copy)
        part_own[chunk] = contract(chunk, y)
        if chunk > 0:
            give_back(chunk - 1)
        if chunk == 1:
            mix()
    give_back(CHUNKS - 1)

    remote(mix_send, mix_recv, mix_out, mix_in, (e, over)).wait_recv()
    mixer_ref[...] = (
        mixer_ref[...].astype(jnp.float32) + mix_recv[...].astype(jnp.float32)
    ).astype(jnp.bfloat16)

    for chunk in range(CHUNKS):
        for step in range(1, lines):
            there = lax.rem(z + step, lines)
            arrived = back_recv.at[chunk, there]
            remote(
                arrived, arrived, back_out.at[chunk, 0], back_in.at[chunk, there], (side, t)
            ).wait_recv()
        routed_ref[:, chunk * span : (chunk + 1) * span] = jnp.dot(
            placed[...],
            back_recv[chunk].reshape(groups * slots, span),
            preferred_element_type=jnp.float32,
        ).astype(jnp.bfloat16)

    for copy in pending:
        copy.wait_send()
    for order in range(lines - 1):
        pass_rows(order).wait_send()

    def drain(i, _):
        for other in range(PAIR):

            @pl.when(jnp.logical_not(jnp.logical_and(i == e, core == other)))
            def _():
                send_attended(i, other).wait_send()

        return 0

    lax.fori_loop(0, ep_count, drain, 0)


def fused(
    query_rows,
    key_rows,
    value_rows,
    key_bias,
    out_weight,
    moe_input,
    moe_gain,
    expert_pick,
    route_weight,
    w_gate,
    w_up,
    w_down,
):
    ep_count = lax.axis_size("ep")
    tp_count = lax.axis_size("tp")
    lines = ep_count // PAIR
    block_rows, width = query_rows.shape
    half = block_rows // PAIR
    quarter = half // PAIR
    tokens, model = moe_input.shape
    slots = GROUPS * tokens // (w_gate.shape[0] * ep_count)
    shard = w_gate.shape[2]
    span = model // CHUNKS
    bf16, f32 = jnp.bfloat16, jnp.float32
    dma = pltpu.SemaphoreType.DMA
    vmem = pltpu.VMEM
    scratch = [
        vmem((lines, HEAD_DIM, block_rows), bf16),
        vmem((ep_count, 2 * HEAD_DIM, half), bf16),
        vmem((lines, 2 * HEAD_DIM, block_rows), bf16),
        vmem((ep_count, 2 * HEAD_DIM, block_rows), bf16),
        vmem((ep_count * block_rows, 2 * HEAD_DIM), bf16),
        vmem((PAIR, half, half), f32),
        vmem((PAIR, half, half), f32),
        vmem((block_rows, half), bf16),
        vmem((HEAD_DIM, half), f32),
        vmem((ep_count, HEAD_DIM, half), bf16),
        vmem((PAIR * width, half), bf16),
        vmem((PAIR * width, model), bf16),
        vmem((quarter, model), bf16),
        vmem((quarter, model), bf16),
        vmem((lines, slots, model + 128), bf16),
        vmem((ep_count, slots, model + 128), bf16),
        vmem((tokens, lines * slots), bf16),
        vmem((tp_count, model, shard), bf16),
        vmem((tp_count, model, shard), bf16),
        vmem((CHUNKS, tp_count * shard, span), bf16),
        vmem((ep_count * slots, tp_count * shard), bf16),
        vmem((CHUNKS, lines * slots, span), bf16),
        vmem((CHUNKS, lines * slots, span), bf16),
        vmem((CHUNKS, lines * slots, span), f32),
        vmem((CHUNKS, lines, slots, span), bf16),
        vmem((CHUNKS, lines, slots, span), bf16),
        dma((CHUNKS + 3,)),
        dma((CHUNKS + 2,)),
        dma((CHUNKS + 2,)),
        dma((CHUNKS + 2,)),
        dma((CHUNKS + 2,)),
        dma((CHUNKS + 2,)),
        dma((CHUNKS + 2,)),
        dma,
        dma,
        dma((ep_count,)),
        dma((ep_count,)),
        dma((lines,)),
        dma((lines,)),
        dma((ep_count,)),
        dma((lines,)),
        dma((lines,)),
        dma((ep_count,)),
        dma((ep_count, PAIR)),
        dma((PAIR, ep_count)),
        dma,
        dma,
        dma((CHUNKS,)),
        dma((CHUNKS,)),
        dma((CHUNKS, lines)),
        dma((CHUNKS, lines)),
    ]
    in_vmem = pl.BlockSpec(memory_space=pltpu.VMEM)
    anywhere = pl.BlockSpec(memory_space=pl.ANY)
    return pl.pallas_call(
        fused_kernel,
        out_shape=(
            jax.ShapeDtypeStruct((quarter, model), bf16),
            jax.ShapeDtypeStruct((tokens, model), bf16),
        ),
        in_specs=[in_vmem] * 4 + [anywhere] + [in_vmem] * 4 + [anywhere] * 3,
        out_specs=(in_vmem, in_vmem),
        scratch_shapes=scratch,
        compiler_params=pltpu.CompilerParams(
            collective_id=0, has_side_effects=True, vmem_limit_bytes=60 * 1024 * 1024
        ),
    )(
        query_rows,
        key_rows,
        value_rows,
        jnp.transpose(key_bias),
        out_weight,
        moe_input,
        moe_gain.reshape(1, model),
        jnp.transpose(expert_pick),
        jnp.transpose(route_weight),
        w_gate,
        w_up,
        w_down,
    )


def fits(query_rows, w_gate):
    ep_count = lax.axis_size("ep")
    return (
        lax.axis_size("tp") == PAIR * PAIR
        and TOPK == PAIR
        and w_gate.shape[0] == 1
        and ep_count == GROUPS * TOPK
        and query_rows.shape[1] == GROUPS * HEAD_DIM
    )


def step(*args):
    return (fused if fits(args[0], args[9]) else local)(*args)


def solution(mesh):
    placed = (
        P("ep", "tp"),
        P("ep", "tp"),
        P("ep", "tp"),
        P(None, "tp"),
        P("tp", None),
        P(("ep", "tp"), None),
        P(),
        P(("ep", "tp"), None),
        P(("ep", "tp"), None),
        P("ep", None, "tp"),
        P("ep", None, "tp"),
        P("ep", "tp", None),
    )
    return jax.shard_map(
        step,
        mesh=mesh,
        in_specs=placed,
        out_specs=(P(("ep", "tp"), None), P(("ep", "tp"), None)),
        check_vma=False,
    )
```

```python
import jax
import jax.numpy as jnp
from jax import lax
from jax.experimental import pallas as pl
from jax.experimental.pallas import tpu as pltpu
from jax.sharding import PartitionSpec as P

HEAD_DIM = 64
GROUPS = 4
TOPK = 2
PAIR = 2


norm_eps = 1e-06


def attend_kernel(tops_ref, query_ref, bias_ref, *rest):
    block_refs = rest[:-4]
    out_ref, acc_ref, kv_ref, sems = rest[-4:]

    @pl.when(pl.program_id(0) == 0)
    def _():
        copies = [
            pltpu.make_async_copy(ref, kv_ref.at[slot], sems.at[slot])
            for slot, ref in enumerate(block_refs)
        ]
        for copy in copies:
            copy.start()
        for copy in copies:
            copy.wait()

    tile = query_ref.shape[1]
    width = query_ref.shape[2]
    heads = width // HEAD_DIM
    slots = kv_ref.shape[0]
    per_block = kv_ref.shape[1] // tile
    top = tops_ref[pl.program_id(0)]
    own = tops_ref[2]
    turned = jnp.transpose(query_ref[0].astype(jnp.float32) * HEAD_DIM ** (-0.5))
    row_head = lax.broadcasted_iota(jnp.int32, (width, tile), 0) // HEAD_DIM
    queries = [jnp.where(row_head == h, turned, 0.0).astype(jnp.bfloat16) for h in range(heads)]
    key_at = lax.broadcasted_iota(jnp.int32, (tile, tile), 0)
    query_at = lax.broadcasted_iota(jnp.int32, (tile, tile), 1)
    causal = key_at < query_at
    later = jnp.where(causal, 1.0, 0.0).astype(jnp.bfloat16)
    acc_ref[...] = jnp.zeros_like(acc_ref)

    def visit(index, running, masked):
        block = index // per_block
        away = lax.rem(own // PAIR - block // PAIR + slots // PAIR, slots // PAIR)
        slot = away * PAIR + lax.rem(own + block, PAIR)
        rows = pl.ds(pl.multiple_of((index - block * per_block) * tile, tile), tile)
        first = pl.multiple_of(index * tile, tile)
        keys = kv_ref[slot, rows, :width]
        values = jnp.transpose(kv_ref[slot, rows, width:])
        passed = []
        for h in range(heads):
            scores = jnp.dot(keys, queries[h], preferred_element_type=jnp.float32)
            scores = scores + bias_ref[pl.ds(first, tile), h : h + 1]
            tail = jnp.log(1.0 + jnp.exp(-jnp.abs(scores)))
            lost = jnp.maximum(scores, 0.0) + tail
            won = jnp.minimum(scores, 0.0) - tail
            if masked:
                lost = jnp.where(causal, lost, 0.0)
            lost = lost.astype(jnp.bfloat16)
            after = jnp.dot(later, lost, preferred_element_type=jnp.float32)
            weight = jnp.exp(won - (after + running[h]))
            if masked:
                weight = jnp.where(causal, weight, 0.0)
            span = slice(h * HEAD_DIM, (h + 1) * HEAD_DIM)
            acc_ref[span, :] += jnp.dot(
                values[span, :], weight.astype(jnp.bfloat16), preferred_element_type=jnp.float32
            )
            passed.append(running[h] + after[0:1, :] + lost[0:1, :].astype(jnp.float32))
        return tuple(passed)

    running = tuple(jnp.zeros((1, tile), jnp.float32) for _ in range(heads))
    running = visit(top, running, True)
    lax.fori_loop(0, top, lambda step, carried: visit(top - 1 - step, carried, False), running)
    out_ref[0] = jnp.transpose(acc_ref[...]).astype(jnp.bfloat16)


def attend(tops, queries, blocks, bias):
    parts, tile, width = queries.shape
    held = (len(blocks),) + blocks[0].shape
    pairs = parts * tile * held[0] * held[1] * width // HEAD_DIM // 2
    return pl.pallas_call(
        attend_kernel,
        out_shape=jax.ShapeDtypeStruct(queries.shape, jnp.bfloat16),
        grid_spec=pltpu.PrefetchScalarGridSpec(
            num_scalar_prefetch=1,
            grid=(parts,),
            in_specs=[
                pl.BlockSpec((1, tile, width), lambda c, tops: (c, 0, 0)),
                pl.BlockSpec(memory_space=pltpu.VMEM),
            ]
            + [pl.BlockSpec(memory_space=pl.ANY)] * len(blocks),
            out_specs=pl.BlockSpec((1, tile, width), lambda c, tops: (c, 0, 0)),
            scratch_shapes=[
                pltpu.VMEM((width, tile), jnp.float32),
                pltpu.VMEM(held, blocks[0].dtype),
                pltpu.SemaphoreType.DMA((len(blocks),)),
            ],
        ),
        cost_estimate=pl.CostEstimate(
            flops=pairs * 1000, bytes_accessed=len(blocks) * blocks[0].size * 2, transcendentals=pairs * 3
        ),
        compiler_params=pltpu.CompilerParams(vmem_limit_bytes=58 * 1024 * 1024),
    )(tops, queries, bias, *blocks)


def gather_blocks(own, count):
    ring = count // PAIR
    swap = [(i, i // PAIR * PAIR + (i + 1) % PAIR) for i in range(count)]
    ahead = [(i, (i + PAIR) % count) for i in range(count)]
    behind = [(j, i) for i, j in ahead]
    near = [own, lax.ppermute(own, "ep", swap)]
    far = {}
    for member in range(PAIR):
        reach = (ring - 1 + (member == 0)) // 2
        held = near[member]
        for step in range(1, reach + 1):
            held = lax.ppermute(held, "ep", ahead)
            far[step, member] = held
        held = near[member]
        for step in range(ring - 1, reach, -1):
            held = lax.ppermute(held, "ep", behind)
            far[step, member] = held
    return near + [far[step, member] for step in range(1, ring) for member in range(PAIR)]


def expand(arrived, gate_weights, up_weights):
    gate_in = jnp.einsum(
        "necm,emf->necf", arrived, gate_weights, preferred_element_type=jnp.float32
    )
    up_in = jnp.einsum("necm,emf->necf", arrived, up_weights, preferred_element_type=jnp.float32)
    return (jax.nn.silu(gate_in) * up_in).astype(jnp.bfloat16)


def contract(hidden, down_weights):
    return jnp.einsum("necf,efm->necm", hidden, down_weights, preferred_element_type=jnp.float32)


def local(
    query_rows,
    key_rows,
    value_rows,
    key_bias,
    out_weight,
    moe_input,
    moe_gain,
    expert_pick,
    route_weight,
    w_gate,
    w_up,
    w_down,
):
    block_rows = query_rows.shape[0]
    half_rows = block_rows // 2
    ep_index = lax.axis_index("ep")
    ep_count = lax.axis_size("ep")
    own_kv = jnp.concatenate([key_rows, value_rows], axis=1)
    mirror = [(i, ep_count - 1 - i) for i in range(ep_count)]
    far_query = lax.ppermute(query_rows[half_rows:], "ep", mirror)
    blocks = gather_blocks(own_kv, ep_count)
    tops = jnp.stack(
        [2 * ep_index, 2 * (ep_count - 1 - ep_index) + 1, ep_index]
    ).astype(jnp.int32)
    near, far = attend(
        tops, jnp.stack([query_rows[:half_rows], far_query]), blocks, key_bias
    )
    attended = jnp.concatenate([near, lax.ppermute(far, "ep", mirror)], axis=0)
    mixer_out = lax.psum_scatter(
        jnp.dot(attended, out_weight, preferred_element_type=jnp.float32).astype(jnp.bfloat16),
        "tp",
        scatter_dimension=0,
        tiled=True,
    )
    token_count = moe_input.shape[0]
    widened = moe_input.astype(jnp.float32)
    normed = (
        widened
        * lax.rsqrt(jnp.mean(widened * widened, axis=1, keepdims=True) + norm_eps)
        * moe_gain
    ).astype(jnp.bfloat16)
    local_experts = w_gate.shape[0]
    expert_total = local_experts * ep_count
    capacity = GROUPS * token_count // expert_total
    picks = expert_pick.reshape(-1)
    matches = (picks[:, None] == jnp.arange(expert_total, dtype=jnp.int32)[None, :]).astype(
        jnp.int32
    )
    ranks = jnp.sum((jnp.cumsum(matches, axis=0) - matches) * matches, axis=1)
    slots = picks * capacity + ranks
    owners = jnp.arange(picks.shape[0], dtype=jnp.int32) // TOPK
    table = jnp.full((expert_total * capacity,), token_count, jnp.int32).at[slots].set(owners)
    padded = jnp.concatenate([normed, jnp.zeros((1, normed.shape[1]), jnp.bfloat16)], axis=0)
    outgoing = padded[table].reshape(ep_count, local_experts, capacity, normed.shape[1])
    outgoing = lax.optimization_barrier((outgoing, far_query, *blocks))[0]
    arrived = lax.all_to_all(outgoing, "ep", split_axis=0, concat_axis=0, tiled=True)
    gate_all, up_all, down_all = (
        lax.all_gather(w_gate, "tp", axis=2, tiled=True),
        lax.all_gather(w_up, "tp", axis=2, tiled=True),
        lax.all_gather(w_down, "tp", axis=1, tiled=True),
    )
    served = contract(expand(arrived, gate_all, up_all), down_all).astype(jnp.bfloat16)
    returned = lax.all_to_all(served, "ep", split_axis=0, concat_axis=0, tiled=True)
    flat = returned.reshape(expert_total * capacity, returned.shape[3])
    chosen = flat[slots].reshape(token_count, TOPK, flat.shape[1]).astype(jnp.float32)
    routed_out = jnp.sum(chosen * route_weight[:, :, None], axis=1).astype(jnp.bfloat16)
    return (mixer_out, routed_out)


MESH = pl.DeviceIdType.MESH
CHUNKS = 8


def remote(src, dst, send, recv, device):
    return pltpu.make_async_remote_copy(
        src_ref=src,
        dst_ref=dst,
        send_sem=send,
        recv_sem=recv,
        device_id=device,
        device_id_type=MESH,
    )


def split_parts(values):
    high = values.astype(jnp.bfloat16).astype(jnp.float32)
    rest = values - high
    middle = rest.astype(jnp.bfloat16).astype(jnp.float32)
    return high, middle, rest - middle


def fused_kernel(
    q_hbm,
    k_hbm,
    v_hbm,
    bias_hbm,
    out_weight_ref,
    moe_hbm,
    gain_hbm,
    pick_hbm,
    route_hbm,
    gate_ref,
    up_ref,
    down_ref,
    mixer_ref,
    routed_ref,
    q_ref,
    k_ref,
    v_ref,
    bias_ref,
    moe_ref,
    gain_ref,
    pick_ref,
    route_ref,
    q_send,
    q_recv,
    kv_send,
    kv_recv,
    keys,
    scores_buf,
    won,
    weights,
    acc,
    att_send,
    att_recv,
    project,
    mix_send,
    mix_recv,
    rows_send,
    rows_recv,
    placed,
    gate_all,
    up_all,
    down_all,
    hidden,
    part_send,
    part_recv,
    part_own,
    back_send,
    back_recv,
    local_sem,
    over_send,
    over_recv,
    die_send,
    die_recv,
    pass_send,
    pass_recv,
    project_send,
    project_recv,
    q_out,
    q_in,
    kv_out,
    kv_pass,
    kv_in,
    rows_out,
    rows_pass,
    rows_in,
    att_out,
    att_in,
    mix_out,
    mix_in,
    part_out,
    part_in,
    back_out,
    back_in,
    fetch_sem,
):
    ep_count = q_recv.shape[0]
    lines = ep_count // PAIR
    e, t = lax.axis_index("ep"), lax.axis_index("tp")
    z, y = lax.div(e, PAIR), lax.rem(e, PAIR)
    chip, core = lax.div(t, PAIR), lax.rem(t, PAIR)
    die = PAIR * chip + 1 - core
    over = PAIR * (1 - chip) + core
    across = PAIR * (1 - chip) + 1 - core
    side = PAIR * z + 1 - y
    block_rows, width = q_ref.shape
    half = block_rows // PAIR
    quarter = half // PAIR
    tokens, model = moe_ref.shape
    slots = rows_send.shape[1]
    shard = gate_ref.shape[2]
    span = model // CHUNKS

    upper = lax.div(z, PAIR)
    inner = lax.rem(z + upper, PAIR)

    def nearest(order):
        away = (1 + 2 * inner, 2 - inner, 3 - inner)[order]
        return lax.rem(z + away + upper * (2 * lines - 2 * away), lines)

    fetches = [
        pltpu.make_async_copy(src, dst, fetch_sem.at[i])
        for i, (src, dst) in enumerate(
            (
                (k_hbm, k_ref),
                (v_hbm, v_ref),
                (q_hbm, q_ref),
                (moe_hbm, moe_ref),
                (gain_hbm, gain_ref),
                (pick_hbm, pick_ref),
                (route_hbm, route_ref),
                (bias_hbm, bias_ref),
            )
        )
    ]
    for copy in fetches:
        copy.start()

    barrier = pltpu.get_barrier_semaphore()
    for step in range(1, ep_count):
        for other in range(PAIR):
            pl.semaphore_signal(
                barrier,
                inc=1,
                device_id=(lax.rem(e + step, ep_count), PAIR * chip + other),
                device_id_type=MESH,
            )
    for other in (die, over):
        pl.semaphore_signal(barrier, inc=1, device_id=(e, other), device_id_type=MESH)

    pieces = []
    own_rows = pl.ds(pl.multiple_of(t * shard, shard), shard)
    pieces.append((gate_ref.at[0], gate_all.at[t]))
    pieces.append((up_ref.at[0], up_all.at[t]))
    for chunk in range(CHUNKS):
        pieces.append(
            (
                down_ref.at[0, :, chunk * span : (chunk + 1) * span],
                down_all.at[chunk, own_rows, :],
            )
        )

    def held(index, owner):
        if index == 0:
            return gate_all.at[owner]
        if index == 1:
            return up_all.at[owner]
        rows = pl.ds(pl.multiple_of(owner * shard, shard), shard)
        return down_all.at[index - 2, rows, :]

    project_rows = pl.ds(pl.multiple_of(core * width, width), width)
    die_rows = pl.ds(pl.multiple_of((1 - core) * width, width), width)
    locals_ = [
        pltpu.make_async_copy(src, dst, local_sem.at[i]) for i, (src, dst) in enumerate(pieces)
    ]
    locals_.append(
        pltpu.make_async_copy(out_weight_ref, project.at[project_rows, :], local_sem.at[len(pieces)])
    )
    for copy in locals_:
        copy.start()

    for copy in fetches:
        copy.wait()
    keys_turned = jnp.transpose(k_ref[...].astype(jnp.float32)).astype(jnp.bfloat16)
    values_turned = jnp.transpose(v_ref[...].astype(jnp.float32)).astype(jnp.bfloat16)
    for h in range(lines):
        span_h = slice(h * HEAD_DIM, (h + 1) * HEAD_DIM)
        kv_send[h, :HEAD_DIM, :] = keys_turned[span_h, :]
        kv_send[h, HEAD_DIM:, :] = values_turned[span_h, :]
    q_turned = jnp.transpose(q_ref[...].astype(jnp.float32) * HEAD_DIM ** (-0.5))
    for h in range(lines):
        q_send[h] = q_turned[h * HEAD_DIM : (h + 1) * HEAD_DIM, :].astype(jnp.bfloat16)
    pl.semaphore_wait(barrier, PAIR * (ep_count - 1) + 2)

    pending = []
    for i, (src, dst) in enumerate(pieces):
        copy = remote(src, dst, over_send.at[i], over_recv.at[i], (e, over))
        copy.start()
        pending.append(copy)
    copy = remote(kv_send.at[z], kv_recv.at[e], kv_pass.at[z], kv_in.at[e], (side, t))
    copy.start()
    pending.append(copy)

    def send_queries(head, column, index):
        lanes = pl.ds(pl.multiple_of(lax.rem(column + e, PAIR) * half, half), half)
        return remote(
            q_send.at[head, :, lanes],
            q_recv.at[e, :HEAD_DIM, :],
            q_out.at[index],
            q_in.at[e],
            (PAIR * head + column, t),
        )

    for order in range(lines - 1):
        there = nearest(order)
        copies = [
            remote(
                kv_send.at[there], kv_recv.at[e], kv_out.at[order], kv_in.at[e], (PAIR * there + y, t)
            )
        ]
        copies += [send_queries(there, column, PAIR * (order + 1) + column) for column in range(PAIR)]
        for copy in copies:
            copy.start()
        pending += copies
    copy = send_queries(z, 1 - y, 0)
    copy.start()
    pending.append(copy)
    kv_recv[e] = kv_send[z]
    ones_at = lax.broadcasted_iota(jnp.int32, (HEAD_DIM, half), 0) < 3
    ones_rows = jnp.where(ones_at, 1.0, 0.0).astype(jnp.bfloat16)
    for i in range(ep_count):
        q_recv[i, HEAD_DIM:, :] = ones_rows
    own_lanes = pl.ds(pl.multiple_of(lax.rem(y + e, PAIR) * half, half), half)
    q_recv[e, :HEAD_DIM, :] = q_send[z, :, own_lanes]

    for i, (src, dst) in enumerate(pieces):
        copy = remote(src, dst, die_send.at[i], die_recv.at[i], (e, die))
        copy.start()
        pending.append(copy)
    copy = remote(
        out_weight_ref, project.at[project_rows, :], project_send, project_recv, (e, die)
    )
    copy.start()
    pending.append(copy)

    widened = moe_ref[...].astype(jnp.float32)
    normed = (
        widened
        * lax.rsqrt(jnp.mean(widened * widened, axis=1, keepdims=True) + norm_eps)
        * gain_ref[...]
    ).astype(jnp.bfloat16)
    group_row = lax.shift_right_logical(pick_ref[0:1, :], 1)
    groups = lines
    group_at = lax.broadcasted_iota(jnp.int32, (8, tokens), 0)
    chosen = (group_at == group_row).astype(jnp.float32)
    earlier = (
        lax.broadcasted_iota(jnp.int32, (tokens, tokens), 0)
        < lax.broadcasted_iota(jnp.int32, (tokens, tokens), 1)
    ).astype(jnp.float32)
    ranks = jnp.dot(
        chosen.astype(jnp.bfloat16),
        earlier.astype(jnp.bfloat16),
        preferred_element_type=jnp.float32,
    )
    slot_row = jnp.sum(
        chosen * (ranks + group_at.astype(jnp.float32) * slots), axis=0, keepdims=True
    )
    slot_at = lax.broadcasted_iota(jnp.int32, (groups * slots, tokens), 0)
    picked = (slot_at == slot_row.astype(jnp.int32)).astype(jnp.float32)
    placed[...] = jnp.transpose(picked).astype(jnp.bfloat16)
    first_low = (pick_ref[0:1, :] & 1) == 0
    low_row = jnp.where(first_low, route_ref[0:1, :], route_ref[1:2, :])
    high_row = jnp.where(first_low, route_ref[1:2, :], route_ref[0:1, :])
    low = split_parts(jnp.sum(picked * low_row, axis=1, keepdims=True))
    high = split_parts(jnp.sum(picked * high_row, axis=1, keepdims=True))
    lane = lax.broadcasted_iota(jnp.int32, (groups * slots, 128), 1)
    shares = jnp.zeros((groups * slots, 128), jnp.float32)
    for i, part in enumerate(low + high):
        shares = jnp.where(lane == i, part, shares)
    rows_send[:, :, model:] = shares.astype(jnp.bfloat16).reshape(groups, slots, 128)
    picked = picked.astype(jnp.bfloat16)
    for first in range(0, model, span):
        rows_send[:, :, first : first + span] = (
            jnp.dot(picked, normed[:, first : first + span], preferred_element_type=jnp.float32)
            .astype(jnp.bfloat16)
            .reshape(groups, slots, span)
        )
    home = y * lines + z
    rows_recv[home] = rows_send[z]

    def send_rows(order):
        there = nearest(order)
        return remote(
            rows_send.at[there],
            rows_recv.at[home],
            rows_out.at[order],
            rows_in.at[home],
            (PAIR * there + y, t),
        )

    for order in range(lines - 1):
        send_rows(order).start()

    def send_own_rows():
        return remote(
            rows_send.at[z], rows_recv.at[home], rows_pass.at[z], rows_in.at[home], (side, t)
        )

    def arrived_keys(source):
        arrived = kv_recv.at[source]
        return remote(
            arrived, arrived, kv_pass.at[lax.div(source, PAIR)], kv_in.at[source], (side, t)
        )

    def pass_keys(pair):
        @pl.when(pair != z)
        def _():
            copy = arrived_keys(PAIR * pair + y)
            copy.wait_recv()
            copy.start()

    head_at = lax.broadcasted_iota(jnp.int32, (lines, block_rows), 0)
    aug_at = lax.broadcasted_iota(jnp.int32, (HEAD_DIM, block_rows), 0)

    def ready(i):
        @pl.when(i != e)
        def _():
            arrived = q_recv.at[i, :HEAD_DIM, :]
            remote(arrived, arrived, q_out.at[0], q_in.at[i], (side, t)).wait_recv()

        rows = pl.ds(pl.multiple_of(i * block_rows, block_rows), block_rows)
        bias = jnp.sum(
            jnp.where(head_at == z, bias_ref[:, rows], 0.0), axis=0, keepdims=True
        )
        extra = jnp.zeros((HEAD_DIM, block_rows), jnp.float32)
        for place, part in enumerate(split_parts(bias)):
            extra = jnp.where(aug_at == place, part, extra)
        stacked = jnp.concatenate([kv_recv[i, :HEAD_DIM, :].astype(jnp.float32), extra], axis=0)
        keys[rows, :] = jnp.transpose(stacked).astype(jnp.bfloat16)

    key_at = lax.broadcasted_iota(jnp.int32, (half, half), 0)
    query_at = lax.broadcasted_iota(jnp.int32, (half, half), 1)
    later = jnp.where(key_at < query_at, 1.0, 0.0).astype(jnp.bfloat16)

    def score(block, queries):
        for sub in range(PAIR):
            rows = pl.ds(pl.multiple_of(block * block_rows + sub * half, half), half)
            scores_buf[sub] = jnp.dot(keys[rows, :], queries, preferred_element_type=jnp.float32)

    def gather_values(block):
        acc[...] += jnp.dot(
            kv_recv[block, HEAD_DIM:, :], weights[...], preferred_element_type=jnp.float32
        )

    def visit(following, queries, running, place):
        firsts, afters = {}, {}
        for sub in range(PAIR - 1, -1, -1):
            scores = scores_buf[sub]
            lost = jnp.maximum(scores, jnp.log(1.0 + jnp.exp(jnp.minimum(scores, 80.0))))
            won[sub] = scores - lost
            if place is not None:
                lost = jnp.where(key_at - query_at < (place - sub) * half, lost, 0.0)
            lost = lost.astype(jnp.bfloat16)
            firsts[sub] = lost[0:1, :].astype(jnp.float32)
            afters[sub] = jnp.dot(later, lost, preferred_element_type=jnp.float32)
        score(following, queries)
        for sub in range(PAIR - 1, -1, -1):
            weight = jnp.exp(won[sub] - (afters[sub] + running))
            if place is not None:
                weight = jnp.where(key_at - query_at < (place - sub) * half, weight, 0.0)
            weights[sub * half : (sub + 1) * half, :] = weight.astype(jnp.bfloat16)
            running = running + afters[sub][0:1, :] + firsts[sub]
        return running

    def send_attended(i, other):
        place = lax.rem(y + i, PAIR)
        return remote(
            att_send.at[i, :, other * quarter : (other + 1) * quarter],
            att_recv.at[
                pl.ds(pl.multiple_of(core * width + z * HEAD_DIM, HEAD_DIM), HEAD_DIM),
                pl.ds(pl.multiple_of(place * quarter, quarter), quarter),
            ],
            att_out.at[i, other],
            att_in.at[core, e],
            (i, PAIR * chip + other),
        )

    def wait_rows(place):
        arrived = rows_recv.at[place]
        remote(arrived, arrived, rows_out.at[0], rows_in.at[place], (side, t)).wait_recv()

    def pass_rows(order):
        there = nearest(order)
        place = y * lines + there
        arrived = rows_recv.at[place]
        return remote(arrived, arrived, rows_pass.at[there], rows_in.at[place], (side, t))

    def pass_rows_on(order):
        wait_rows(y * lines + nearest(order))
        pass_rows(order).start()

    def one_tile(i, _):
        pair = lax.div(i, PAIR)

        @pl.when(lax.rem(i, PAIR) == 0)
        def _():
            arrived_keys(i + 1 - y).wait_recv()
            ready(i)
            ready(i + 1)

        @pl.when(jnp.logical_and(lax.rem(i, PAIR) == 1, i < ep_count - 1))
        def _():
            pass_keys(pair + 1)

        @pl.when(i == PAIR)
        def _():
            send_own_rows().start()

        for order in range(lines - 2):

            @pl.when(jnp.logical_and(i == lines + PAIR * order, inner >= order))
            def _():
                pass_rows_on(order)

        place = lax.rem(y + i, PAIR)
        queries = q_recv[i]
        acc[...] = jnp.zeros_like(acc)
        score(i, queries)
        running = visit(
            jnp.maximum(i - 1, 0), queries, jnp.zeros((1, half), jnp.float32), place
        )

        def next_block(s, running):
            gather_values(i - s)
            return visit(jnp.maximum(i - 2 - s, 0), queries, running, None)

        lax.fori_loop(0, i, next_block, running)
        gather_values(0)
        att_send[i] = acc[...].astype(jnp.bfloat16)
        for other in range(PAIR):
            here = jnp.logical_and(i == e, core == other)

            @pl.when(jnp.logical_not(here))
            def _():
                send_attended(i, other).start()

            @pl.when(here)
            def _():
                att_recv[
                    pl.ds(pl.multiple_of(core * width + z * HEAD_DIM, HEAD_DIM), HEAD_DIM),
                    pl.ds(pl.multiple_of(place * quarter, quarter), quarter),
                ] = att_send[i, :, other * quarter : (other + 1) * quarter]

        return 0

    pass_keys(0)
    lax.fori_loop(0, ep_count, one_tile, 0)

    @pl.when(inner == 0)
    def _():
        pass_rows_on(1)

    pass_rows_on(lines - 2)

    def pass_on(index):
        arrived = held(index, over)
        remote(arrived, arrived, over_send.at[index], over_recv.at[index], (e, over)).wait_recv()
        copy = remote(arrived, arrived, pass_send.at[index], pass_recv.at[index], (e, die))
        copy.start()
        pending.append(copy)

    def wait_die(index):
        arrived = held(index, die)
        remote(arrived, arrived, die_send.at[index], die_recv.at[index], (e, die)).wait_recv()

    def wait_across(index):
        arrived = held(index, across)
        remote(arrived, arrived, pass_send.at[index], pass_recv.at[index], (e, die)).wait_recv()

    def serve(owner, column):
        hidden_lanes = pl.ds(pl.multiple_of(owner * shard, shard), shard)
        rows = rows_recv[pl.ds(column * lines, lines), :, :model].reshape(lines * slots, model)
        gate_in = jnp.dot(rows, gate_all[owner], preferred_element_type=jnp.float32)
        up_in = jnp.dot(rows, up_all[owner], preferred_element_type=jnp.float32)
        target = pl.ds(pl.multiple_of(column * lines * slots, lines * slots), lines * slots)
        hidden[target, hidden_lanes] = (gate_in / (1.0 + jnp.exp(-gate_in)) * up_in).astype(
            jnp.bfloat16
        )

    def serve_all(column, first, last):
        def one(k, _):
            serve(PAIR * lax.rem(chip + lax.div(k, PAIR), PAIR) + lax.rem(core + k, PAIR), column)
            return 0

        lax.fori_loop(first, last, one, 0)

    pass_on(0)
    for copy in locals_:
        copy.wait()
    wait_die(0)
    wait_die(1)
    serve_all(y, 0, PAIR)
    pass_on(1)
    wait_across(0)
    wait_across(1)
    serve_all(y, PAIR, 2 * PAIR)
    for i in range(lines):
        wait_rows((1 - y) * lines + i)
    pass_on(2)
    serve_all(1 - y, 0, 2 * PAIR)

    def mix():
        for source_core in range(PAIR):
            for i in range(ep_count):

                @pl.when(jnp.logical_not(jnp.logical_and(core == source_core, e == i)))
                def _():
                    first = source_core * width + i // PAIR * HEAD_DIM
                    place = lax.rem(i % PAIR + e, PAIR)
                    lanes = pl.ds(pl.multiple_of(place * quarter, quarter), quarter)
                    arrived = att_recv.at[first : first + HEAD_DIM, lanes]
                    remote(
                        arrived, arrived, att_out.at[0, 0], att_in.at[source_core, i], (side, t)
                    ).wait_recv()

        arrived = project.at[die_rows, :]
        remote(arrived, arrived, project_send, project_recv, (e, die)).wait_recv()

        def mixed(which):
            lanes = pl.ds(pl.multiple_of(which * quarter, quarter), quarter)
            attended = jnp.transpose(att_recv[:, lanes].astype(jnp.float32)).astype(jnp.bfloat16)
            return jnp.dot(attended, project[...], preferred_element_type=jnp.float32).astype(
                jnp.bfloat16
            )

        mix_send[...] = mixed(1 - chip)
        copy = remote(mix_send, mix_recv, mix_out, mix_in, (e, over))
        copy.start()
        pending.append(copy)
        mixer_ref[...] = mixed(chip)

    share_lane = lax.broadcasted_iota(jnp.int32, (lines * slots, 128), 1)
    share_here = jnp.logical_and(share_lane >= 3 * y, share_lane < 3 * y + 3)

    def contract(chunk, which):
        rows = pl.ds(pl.multiple_of(which * lines * slots, lines * slots), lines * slots)
        shares = rows_recv[pl.ds(which * lines, lines), :, model:].reshape(lines * slots, 128)
        share = jnp.sum(
            jnp.where(share_here, shares.astype(jnp.float32), 0.0), axis=1, keepdims=True
        )
        return (
            jnp.dot(hidden[rows, :], down_all[chunk], preferred_element_type=jnp.float32) * share
        )

    def give_back(chunk):
        arrived = part_recv.at[chunk]
        remote(arrived, arrived, part_out.at[chunk], part_in.at[chunk], (side, t)).wait_recv()
        total = part_own[chunk] + part_recv[chunk].astype(jnp.float32)
        back_send[chunk] = total.astype(jnp.bfloat16).reshape(lines, slots, span)
        for order in range(lines - 1):
            there = nearest(order)
            copy = remote(
                back_send.at[chunk, there],
                back_recv.at[chunk, z],
                back_out.at[chunk, order],
                back_in.at[chunk, z],
                (PAIR * there + y, t),
            )
            copy.start()
            pending.append(copy)
        back_recv[chunk, z] = back_send[chunk, z]

    for chunk in range(CHUNKS):
        if chunk + 1 < CHUNKS:
            pass_on(3 + chunk)
        wait_die(2 + chunk)
        wait_across(2 + chunk)
        part_send[chunk] = contract(chunk, 1 - y).astype(jnp.bfloat16)
        copy = remote(
            part_send.at[chunk],
            part_recv.at[chunk],
            part_out.at[chunk],
            part_in.at[chunk],
            (side, t),
        )
        copy.start()
        pending.append(copy)
        part_own[chunk] = contract(chunk, y)
        if chunk > 0:
            give_back(chunk - 1)
        if chunk == CHUNKS // 2:
            mix()
    give_back(CHUNKS - 1)

    remote(mix_send, mix_recv, mix_out, mix_in, (e, over)).wait_recv()
    mixer_ref[...] = (
        mixer_ref[...].astype(jnp.float32) + mix_recv[...].astype(jnp.float32)
    ).astype(jnp.bfloat16)

    for chunk in range(CHUNKS):
        for step in range(1, lines):
            there = lax.rem(z + step, lines)
            arrived = back_recv.at[chunk, there]
            remote(
                arrived, arrived, back_out.at[chunk, 0], back_in.at[chunk, there], (side, t)
            ).wait_recv()
        routed_ref[:, chunk * span : (chunk + 1) * span] = jnp.dot(
            placed[...],
            back_recv[chunk].reshape(groups * slots, span),
            preferred_element_type=jnp.float32,
        ).astype(jnp.bfloat16)

    for copy in pending:
        copy.wait_send()
    for order in range(lines - 1):
        send_rows(order).wait_send()
        pass_rows(order).wait_send()
    send_own_rows().wait_send()
    for i in range(lines):

        @pl.when(z != i)
        def _():
            arrived_keys(PAIR * i + y).wait_send()

    def drain(i, _):
        for other in range(PAIR):

            @pl.when(jnp.logical_not(jnp.logical_and(i == e, core == other)))
            def _():
                send_attended(i, other).wait_send()

        return 0

    lax.fori_loop(0, ep_count, drain, 0)


def fused(
    query_rows,
    key_rows,
    value_rows,
    key_bias,
    out_weight,
    moe_input,
    moe_gain,
    expert_pick,
    route_weight,
    w_gate,
    w_up,
    w_down,
):
    ep_count = lax.axis_size("ep")
    tp_count = lax.axis_size("tp")
    lines = ep_count // PAIR
    block_rows, width = query_rows.shape
    half = block_rows // PAIR
    quarter = half // PAIR
    tokens, model = moe_input.shape
    slots = GROUPS * tokens // (w_gate.shape[0] * ep_count)
    shard = w_gate.shape[2]
    span = model // CHUNKS
    bf16, f32 = jnp.bfloat16, jnp.float32
    dma = pltpu.SemaphoreType.DMA
    vmem = pltpu.VMEM
    operands = (
        query_rows,
        key_rows,
        value_rows,
        jnp.transpose(key_bias),
        out_weight,
        moe_input,
        moe_gain.reshape(1, model),
        jnp.transpose(expert_pick),
        jnp.transpose(route_weight),
        w_gate,
        w_up,
        w_down,
    )
    fetched = operands[:4] + operands[5:9]
    scratch = [vmem(array.shape, array.dtype) for array in fetched] + [
        vmem((lines, HEAD_DIM, block_rows), bf16),
        vmem((ep_count, 2 * HEAD_DIM, half), bf16),
        vmem((lines, 2 * HEAD_DIM, block_rows), bf16),
        vmem((ep_count, 2 * HEAD_DIM, block_rows), bf16),
        vmem((ep_count * block_rows, 2 * HEAD_DIM), bf16),
        vmem((PAIR, half, half), f32),
        vmem((PAIR, half, half), f32),
        vmem((block_rows, half), bf16),
        vmem((HEAD_DIM, half), f32),
        vmem((ep_count, HEAD_DIM, half), bf16),
        vmem((PAIR * width, half), bf16),
        vmem((PAIR * width, model), bf16),
        vmem((quarter, model), bf16),
        vmem((quarter, model), bf16),
        vmem((lines, slots, model + 128), bf16),
        vmem((ep_count, slots, model + 128), bf16),
        vmem((tokens, lines * slots), bf16),
        vmem((tp_count, model, shard), bf16),
        vmem((tp_count, model, shard), bf16),
        vmem((CHUNKS, tp_count * shard, span), bf16),
        vmem((ep_count * slots, tp_count * shard), bf16),
        vmem((CHUNKS, lines * slots, span), bf16),
        vmem((CHUNKS, lines * slots, span), bf16),
        vmem((CHUNKS, lines * slots, span), f32),
        vmem((CHUNKS, lines, slots, span), bf16),
        vmem((CHUNKS, lines, slots, span), bf16),
        dma((CHUNKS + 3,)),
        dma((CHUNKS + 2,)),
        dma((CHUNKS + 2,)),
        dma((CHUNKS + 2,)),
        dma((CHUNKS + 2,)),
        dma((CHUNKS + 2,)),
        dma((CHUNKS + 2,)),
        dma,
        dma,
        dma((ep_count,)),
        dma((ep_count,)),
        dma((lines,)),
        dma((lines,)),
        dma((ep_count,)),
        dma((lines,)),
        dma((lines,)),
        dma((ep_count,)),
        dma((ep_count, PAIR)),
        dma((PAIR, ep_count)),
        dma,
        dma,
        dma((CHUNKS,)),
        dma((CHUNKS,)),
        dma((CHUNKS, lines)),
        dma((CHUNKS, lines)),
        dma((len(fetched),)),
    ]
    in_hbm = pl.BlockSpec(memory_space=pltpu.HBM)
    in_vmem = pl.BlockSpec(memory_space=pltpu.VMEM)
    return pl.pallas_call(
        fused_kernel,
        out_shape=(
            vmem((quarter, model), bf16),
            vmem((tokens, model), bf16),
        ),
        in_specs=[in_hbm] * len(operands),
        out_specs=(in_vmem, in_vmem),
        scratch_shapes=scratch,
        compiler_params=pltpu.CompilerParams(
            collective_id=0, has_side_effects=True, vmem_limit_bytes=58 * 1024 * 1024
        ),
    )(*operands)


def fits(query_rows, w_gate):
    ep_count = lax.axis_size("ep")
    return (
        lax.axis_size("tp") == PAIR * PAIR
        and TOPK == PAIR
        and w_gate.shape[0] == 1
        and ep_count == GROUPS * TOPK
        and query_rows.shape[1] == GROUPS * HEAD_DIM
    )


def step(*args):
    return (fused if fits(args[0], args[9]) else local)(*args)


def solution(mesh):
    placed = (
        P("ep", "tp"),
        P("ep", "tp"),
        P("ep", "tp"),
        P(None, "tp"),
        P("tp", None),
        P(("ep", "tp"), None),
        P(),
        P(("ep", "tp"), None),
        P(("ep", "tp"), None),
        P("ep", None, "tp"),
        P("ep", None, "tp"),
        P("ep", "tp", None),
    )
    return jax.shard_map(
        step,
        mesh=mesh,
        in_specs=placed,
        out_specs=(P(("ep", "tp"), None), P(("ep", "tp"), None)),
        check_vma=False,
    )
```

```python
import jax
import jax.numpy as jnp
from jax import lax
from jax.experimental import pallas as pl
from jax.experimental.pallas import tpu as pltpu
from jax.sharding import PartitionSpec as P

HEAD_DIM = 64
GROUPS = 4
TOPK = 2
PAIR = 2


norm_eps = 1e-06


def attend_kernel(tops_ref, query_ref, bias_ref, *rest):
    block_refs = rest[:-4]
    out_ref, acc_ref, kv_ref, sems = rest[-4:]

    @pl.when(pl.program_id(0) == 0)
    def _():
        copies = [
            pltpu.make_async_copy(ref, kv_ref.at[slot], sems.at[slot])
            for slot, ref in enumerate(block_refs)
        ]
        for copy in copies:
            copy.start()
        for copy in copies:
            copy.wait()

    tile = query_ref.shape[1]
    width = query_ref.shape[2]
    heads = width // HEAD_DIM
    slots = kv_ref.shape[0]
    per_block = kv_ref.shape[1] // tile
    top = tops_ref[pl.program_id(0)]
    own = tops_ref[2]
    turned = jnp.transpose(query_ref[0].astype(jnp.float32) * HEAD_DIM ** (-0.5))
    row_head = lax.broadcasted_iota(jnp.int32, (width, tile), 0) // HEAD_DIM
    queries = [jnp.where(row_head == h, turned, 0.0).astype(jnp.bfloat16) for h in range(heads)]
    key_at = lax.broadcasted_iota(jnp.int32, (tile, tile), 0)
    query_at = lax.broadcasted_iota(jnp.int32, (tile, tile), 1)
    causal = key_at < query_at
    later = jnp.where(causal, 1.0, 0.0).astype(jnp.bfloat16)
    acc_ref[...] = jnp.zeros_like(acc_ref)

    def visit(index, running, masked):
        block = index // per_block
        away = lax.rem(own // PAIR - block // PAIR + slots // PAIR, slots // PAIR)
        slot = away * PAIR + lax.rem(own + block, PAIR)
        rows = pl.ds(pl.multiple_of((index - block * per_block) * tile, tile), tile)
        first = pl.multiple_of(index * tile, tile)
        keys = kv_ref[slot, rows, :width]
        values = jnp.transpose(kv_ref[slot, rows, width:])
        passed = []
        for h in range(heads):
            scores = jnp.dot(keys, queries[h], preferred_element_type=jnp.float32)
            scores = scores + bias_ref[pl.ds(first, tile), h : h + 1]
            tail = jnp.log(1.0 + jnp.exp(-jnp.abs(scores)))
            lost = jnp.maximum(scores, 0.0) + tail
            won = jnp.minimum(scores, 0.0) - tail
            if masked:
                lost = jnp.where(causal, lost, 0.0)
            lost = lost.astype(jnp.bfloat16)
            after = jnp.dot(later, lost, preferred_element_type=jnp.float32)
            weight = jnp.exp(won - (after + running[h]))
            if masked:
                weight = jnp.where(causal, weight, 0.0)
            span = slice(h * HEAD_DIM, (h + 1) * HEAD_DIM)
            acc_ref[span, :] += jnp.dot(
                values[span, :], weight.astype(jnp.bfloat16), preferred_element_type=jnp.float32
            )
            passed.append(running[h] + after[0:1, :] + lost[0:1, :].astype(jnp.float32))
        return tuple(passed)

    running = tuple(jnp.zeros((1, tile), jnp.float32) for _ in range(heads))
    running = visit(top, running, True)
    lax.fori_loop(0, top, lambda step, carried: visit(top - 1 - step, carried, False), running)
    out_ref[0] = jnp.transpose(acc_ref[...]).astype(jnp.bfloat16)


def attend(tops, queries, blocks, bias):
    parts, tile, width = queries.shape
    held = (len(blocks),) + blocks[0].shape
    pairs = parts * tile * held[0] * held[1] * width // HEAD_DIM // 2
    return pl.pallas_call(
        attend_kernel,
        out_shape=jax.ShapeDtypeStruct(queries.shape, jnp.bfloat16),
        grid_spec=pltpu.PrefetchScalarGridSpec(
            num_scalar_prefetch=1,
            grid=(parts,),
            in_specs=[
                pl.BlockSpec((1, tile, width), lambda c, tops: (c, 0, 0)),
                pl.BlockSpec(memory_space=pltpu.VMEM),
            ]
            + [pl.BlockSpec(memory_space=pl.ANY)] * len(blocks),
            out_specs=pl.BlockSpec((1, tile, width), lambda c, tops: (c, 0, 0)),
            scratch_shapes=[
                pltpu.VMEM((width, tile), jnp.float32),
                pltpu.VMEM(held, blocks[0].dtype),
                pltpu.SemaphoreType.DMA((len(blocks),)),
            ],
        ),
        cost_estimate=pl.CostEstimate(
            flops=pairs * 1000, bytes_accessed=len(blocks) * blocks[0].size * 2, transcendentals=pairs * 3
        ),
        compiler_params=pltpu.CompilerParams(vmem_limit_bytes=58 * 1024 * 1024),
    )(tops, queries, bias, *blocks)


def gather_blocks(own, count):
    ring = count // PAIR
    swap = [(i, i // PAIR * PAIR + (i + 1) % PAIR) for i in range(count)]
    ahead = [(i, (i + PAIR) % count) for i in range(count)]
    behind = [(j, i) for i, j in ahead]
    near = [own, lax.ppermute(own, "ep", swap)]
    far = {}
    for member in range(PAIR):
        reach = (ring - 1 + (member == 0)) // 2
        held = near[member]
        for step in range(1, reach + 1):
            held = lax.ppermute(held, "ep", ahead)
            far[step, member] = held
        held = near[member]
        for step in range(ring - 1, reach, -1):
            held = lax.ppermute(held, "ep", behind)
            far[step, member] = held
    return near + [far[step, member] for step in range(1, ring) for member in range(PAIR)]


def expand(arrived, gate_weights, up_weights):
    gate_in = jnp.einsum(
        "necm,emf->necf", arrived, gate_weights, preferred_element_type=jnp.float32
    )
    up_in = jnp.einsum("necm,emf->necf", arrived, up_weights, preferred_element_type=jnp.float32)
    return (jax.nn.silu(gate_in) * up_in).astype(jnp.bfloat16)


def contract(hidden, down_weights):
    return jnp.einsum("necf,efm->necm", hidden, down_weights, preferred_element_type=jnp.float32)


def local(
    query_rows,
    key_rows,
    value_rows,
    key_bias,
    out_weight,
    moe_input,
    moe_gain,
    expert_pick,
    route_weight,
    w_gate,
    w_up,
    w_down,
):
    block_rows = query_rows.shape[0]
    half_rows = block_rows // 2
    ep_index = lax.axis_index("ep")
    ep_count = lax.axis_size("ep")
    own_kv = jnp.concatenate([key_rows, value_rows], axis=1)
    mirror = [(i, ep_count - 1 - i) for i in range(ep_count)]
    far_query = lax.ppermute(query_rows[half_rows:], "ep", mirror)
    blocks = gather_blocks(own_kv, ep_count)
    tops = jnp.stack(
        [2 * ep_index, 2 * (ep_count - 1 - ep_index) + 1, ep_index]
    ).astype(jnp.int32)
    near, far = attend(
        tops, jnp.stack([query_rows[:half_rows], far_query]), blocks, key_bias
    )
    attended = jnp.concatenate([near, lax.ppermute(far, "ep", mirror)], axis=0)
    mixer_out = lax.psum_scatter(
        jnp.dot(attended, out_weight, preferred_element_type=jnp.float32).astype(jnp.bfloat16),
        "tp",
        scatter_dimension=0,
        tiled=True,
    )
    token_count = moe_input.shape[0]
    widened = moe_input.astype(jnp.float32)
    normed = (
        widened
        * lax.rsqrt(jnp.mean(widened * widened, axis=1, keepdims=True) + norm_eps)
        * moe_gain
    ).astype(jnp.bfloat16)
    local_experts = w_gate.shape[0]
    expert_total = local_experts * ep_count
    capacity = GROUPS * token_count // expert_total
    picks = expert_pick.reshape(-1)
    matches = (picks[:, None] == jnp.arange(expert_total, dtype=jnp.int32)[None, :]).astype(
        jnp.int32
    )
    ranks = jnp.sum((jnp.cumsum(matches, axis=0) - matches) * matches, axis=1)
    slots = picks * capacity + ranks
    owners = jnp.arange(picks.shape[0], dtype=jnp.int32) // TOPK
    table = jnp.full((expert_total * capacity,), token_count, jnp.int32).at[slots].set(owners)
    padded = jnp.concatenate([normed, jnp.zeros((1, normed.shape[1]), jnp.bfloat16)], axis=0)
    outgoing = padded[table].reshape(ep_count, local_experts, capacity, normed.shape[1])
    outgoing = lax.optimization_barrier((outgoing, far_query, *blocks))[0]
    arrived = lax.all_to_all(outgoing, "ep", split_axis=0, concat_axis=0, tiled=True)
    gate_all, up_all, down_all = (
        lax.all_gather(w_gate, "tp", axis=2, tiled=True),
        lax.all_gather(w_up, "tp", axis=2, tiled=True),
        lax.all_gather(w_down, "tp", axis=1, tiled=True),
    )
    served = contract(expand(arrived, gate_all, up_all), down_all).astype(jnp.bfloat16)
    returned = lax.all_to_all(served, "ep", split_axis=0, concat_axis=0, tiled=True)
    flat = returned.reshape(expert_total * capacity, returned.shape[3])
    chosen = flat[slots].reshape(token_count, TOPK, flat.shape[1]).astype(jnp.float32)
    routed_out = jnp.sum(chosen * route_weight[:, :, None], axis=1).astype(jnp.bfloat16)
    return (mixer_out, routed_out)


MESH = pl.DeviceIdType.MESH
CHUNKS = 8
AHEAD = 3


def remote(src, dst, send, recv, device):
    return pltpu.make_async_remote_copy(
        src_ref=src,
        dst_ref=dst,
        send_sem=send,
        recv_sem=recv,
        device_id=device,
        device_id_type=MESH,
    )


def split_parts(values):
    high = values.astype(jnp.bfloat16).astype(jnp.float32)
    rest = values - high
    middle = rest.astype(jnp.bfloat16).astype(jnp.float32)
    return high, middle, rest - middle


def fused_kernel(
    q_hbm,
    k_hbm,
    v_hbm,
    bias_hbm,
    out_weight_ref,
    moe_hbm,
    gain_hbm,
    pick_hbm,
    route_hbm,
    gate_ref,
    up_ref,
    down_ref,
    mixer_ref,
    routed_ref,
    q_ref,
    k_ref,
    v_ref,
    bias_ref,
    moe_ref,
    gain_ref,
    pick_ref,
    route_ref,
    q_send,
    q_recv,
    kv_send,
    kv_recv,
    keys,
    scores_buf,
    won,
    weights,
    acc,
    att_send,
    att_recv,
    project,
    mix_send,
    mix_recv,
    rows_send,
    rows_recv,
    placed,
    gate_all,
    up_all,
    down_all,
    hidden,
    part_send,
    part_recv,
    part_own,
    back_send,
    back_recv,
    local_sem,
    over_send,
    over_recv,
    die_send,
    die_recv,
    pass_send,
    pass_recv,
    project_send,
    project_recv,
    q_out,
    q_in,
    kv_out,
    kv_pass,
    kv_in,
    rows_out,
    rows_pass,
    rows_in,
    att_out,
    att_in,
    mix_out,
    mix_in,
    part_out,
    part_in,
    back_out,
    back_in,
    fetch_sem,
):
    ep_count = q_recv.shape[0]
    lines = ep_count // PAIR
    e, t = lax.axis_index("ep"), lax.axis_index("tp")
    z, y = lax.div(e, PAIR), lax.rem(e, PAIR)
    chip, core = lax.div(t, PAIR), lax.rem(t, PAIR)
    die = PAIR * chip + 1 - core
    over = PAIR * (1 - chip) + core
    across = PAIR * (1 - chip) + 1 - core
    side = PAIR * z + 1 - y
    block_rows, width = q_ref.shape
    half = block_rows // PAIR
    quarter = half // PAIR
    tokens, model = moe_ref.shape
    slots = rows_send.shape[1]
    shard = gate_ref.shape[2]
    span = model // CHUNKS

    upper = lax.div(z, PAIR)
    inner = lax.rem(z + upper, PAIR)

    def nearest(order):
        away = (1 + 2 * inner, 2 - inner, 3 - inner)[order]
        return lax.rem(z + away + upper * (2 * lines - 2 * away), lines)

    def rows_target(order):
        away = (1 + 2 * inner, 2, 3 - 2 * inner)[order]
        return lax.rem(z + away + upper * (2 * lines - 2 * away), lines)

    fetches = [
        pltpu.make_async_copy(src, dst, fetch_sem.at[i])
        for i, (src, dst) in enumerate(
            (
                (k_hbm, k_ref),
                (v_hbm, v_ref),
                (q_hbm, q_ref),
                (moe_hbm, moe_ref),
                (gain_hbm, gain_ref),
                (pick_hbm, pick_ref),
                (route_hbm, route_ref),
                (bias_hbm, bias_ref),
            )
        )
    ]
    for copy in fetches:
        copy.start()

    barrier = pltpu.get_barrier_semaphore()
    for step in range(1, ep_count):
        for other in range(PAIR):
            pl.semaphore_signal(
                barrier,
                inc=1,
                device_id=(lax.rem(e + step, ep_count), PAIR * chip + other),
                device_id_type=MESH,
            )
    for other in (die, over):
        pl.semaphore_signal(barrier, inc=1, device_id=(e, other), device_id_type=MESH)

    pieces = []
    own_rows = pl.ds(pl.multiple_of(t * shard, shard), shard)
    pieces.append((gate_ref.at[0], gate_all.at[t]))
    pieces.append((up_ref.at[0], up_all.at[t]))
    for chunk in range(CHUNKS):
        pieces.append(
            (
                down_ref.at[0, :, chunk * span : (chunk + 1) * span],
                down_all.at[chunk, own_rows, :],
            )
        )

    def held(index, owner):
        if index == 0:
            return gate_all.at[owner]
        if index == 1:
            return up_all.at[owner]
        rows = pl.ds(pl.multiple_of(owner * shard, shard), shard)
        return down_all.at[index - 2, rows, :]

    project_rows = pl.ds(pl.multiple_of(core * width, width), width)
    die_rows = pl.ds(pl.multiple_of((1 - core) * width, width), width)
    locals_ = [
        pltpu.make_async_copy(src, dst, local_sem.at[i]) for i, (src, dst) in enumerate(pieces)
    ]
    locals_.append(
        pltpu.make_async_copy(out_weight_ref, project.at[project_rows, :], local_sem.at[len(pieces)])
    )
    for copy in locals_:
        copy.start()

    for copy in fetches:
        copy.wait()
    keys_turned = jnp.transpose(k_ref[...].astype(jnp.float32)).astype(jnp.bfloat16)
    values_turned = jnp.transpose(v_ref[...].astype(jnp.float32)).astype(jnp.bfloat16)
    for h in range(lines):
        span_h = slice(h * HEAD_DIM, (h + 1) * HEAD_DIM)
        kv_send[h, :HEAD_DIM, :] = keys_turned[span_h, :]
        kv_send[h, HEAD_DIM:, :] = values_turned[span_h, :]
    q_turned = jnp.transpose(q_ref[...].astype(jnp.float32) * HEAD_DIM ** (-0.5))
    for h in range(lines):
        q_send[h] = q_turned[h * HEAD_DIM : (h + 1) * HEAD_DIM, :].astype(jnp.bfloat16)
    pl.semaphore_wait(barrier, PAIR * (ep_count - 1) + 2)

    pending = []
    for i, (src, dst) in enumerate(pieces):
        copy = remote(src, dst, over_send.at[i], over_recv.at[i], (e, over))
        copy.start()
        pending.append(copy)
    copy = remote(kv_send.at[z], kv_recv.at[e], kv_pass.at[z], kv_in.at[e], (side, t))
    copy.start()
    pending.append(copy)

    def send_queries(head, column, index):
        lanes = pl.ds(pl.multiple_of(lax.rem(column + e, PAIR) * half, half), half)
        return remote(
            q_send.at[head, :, lanes],
            q_recv.at[e, :HEAD_DIM, :],
            q_out.at[index],
            q_in.at[e],
            (PAIR * head + column, t),
        )

    for order in range(lines - 1):
        there = nearest(order)
        copies = [
            remote(
                kv_send.at[there], kv_recv.at[e], kv_out.at[order], kv_in.at[e], (PAIR * there + y, t)
            )
        ]
        copies += [send_queries(there, column, PAIR * (order + 1) + column) for column in range(PAIR)]
        for copy in copies:
            copy.start()
        pending += copies
    copy = send_queries(z, 1 - y, 0)
    copy.start()
    pending.append(copy)
    kv_recv[e] = kv_send[z]
    ones_at = lax.broadcasted_iota(jnp.int32, (HEAD_DIM, half), 0) < 3
    ones_rows = jnp.where(ones_at, 1.0, 0.0).astype(jnp.bfloat16)
    for i in range(ep_count):
        q_recv[i, HEAD_DIM:, :] = ones_rows
    own_lanes = pl.ds(pl.multiple_of(lax.rem(y + e, PAIR) * half, half), half)
    q_recv[e, :HEAD_DIM, :] = q_send[z, :, own_lanes]

    for i, (src, dst) in enumerate(pieces):
        copy = remote(src, dst, die_send.at[i], die_recv.at[i], (e, die))
        copy.start()
        pending.append(copy)
    copy = remote(
        out_weight_ref, project.at[project_rows, :], project_send, project_recv, (e, die)
    )
    copy.start()
    pending.append(copy)

    widened = moe_ref[...].astype(jnp.float32)
    normed = (
        widened
        * lax.rsqrt(jnp.mean(widened * widened, axis=1, keepdims=True) + norm_eps)
        * gain_ref[...]
    ).astype(jnp.bfloat16)
    group_row = lax.shift_right_logical(pick_ref[0:1, :], 1)
    groups = lines
    group_at = lax.broadcasted_iota(jnp.int32, (8, tokens), 0)
    chosen = (group_at == group_row).astype(jnp.float32)
    earlier = (
        lax.broadcasted_iota(jnp.int32, (tokens, tokens), 0)
        < lax.broadcasted_iota(jnp.int32, (tokens, tokens), 1)
    ).astype(jnp.float32)
    ranks = jnp.dot(
        chosen.astype(jnp.bfloat16),
        earlier.astype(jnp.bfloat16),
        preferred_element_type=jnp.float32,
    )
    slot_row = jnp.sum(
        chosen * (ranks + group_at.astype(jnp.float32) * slots), axis=0, keepdims=True
    )
    slot_at = lax.broadcasted_iota(jnp.int32, (groups * slots, tokens), 0)
    picked = (slot_at == slot_row.astype(jnp.int32)).astype(jnp.float32)
    placed[...] = jnp.transpose(picked).astype(jnp.bfloat16)
    first_low = (pick_ref[0:1, :] & 1) == 0
    low_row = jnp.where(first_low, route_ref[0:1, :], route_ref[1:2, :])
    high_row = jnp.where(first_low, route_ref[1:2, :], route_ref[0:1, :])
    low = split_parts(jnp.sum(picked * low_row, axis=1, keepdims=True))
    high = split_parts(jnp.sum(picked * high_row, axis=1, keepdims=True))
    lane = lax.broadcasted_iota(jnp.int32, (groups * slots, 128), 1)
    shares = jnp.zeros((groups * slots, 128), jnp.float32)
    for i, part in enumerate(low + high):
        shares = jnp.where(lane == i, part, shares)
    rows_send[:, :, model:] = shares.astype(jnp.bfloat16).reshape(groups, slots, 128)
    picked = picked.astype(jnp.bfloat16)
    for first in range(0, model, span):
        rows_send[:, :, first : first + span] = (
            jnp.dot(picked, normed[:, first : first + span], preferred_element_type=jnp.float32)
            .astype(jnp.bfloat16)
            .reshape(groups, slots, span)
        )
    home = y * lines + z
    rows_recv[home] = rows_send[z]

    def send_rows(order):
        there = rows_target(order)
        return remote(
            rows_send.at[there],
            rows_recv.at[home],
            rows_out.at[order],
            rows_in.at[home],
            (PAIR * there + y, t),
        )

    for order in range(lines - 1):
        send_rows(order).start()

    def send_own_rows():
        return remote(
            rows_send.at[z], rows_recv.at[home], rows_pass.at[z], rows_in.at[home], (side, t)
        )

    def arrived_keys(source):
        arrived = kv_recv.at[source]
        return remote(
            arrived, arrived, kv_pass.at[lax.div(source, PAIR)], kv_in.at[source], (side, t)
        )

    def pass_keys(pair):
        @pl.when(pair != z)
        def _():
            copy = arrived_keys(PAIR * pair + y)
            copy.wait_recv()
            copy.start()

    head_at = lax.broadcasted_iota(jnp.int32, (lines, block_rows), 0)
    aug_at = lax.broadcasted_iota(jnp.int32, (HEAD_DIM, block_rows), 0)

    def ready(i):
        @pl.when(i != e)
        def _():
            arrived = q_recv.at[i, :HEAD_DIM, :]
            remote(arrived, arrived, q_out.at[0], q_in.at[i], (side, t)).wait_recv()

        rows = pl.ds(pl.multiple_of(i * block_rows, block_rows), block_rows)
        bias = jnp.sum(
            jnp.where(head_at == z, bias_ref[:, rows], 0.0), axis=0, keepdims=True
        )
        extra = jnp.zeros((HEAD_DIM, block_rows), jnp.float32)
        for place, part in enumerate(split_parts(bias)):
            extra = jnp.where(aug_at == place, part, extra)
        stacked = jnp.concatenate([kv_recv[i, :HEAD_DIM, :].astype(jnp.float32), extra], axis=0)
        keys[rows, :] = jnp.transpose(stacked).astype(jnp.bfloat16)

    key_at = lax.broadcasted_iota(jnp.int32, (half, half), 0)
    query_at = lax.broadcasted_iota(jnp.int32, (half, half), 1)
    later = jnp.where(key_at < query_at, 1.0, 0.0).astype(jnp.bfloat16)

    def score(block, queries):
        for sub in range(PAIR):
            rows = pl.ds(pl.multiple_of(block * block_rows + sub * half, half), half)
            scores_buf[sub] = jnp.dot(keys[rows, :], queries, preferred_element_type=jnp.float32)

    def gather_values(block):
        acc[...] += jnp.dot(
            kv_recv[block, HEAD_DIM:, :], weights[...], preferred_element_type=jnp.float32
        )

    def visit(following, queries, running, place):
        firsts, afters = {}, {}
        for sub in range(PAIR - 1, -1, -1):
            scores = scores_buf[sub]
            lost = jnp.maximum(scores, jnp.log(1.0 + jnp.exp(jnp.minimum(scores, 80.0))))
            won[sub] = scores - lost
            if place is not None:
                lost = jnp.where(key_at - query_at < (place - sub) * half, lost, 0.0)
            lost = lost.astype(jnp.bfloat16)
            firsts[sub] = lost[0:1, :].astype(jnp.float32)
            afters[sub] = jnp.dot(later, lost, preferred_element_type=jnp.float32)
        score(following, queries)
        for sub in range(PAIR - 1, -1, -1):
            weight = jnp.exp(won[sub] - (afters[sub] + running))
            if place is not None:
                weight = jnp.where(key_at - query_at < (place - sub) * half, weight, 0.0)
            weights[sub * half : (sub + 1) * half, :] = weight.astype(jnp.bfloat16)
            running = running + afters[sub][0:1, :] + firsts[sub]
        return running

    def send_attended(i, other):
        place = lax.rem(y + i, PAIR)
        return remote(
            att_send.at[i, :, other * quarter : (other + 1) * quarter],
            att_recv.at[
                pl.ds(pl.multiple_of(core * width + z * HEAD_DIM, HEAD_DIM), HEAD_DIM),
                pl.ds(pl.multiple_of(place * quarter, quarter), quarter),
            ],
            att_out.at[i, other],
            att_in.at[core, e],
            (i, PAIR * chip + other),
        )

    def wait_rows(place):
        arrived = rows_recv.at[place]
        remote(arrived, arrived, rows_out.at[0], rows_in.at[place], (side, t)).wait_recv()

    def pass_rows(order):
        there = nearest(order)
        place = y * lines + there
        arrived = rows_recv.at[place]
        return remote(arrived, arrived, rows_pass.at[there], rows_in.at[place], (side, t))

    def pass_rows_on(order):
        wait_rows(y * lines + nearest(order))
        pass_rows(order).start()

    def pass_copy(index):
        arrived = held(index, over)
        return remote(arrived, arrived, pass_send.at[index], pass_recv.at[index], (e, die))

    def pass_on(index):
        arrived = held(index, over)
        remote(arrived, arrived, over_send.at[index], over_recv.at[index], (e, over)).wait_recv()
        pass_copy(index).start()

    def one_tile(i, _):
        pair = lax.div(i, PAIR)

        @pl.when(lax.rem(i, PAIR) == 0)
        def _():
            arrived_keys(i + 1 - y).wait_recv()
            ready(i)
            ready(i + 1)

        @pl.when(jnp.logical_and(lax.rem(i, PAIR) == 1, i < ep_count - 1))
        def _():
            pass_keys(pair + 1)

        @pl.when(i == PAIR)
        def _():
            send_own_rows().start()

        @pl.when(i == ep_count - PAIR - 1)
        def _():
            pass_on(0)

        for order in range(lines - 2):

            @pl.when(jnp.logical_and(i == lines + PAIR * order, inner * order == 0))
            def _():
                pass_rows_on(order)

        place = lax.rem(y + i, PAIR)
        queries = q_recv[i]
        acc[...] = jnp.zeros_like(acc)
        score(i, queries)
        running = visit(
            jnp.maximum(i - 1, 0), queries, jnp.zeros((1, half), jnp.float32), place
        )

        def next_block(s, running):
            gather_values(i - s)
            return visit(jnp.maximum(i - 2 - s, 0), queries, running, None)

        lax.fori_loop(0, i, next_block, running)
        gather_values(0)
        att_send[i] = acc[...].astype(jnp.bfloat16)
        for other in range(PAIR):
            here = jnp.logical_and(i == e, core == other)

            @pl.when(jnp.logical_not(here))
            def _():
                send_attended(i, other).start()

            @pl.when(here)
            def _():
                att_recv[
                    pl.ds(pl.multiple_of(core * width + z * HEAD_DIM, HEAD_DIM), HEAD_DIM),
                    pl.ds(pl.multiple_of(place * quarter, quarter), quarter),
                ] = att_send[i, :, other * quarter : (other + 1) * quarter]

        return 0

    pass_keys(0)
    lax.fori_loop(0, ep_count, one_tile, 0)

    def wait_die(index):
        arrived = held(index, die)
        remote(arrived, arrived, die_send.at[index], die_recv.at[index], (e, die)).wait_recv()

    def wait_across(index):
        arrived = held(index, across)
        remote(arrived, arrived, pass_send.at[index], pass_recv.at[index], (e, die)).wait_recv()

    def serve(owner, first, count):
        hidden_lanes = pl.ds(pl.multiple_of(owner * shard, shard), shard)
        rows = rows_recv[pl.ds(first, count), :, :model].reshape(count * slots, model)
        gate_in = jnp.dot(rows, gate_all[owner], preferred_element_type=jnp.float32)
        up_in = jnp.dot(rows, up_all[owner], preferred_element_type=jnp.float32)
        target = pl.ds(pl.multiple_of(first * slots, slots), count * slots)
        hidden[target, hidden_lanes] = (gate_in / (1.0 + jnp.exp(-gate_in)) * up_in).astype(
            jnp.bfloat16
        )

    def serve_all(first, count, start, stop):
        def one(k, _):
            owner = PAIR * lax.rem(chip + lax.div(k, PAIR), PAIR) + lax.rem(core + k, PAIR)
            serve(owner, first, count)
            return 0

        lax.fori_loop(start, stop, one, 0)

    own_first = y * lines
    early = (1 - y) * lines + PAIR * upper
    late = (1 - y) * lines + PAIR * (1 - upper)

    @pl.when(inner == 1)
    def _():
        pass_rows_on(1)

    pass_rows_on(lines - 2)
    pass_on(1)
    for copy in locals_:
        copy.wait()
    wait_die(0)
    wait_die(1)
    for i in range(PAIR):
        wait_rows(early + i)
    serve_all(early, PAIR, 0, PAIR)
    pass_on(2)
    serve_all(own_first, lines, 0, PAIR)
    serve_all(early, PAIR, PAIR, PAIR + 1)
    wait_across(0)
    wait_across(1)
    serve_all(early, PAIR, PAIR + 1, 2 * PAIR)

    def mix():
        for source_core in range(PAIR):
            for i in range(ep_count):

                @pl.when(jnp.logical_not(jnp.logical_and(core == source_core, e == i)))
                def _():
                    first = source_core * width + i // PAIR * HEAD_DIM
                    place = lax.rem(i % PAIR + e, PAIR)
                    lanes = pl.ds(pl.multiple_of(place * quarter, quarter), quarter)
                    arrived = att_recv.at[first : first + HEAD_DIM, lanes]
                    remote(
                        arrived, arrived, att_out.at[0, 0], att_in.at[source_core, i], (side, t)
                    ).wait_recv()

        arrived = project.at[die_rows, :]
        remote(arrived, arrived, project_send, project_recv, (e, die)).wait_recv()

        def mixed(which):
            lanes = pl.ds(pl.multiple_of(which * quarter, quarter), quarter)
            attended = jnp.transpose(att_recv[:, lanes].astype(jnp.float32)).astype(jnp.bfloat16)
            return jnp.dot(attended, project[...], preferred_element_type=jnp.float32).astype(
                jnp.bfloat16
            )

        mix_send[...] = mixed(1 - chip)
        copy = remote(mix_send, mix_recv, mix_out, mix_in, (e, over))
        copy.start()
        pending.append(copy)
        mixer_ref[...] = mixed(chip)

    def share_here(count):
        lane = lax.broadcasted_iota(jnp.int32, (count * slots, 128), 1)
        return jnp.logical_and(lane >= 3 * y, lane < 3 * y + 3)

    def contract(chunk, first, count):
        rows = pl.ds(pl.multiple_of(first * slots, slots), count * slots)
        shares = rows_recv[pl.ds(first, count), :, model:].reshape(count * slots, 128)
        share = jnp.sum(
            jnp.where(share_here(count), shares.astype(jnp.float32), 0.0), axis=1, keepdims=True
        )
        return (
            jnp.dot(hidden[rows, :], down_all[chunk], preferred_element_type=jnp.float32) * share
        )

    def part_copy(chunk, place):
        rows = pl.ds(pl.multiple_of(place * PAIR * slots, PAIR * slots), PAIR * slots)
        return remote(
            part_send.at[chunk, rows],
            part_recv.at[chunk, rows],
            part_out.at[chunk, place],
            part_in.at[chunk, place],
            (side, t),
        )

    def send_part(chunk, first, place):
        rows = pl.ds(pl.multiple_of(place * PAIR * slots, PAIR * slots), PAIR * slots)
        part_send[chunk, rows, :] = contract(chunk, first, PAIR).astype(jnp.bfloat16)
        copy = part_copy(chunk, place)
        copy.start()
        pending.append(copy)

    def give_back(chunk):
        for place in range(PAIR):
            part_copy(chunk, place).wait_recv()
        total = part_own[chunk] + part_recv[chunk].astype(jnp.float32)
        back_send[chunk] = total.astype(jnp.bfloat16).reshape(lines, slots, span)
        for order in range(lines - 1):
            there = nearest(order)
            copy = remote(
                back_send.at[chunk, there],
                back_recv.at[chunk, z],
                back_out.at[chunk, order],
                back_in.at[chunk, z],
                (PAIR * there + y, t),
            )
            copy.start()
            pending.append(copy)
        back_recv[chunk, z] = back_send[chunk, z]

    def send_early(chunk):
        wait_die(2 + chunk)
        wait_across(2 + chunk)
        send_part(chunk, early, upper)

    def pass_down(chunk):
        if chunk < CHUNKS:
            pass_on(2 + chunk)

    for chunk in range(AHEAD):
        send_early(chunk)
        if chunk == 0:
            mix()
        pass_down(chunk + 1)
    for i in range(PAIR):
        wait_rows(late + i)
    serve_all(late, PAIR, 0, 2 * PAIR)
    for chunk in range(AHEAD):
        send_part(chunk, late, 1 - upper)
    serve_all(own_first, lines, PAIR, 2 * PAIR)
    for chunk in range(CHUNKS):
        if chunk >= AHEAD:
            send_early(chunk)
            send_part(chunk, late, 1 - upper)
            pass_down(chunk + 1)
        part_own[chunk] = contract(chunk, own_first, lines)
        if chunk > 0:
            give_back(chunk - 1)
    give_back(CHUNKS - 1)

    remote(mix_send, mix_recv, mix_out, mix_in, (e, over)).wait_recv()
    mixer_ref[...] = (
        mixer_ref[...].astype(jnp.float32) + mix_recv[...].astype(jnp.float32)
    ).astype(jnp.bfloat16)

    for chunk in range(CHUNKS):
        for step in range(1, lines):
            there = lax.rem(z + step, lines)
            arrived = back_recv.at[chunk, there]
            remote(
                arrived, arrived, back_out.at[chunk, 0], back_in.at[chunk, there], (side, t)
            ).wait_recv()
        routed_ref[:, chunk * span : (chunk + 1) * span] = jnp.dot(
            placed[...],
            back_recv[chunk].reshape(groups * slots, span),
            preferred_element_type=jnp.float32,
        ).astype(jnp.bfloat16)

    for copy in pending:
        copy.wait_send()
    for index in range(CHUNKS + 2):
        pass_copy(index).wait_send()
    for order in range(lines - 1):
        send_rows(order).wait_send()
        pass_rows(order).wait_send()
    send_own_rows().wait_send()
    for i in range(lines):

        @pl.when(z != i)
        def _():
            arrived_keys(PAIR * i + y).wait_send()

    def drain(i, _):
        for other in range(PAIR):

            @pl.when(jnp.logical_not(jnp.logical_and(i == e, core == other)))
            def _():
                send_attended(i, other).wait_send()

        return 0

    lax.fori_loop(0, ep_count, drain, 0)


def fused(
    query_rows,
    key_rows,
    value_rows,
    key_bias,
    out_weight,
    moe_input,
    moe_gain,
    expert_pick,
    route_weight,
    w_gate,
    w_up,
    w_down,
):
    ep_count = lax.axis_size("ep")
    tp_count = lax.axis_size("tp")
    lines = ep_count // PAIR
    block_rows, width = query_rows.shape
    half = block_rows // PAIR
    quarter = half // PAIR
    tokens, model = moe_input.shape
    slots = GROUPS * tokens // (w_gate.shape[0] * ep_count)
    shard = w_gate.shape[2]
    span = model // CHUNKS
    bf16, f32 = jnp.bfloat16, jnp.float32
    dma = pltpu.SemaphoreType.DMA
    vmem = pltpu.VMEM
    operands = (
        query_rows,
        key_rows,
        value_rows,
        jnp.transpose(key_bias),
        out_weight,
        moe_input,
        moe_gain.reshape(1, model),
        jnp.transpose(expert_pick),
        jnp.transpose(route_weight),
        w_gate,
        w_up,
        w_down,
    )
    fetched = operands[:4] + operands[5:9]
    scratch = [vmem(array.shape, array.dtype) for array in fetched] + [
        vmem((lines, HEAD_DIM, block_rows), bf16),
        vmem((ep_count, 2 * HEAD_DIM, half), bf16),
        vmem((lines, 2 * HEAD_DIM, block_rows), bf16),
        vmem((ep_count, 2 * HEAD_DIM, block_rows), bf16),
        vmem((ep_count * block_rows, 2 * HEAD_DIM), bf16),
        vmem((PAIR, half, half), f32),
        vmem((PAIR, half, half), f32),
        vmem((block_rows, half), bf16),
        vmem((HEAD_DIM, half), f32),
        vmem((ep_count, HEAD_DIM, half), bf16),
        vmem((PAIR * width, half), bf16),
        vmem((PAIR * width, model), bf16),
        vmem((quarter, model), bf16),
        vmem((quarter, model), bf16),
        vmem((lines, slots, model + 128), bf16),
        vmem((ep_count, slots, model + 128), bf16),
        vmem((tokens, lines * slots), bf16),
        vmem((tp_count, model, shard), bf16),
        vmem((tp_count, model, shard), bf16),
        vmem((CHUNKS, tp_count * shard, span), bf16),
        vmem((ep_count * slots, tp_count * shard), bf16),
        vmem((CHUNKS, lines * slots, span), bf16),
        vmem((CHUNKS, lines * slots, span), bf16),
        vmem((CHUNKS, lines * slots, span), f32),
        vmem((CHUNKS, lines, slots, span), bf16),
        vmem((CHUNKS, lines, slots, span), bf16),
        dma((CHUNKS + 3,)),
        dma((CHUNKS + 2,)),
        dma((CHUNKS + 2,)),
        dma((CHUNKS + 2,)),
        dma((CHUNKS + 2,)),
        dma((CHUNKS + 2,)),
        dma((CHUNKS + 2,)),
        dma,
        dma,
        dma((ep_count,)),
        dma((ep_count,)),
        dma((lines,)),
        dma((lines,)),
        dma((ep_count,)),
        dma((lines,)),
        dma((lines,)),
        dma((ep_count,)),
        dma((ep_count, PAIR)),
        dma((PAIR, ep_count)),
        dma,
        dma,
        dma((CHUNKS, PAIR)),
        dma((CHUNKS, PAIR)),
        dma((CHUNKS, lines)),
        dma((CHUNKS, lines)),
        dma((len(fetched),)),
    ]
    in_hbm = pl.BlockSpec(memory_space=pltpu.HBM)
    in_vmem = pl.BlockSpec(memory_space=pltpu.VMEM)
    return pl.pallas_call(
        fused_kernel,
        out_shape=(
            vmem((quarter, model), bf16),
            vmem((tokens, model), bf16),
        ),
        in_specs=[in_hbm] * len(operands),
        out_specs=(in_vmem, in_vmem),
        scratch_shapes=scratch,
        compiler_params=pltpu.CompilerParams(
            collective_id=0, has_side_effects=True, vmem_limit_bytes=58 * 1024 * 1024
        ),
    )(*operands)


def fits(query_rows, w_gate):
    ep_count = lax.axis_size("ep")
    return (
        lax.axis_size("tp") == PAIR * PAIR
        and TOPK == PAIR
        and w_gate.shape[0] == 1
        and ep_count == GROUPS * TOPK
        and query_rows.shape[1] == GROUPS * HEAD_DIM
    )


def step(*args):
    return (fused if fits(args[0], args[9]) else local)(*args)


def solution(mesh):
    placed = (
        P("ep", "tp"),
        P("ep", "tp"),
        P("ep", "tp"),
        P(None, "tp"),
        P("tp", None),
        P(("ep", "tp"), None),
        P(),
        P(("ep", "tp"), None),
        P(("ep", "tp"), None),
        P("ep", None, "tp"),
        P("ep", None, "tp"),
        P("ep", "tp", None),
    )
    return jax.shard_map(
        step,
        mesh=mesh,
        in_specs=placed,
        out_specs=(P(("ep", "tp"), None), P(("ep", "tp"), None)),
        check_vma=False,
    )
```

```python
import jax
import jax.numpy as jnp
from jax import lax
from jax.experimental import pallas as pl
from jax.experimental.pallas import tpu as pltpu
from jax.sharding import PartitionSpec as P

HEAD_DIM = 64
GROUPS = 4
TOPK = 2
PAIR = 2


norm_eps = 1e-06


def attend_kernel(tops_ref, query_ref, bias_ref, *rest):
    block_refs = rest[:-4]
    out_ref, acc_ref, kv_ref, sems = rest[-4:]

    @pl.when(pl.program_id(0) == 0)
    def _():
        copies = [
            pltpu.make_async_copy(ref, kv_ref.at[slot], sems.at[slot])
            for slot, ref in enumerate(block_refs)
        ]
        for copy in copies:
            copy.start()
        for copy in copies:
            copy.wait()

    tile = query_ref.shape[1]
    width = query_ref.shape[2]
    heads = width // HEAD_DIM
    slots = kv_ref.shape[0]
    per_block = kv_ref.shape[1] // tile
    top = tops_ref[pl.program_id(0)]
    own = tops_ref[2]
    turned = jnp.transpose(query_ref[0].astype(jnp.float32) * HEAD_DIM ** (-0.5))
    row_head = lax.broadcasted_iota(jnp.int32, (width, tile), 0) // HEAD_DIM
    queries = [jnp.where(row_head == h, turned, 0.0).astype(jnp.bfloat16) for h in range(heads)]
    key_at = lax.broadcasted_iota(jnp.int32, (tile, tile), 0)
    query_at = lax.broadcasted_iota(jnp.int32, (tile, tile), 1)
    causal = key_at < query_at
    later = jnp.where(causal, 1.0, 0.0).astype(jnp.bfloat16)
    acc_ref[...] = jnp.zeros_like(acc_ref)

    def visit(index, running, masked):
        block = index // per_block
        away = lax.rem(own // PAIR - block // PAIR + slots // PAIR, slots // PAIR)
        slot = away * PAIR + lax.rem(own + block, PAIR)
        rows = pl.ds(pl.multiple_of((index - block * per_block) * tile, tile), tile)
        first = pl.multiple_of(index * tile, tile)
        keys = kv_ref[slot, rows, :width]
        values = jnp.transpose(kv_ref[slot, rows, width:])
        passed = []
        for h in range(heads):
            scores = jnp.dot(keys, queries[h], preferred_element_type=jnp.float32)
            scores = scores + bias_ref[pl.ds(first, tile), h : h + 1]
            tail = jnp.log(1.0 + jnp.exp(-jnp.abs(scores)))
            lost = jnp.maximum(scores, 0.0) + tail
            won = jnp.minimum(scores, 0.0) - tail
            if masked:
                lost = jnp.where(causal, lost, 0.0)
            lost = lost.astype(jnp.bfloat16)
            after = jnp.dot(later, lost, preferred_element_type=jnp.float32)
            weight = jnp.exp(won - (after + running[h]))
            if masked:
                weight = jnp.where(causal, weight, 0.0)
            span = slice(h * HEAD_DIM, (h + 1) * HEAD_DIM)
            acc_ref[span, :] += jnp.dot(
                values[span, :], weight.astype(jnp.bfloat16), preferred_element_type=jnp.float32
            )
            passed.append(running[h] + after[0:1, :] + lost[0:1, :].astype(jnp.float32))
        return tuple(passed)

    running = tuple(jnp.zeros((1, tile), jnp.float32) for _ in range(heads))
    running = visit(top, running, True)
    lax.fori_loop(0, top, lambda step, carried: visit(top - 1 - step, carried, False), running)
    out_ref[0] = jnp.transpose(acc_ref[...]).astype(jnp.bfloat16)


def attend(tops, queries, blocks, bias):
    parts, tile, width = queries.shape
    held = (len(blocks),) + blocks[0].shape
    pairs = parts * tile * held[0] * held[1] * width // HEAD_DIM // 2
    return pl.pallas_call(
        attend_kernel,
        out_shape=jax.ShapeDtypeStruct(queries.shape, jnp.bfloat16),
        grid_spec=pltpu.PrefetchScalarGridSpec(
            num_scalar_prefetch=1,
            grid=(parts,),
            in_specs=[
                pl.BlockSpec((1, tile, width), lambda c, tops: (c, 0, 0)),
                pl.BlockSpec(memory_space=pltpu.VMEM),
            ]
            + [pl.BlockSpec(memory_space=pl.ANY)] * len(blocks),
            out_specs=pl.BlockSpec((1, tile, width), lambda c, tops: (c, 0, 0)),
            scratch_shapes=[
                pltpu.VMEM((width, tile), jnp.float32),
                pltpu.VMEM(held, blocks[0].dtype),
                pltpu.SemaphoreType.DMA((len(blocks),)),
            ],
        ),
        cost_estimate=pl.CostEstimate(
            flops=pairs * 1000, bytes_accessed=len(blocks) * blocks[0].size * 2, transcendentals=pairs * 3
        ),
        compiler_params=pltpu.CompilerParams(vmem_limit_bytes=58 * 1024 * 1024),
    )(tops, queries, bias, *blocks)


def gather_blocks(own, count):
    ring = count // PAIR
    swap = [(i, i // PAIR * PAIR + (i + 1) % PAIR) for i in range(count)]
    ahead = [(i, (i + PAIR) % count) for i in range(count)]
    behind = [(j, i) for i, j in ahead]
    near = [own, lax.ppermute(own, "ep", swap)]
    far = {}
    for member in range(PAIR):
        reach = (ring - 1 + (member == 0)) // 2
        held = near[member]
        for step in range(1, reach + 1):
            held = lax.ppermute(held, "ep", ahead)
            far[step, member] = held
        held = near[member]
        for step in range(ring - 1, reach, -1):
            held = lax.ppermute(held, "ep", behind)
            far[step, member] = held
    return near + [far[step, member] for step in range(1, ring) for member in range(PAIR)]


def expand(arrived, gate_weights, up_weights):
    gate_in = jnp.einsum(
        "necm,emf->necf", arrived, gate_weights, preferred_element_type=jnp.float32
    )
    up_in = jnp.einsum("necm,emf->necf", arrived, up_weights, preferred_element_type=jnp.float32)
    return (jax.nn.silu(gate_in) * up_in).astype(jnp.bfloat16)


def contract(hidden, down_weights):
    return jnp.einsum("necf,efm->necm", hidden, down_weights, preferred_element_type=jnp.float32)


def local(
    query_rows,
    key_rows,
    value_rows,
    key_bias,
    out_weight,
    moe_input,
    moe_gain,
    expert_pick,
    route_weight,
    w_gate,
    w_up,
    w_down,
):
    block_rows = query_rows.shape[0]
    half_rows = block_rows // 2
    ep_index = lax.axis_index("ep")
    ep_count = lax.axis_size("ep")
    own_kv = jnp.concatenate([key_rows, value_rows], axis=1)
    mirror = [(i, ep_count - 1 - i) for i in range(ep_count)]
    far_query = lax.ppermute(query_rows[half_rows:], "ep", mirror)
    blocks = gather_blocks(own_kv, ep_count)
    tops = jnp.stack(
        [2 * ep_index, 2 * (ep_count - 1 - ep_index) + 1, ep_index]
    ).astype(jnp.int32)
    near, far = attend(
        tops, jnp.stack([query_rows[:half_rows], far_query]), blocks, key_bias
    )
    attended = jnp.concatenate([near, lax.ppermute(far, "ep", mirror)], axis=0)
    mixer_out = lax.psum_scatter(
        jnp.dot(attended, out_weight, preferred_element_type=jnp.float32).astype(jnp.bfloat16),
        "tp",
        scatter_dimension=0,
        tiled=True,
    )
    token_count = moe_input.shape[0]
    widened = moe_input.astype(jnp.float32)
    normed = (
        widened
        * lax.rsqrt(jnp.mean(widened * widened, axis=1, keepdims=True) + norm_eps)
        * moe_gain
    ).astype(jnp.bfloat16)
    local_experts = w_gate.shape[0]
    expert_total = local_experts * ep_count
    capacity = GROUPS * token_count // expert_total
    picks = expert_pick.reshape(-1)
    matches = (picks[:, None] == jnp.arange(expert_total, dtype=jnp.int32)[None, :]).astype(
        jnp.int32
    )
    ranks = jnp.sum((jnp.cumsum(matches, axis=0) - matches) * matches, axis=1)
    slots = picks * capacity + ranks
    owners = jnp.arange(picks.shape[0], dtype=jnp.int32) // TOPK
    table = jnp.full((expert_total * capacity,), token_count, jnp.int32).at[slots].set(owners)
    padded = jnp.concatenate([normed, jnp.zeros((1, normed.shape[1]), jnp.bfloat16)], axis=0)
    outgoing = padded[table].reshape(ep_count, local_experts, capacity, normed.shape[1])
    outgoing = lax.optimization_barrier((outgoing, far_query, *blocks))[0]
    arrived = lax.all_to_all(outgoing, "ep", split_axis=0, concat_axis=0, tiled=True)
    gate_all, up_all, down_all = (
        lax.all_gather(w_gate, "tp", axis=2, tiled=True),
        lax.all_gather(w_up, "tp", axis=2, tiled=True),
        lax.all_gather(w_down, "tp", axis=1, tiled=True),
    )
    served = contract(expand(arrived, gate_all, up_all), down_all).astype(jnp.bfloat16)
    returned = lax.all_to_all(served, "ep", split_axis=0, concat_axis=0, tiled=True)
    flat = returned.reshape(expert_total * capacity, returned.shape[3])
    chosen = flat[slots].reshape(token_count, TOPK, flat.shape[1]).astype(jnp.float32)
    routed_out = jnp.sum(chosen * route_weight[:, :, None], axis=1).astype(jnp.bfloat16)
    return (mixer_out, routed_out)


MESH = pl.DeviceIdType.MESH
CHUNKS = 8
AHEAD = 3


def remote(src, dst, send, recv, device):
    return pltpu.make_async_remote_copy(
        src_ref=src,
        dst_ref=dst,
        send_sem=send,
        recv_sem=recv,
        device_id=device,
        device_id_type=MESH,
    )


def split_parts(values):
    high = values.astype(jnp.bfloat16).astype(jnp.float32)
    rest = values - high
    middle = rest.astype(jnp.bfloat16).astype(jnp.float32)
    return high, middle, rest - middle


def fused_kernel(
    q_hbm,
    k_hbm,
    v_hbm,
    bias_hbm,
    out_weight_ref,
    moe_hbm,
    gain_hbm,
    pick_hbm,
    route_hbm,
    gate_ref,
    up_ref,
    down_ref,
    mixer_ref,
    routed_ref,
    q_ref,
    k_ref,
    v_ref,
    bias_ref,
    moe_ref,
    gain_ref,
    pick_ref,
    route_ref,
    q_send,
    q_recv,
    kv_send,
    kv_recv,
    keys,
    scores_buf,
    won,
    weights,
    acc,
    att_send,
    att_recv,
    project,
    mix_send,
    mix_recv,
    rows_send,
    rows_recv,
    placed,
    gate_all,
    up_all,
    down_all,
    hidden,
    part_send,
    part_recv,
    part_own,
    back_send,
    back_recv,
    local_sem,
    over_send,
    over_recv,
    die_send,
    die_recv,
    pass_send,
    pass_recv,
    project_send,
    project_recv,
    q_out,
    q_in,
    kv_out,
    kv_pass,
    kv_in,
    rows_out,
    rows_pass,
    rows_in,
    att_out,
    att_in,
    mix_out,
    mix_in,
    part_out,
    part_in,
    back_out,
    back_in,
    fetch_sem,
):
    ep_count = q_recv.shape[0]
    lines = ep_count // PAIR
    e, t = lax.axis_index("ep"), lax.axis_index("tp")
    z, y = lax.div(e, PAIR), lax.rem(e, PAIR)
    chip, core = lax.div(t, PAIR), lax.rem(t, PAIR)
    die = PAIR * chip + 1 - core
    over = PAIR * (1 - chip) + core
    across = PAIR * (1 - chip) + 1 - core
    side = PAIR * z + 1 - y
    block_rows, width = q_ref.shape
    half = block_rows // PAIR
    quarter = half // PAIR
    tokens, model = moe_ref.shape
    slots = rows_send.shape[1]
    shard = gate_ref.shape[2]
    span = model // CHUNKS

    upper = lax.div(z, PAIR)
    inner = lax.rem(z + upper, PAIR)

    def nearest(order):
        away = (1 + 2 * inner, 2 - inner, 3 - inner)[order]
        return lax.rem(z + away + upper * (2 * lines - 2 * away), lines)

    def rows_target(order):
        away = (1 + 2 * inner, 2, 3 - 2 * inner)[order]
        return lax.rem(z + away + upper * (2 * lines - 2 * away), lines)

    fetches = [
        pltpu.make_async_copy(src, dst, fetch_sem.at[i])
        for i, (src, dst) in enumerate(
            (
                (k_hbm, k_ref),
                (v_hbm, v_ref),
                (q_hbm, q_ref),
                (moe_hbm, moe_ref),
                (gain_hbm, gain_ref),
                (pick_hbm, pick_ref),
                (route_hbm, route_ref),
                (bias_hbm, bias_ref),
            )
        )
    ]
    for copy in fetches:
        copy.start()

    barrier = pltpu.get_barrier_semaphore()
    for step in range(1, ep_count):
        for other in range(PAIR):
            pl.semaphore_signal(
                barrier,
                inc=1,
                device_id=(lax.rem(e + step, ep_count), PAIR * chip + other),
                device_id_type=MESH,
            )
    for other in (die, over):
        pl.semaphore_signal(barrier, inc=1, device_id=(e, other), device_id_type=MESH)

    pieces = []
    own_rows = pl.ds(pl.multiple_of(t * shard, shard), shard)
    pieces.append((gate_ref.at[0], gate_all.at[t]))
    pieces.append((up_ref.at[0], up_all.at[t]))
    for chunk in range(CHUNKS):
        pieces.append(
            (
                down_ref.at[0, :, chunk * span : (chunk + 1) * span],
                down_all.at[chunk, own_rows, :],
            )
        )

    def held(index, owner):
        if index == 0:
            return gate_all.at[owner]
        if index == 1:
            return up_all.at[owner]
        rows = pl.ds(pl.multiple_of(owner * shard, shard), shard)
        return down_all.at[index - 2, rows, :]

    project_rows = pl.ds(pl.multiple_of(core * width, width), width)
    die_rows = pl.ds(pl.multiple_of((1 - core) * width, width), width)
    locals_ = [
        pltpu.make_async_copy(src, dst, local_sem) for src, dst in pieces
    ]
    locals_.append(
        pltpu.make_async_copy(out_weight_ref, project.at[project_rows, :], local_sem)
    )
    for copy in locals_:
        copy.start()

    pl.semaphore_wait(barrier, PAIR * (ep_count - 1) + 2)

    for i, (src, dst) in enumerate(pieces):
        remote(src, dst, over_send, over_recv.at[i], (e, over)).start()

    for copy in fetches:
        copy.wait()
    keys_turned = jnp.transpose(k_ref[...].astype(jnp.float32)).astype(jnp.bfloat16)
    values_turned = jnp.transpose(v_ref[...].astype(jnp.float32)).astype(jnp.bfloat16)
    for h in range(lines):
        span_h = slice(h * HEAD_DIM, (h + 1) * HEAD_DIM)
        kv_send[h, :HEAD_DIM, :] = keys_turned[span_h, :]
        kv_send[h, HEAD_DIM:, :] = values_turned[span_h, :]
    q_turned = jnp.transpose(q_ref[...].astype(jnp.float32) * HEAD_DIM ** (-0.5))
    for h in range(lines):
        q_send[h] = q_turned[h * HEAD_DIM : (h + 1) * HEAD_DIM, :].astype(jnp.bfloat16)
    copy = remote(kv_send.at[z], kv_recv.at[e], kv_pass, kv_in.at[e], (side, t))
    copy.start()

    def send_queries(head, column):
        lanes = pl.ds(pl.multiple_of(lax.rem(column + e, PAIR) * half, half), half)
        return remote(
            q_send.at[head, :, lanes],
            q_recv.at[e, :HEAD_DIM, :],
            q_out,
            q_in.at[e],
            (PAIR * head + column, t),
        )

    for order in range(lines - 1):
        there = nearest(order)
        copies = [
            remote(
                kv_send.at[there], kv_recv.at[e], kv_out, kv_in.at[e], (PAIR * there + y, t)
            )
        ]
        copies += [send_queries(there, column) for column in range(PAIR)]
        for copy in copies:
            copy.start()
    send_queries(z, 1 - y).start()
    kv_recv[e] = kv_send[z]
    ones_at = lax.broadcasted_iota(jnp.int32, (HEAD_DIM, half), 0) < 3
    ones_rows = jnp.where(ones_at, 1.0, 0.0).astype(jnp.bfloat16)
    for i in range(ep_count):
        q_recv[i, HEAD_DIM:, :] = ones_rows
    own_lanes = pl.ds(pl.multiple_of(lax.rem(y + e, PAIR) * half, half), half)
    q_recv[e, :HEAD_DIM, :] = q_send[z, :, own_lanes]

    for i, (src, dst) in enumerate(pieces):
        remote(src, dst, die_send, die_recv.at[i], (e, die)).start()
    give_project = remote(
        out_weight_ref, project.at[project_rows, :], project_send, project_recv, (e, die)
    )
    give_project.start()

    widened = moe_ref[...].astype(jnp.float32)
    normed = (
        widened
        * lax.rsqrt(jnp.mean(widened * widened, axis=1, keepdims=True) + norm_eps)
        * gain_ref[...]
    ).astype(jnp.bfloat16)
    group_row = lax.shift_right_logical(pick_ref[0:1, :], 1)
    groups = lines
    group_at = lax.broadcasted_iota(jnp.int32, (8, tokens), 0)
    chosen = (group_at == group_row).astype(jnp.float32)
    earlier = (
        lax.broadcasted_iota(jnp.int32, (tokens, tokens), 0)
        < lax.broadcasted_iota(jnp.int32, (tokens, tokens), 1)
    ).astype(jnp.float32)
    ranks = jnp.dot(
        chosen.astype(jnp.bfloat16),
        earlier.astype(jnp.bfloat16),
        preferred_element_type=jnp.float32,
    )
    slot_row = jnp.sum(
        chosen * (ranks + group_at.astype(jnp.float32) * slots), axis=0, keepdims=True
    )
    slot_at = lax.broadcasted_iota(jnp.int32, (groups * slots, tokens), 0)
    picked = (slot_at == slot_row.astype(jnp.int32)).astype(jnp.float32)
    placed[...] = jnp.transpose(picked).astype(jnp.bfloat16)
    first_low = (pick_ref[0:1, :] & 1) == 0
    low_row = jnp.where(first_low, route_ref[0:1, :], route_ref[1:2, :])
    high_row = jnp.where(first_low, route_ref[1:2, :], route_ref[0:1, :])
    low = split_parts(jnp.sum(picked * low_row, axis=1, keepdims=True))
    high = split_parts(jnp.sum(picked * high_row, axis=1, keepdims=True))
    lane = lax.broadcasted_iota(jnp.int32, (groups * slots, 128), 1)
    shares = jnp.zeros((groups * slots, 128), jnp.float32)
    for i, part in enumerate(low + high):
        shares = jnp.where(lane == i, part, shares)
    rows_send[:, :, model:] = shares.astype(jnp.bfloat16).reshape(groups, slots, 128)
    picked = picked.astype(jnp.bfloat16)
    for first in range(0, model, span):
        rows_send[:, :, first : first + span] = (
            jnp.dot(picked, normed[:, first : first + span], preferred_element_type=jnp.float32)
            .astype(jnp.bfloat16)
            .reshape(groups, slots, span)
        )
    home = y * lines + z
    rows_recv[home] = rows_send[z]

    def send_rows(order):
        there = rows_target(order)
        return remote(
            rows_send.at[there],
            rows_recv.at[home],
            rows_out,
            rows_in.at[home],
            (PAIR * there + y, t),
        )

    for order in range(lines - 1):
        send_rows(order).start()

    def send_own_rows():
        return remote(
            rows_send.at[z], rows_recv.at[home], rows_pass, rows_in.at[home], (side, t)
        )

    def arrived_keys(source):
        arrived = kv_recv.at[source]
        return remote(arrived, arrived, kv_pass, kv_in.at[source], (side, t))

    def pass_keys(pair):
        @pl.when(pair != z)
        def _():
            copy = arrived_keys(PAIR * pair + y)
            copy.wait_recv()
            copy.start()

    head_at = lax.broadcasted_iota(jnp.int32, (lines, block_rows), 0)
    aug_at = lax.broadcasted_iota(jnp.int32, (HEAD_DIM, block_rows), 0)

    def ready(i):
        @pl.when(i != e)
        def _():
            arrived = q_recv.at[i, :HEAD_DIM, :]
            remote(arrived, arrived, q_out, q_in.at[i], (side, t)).wait_recv()

        rows = pl.ds(pl.multiple_of(i * block_rows, block_rows), block_rows)
        bias = jnp.sum(
            jnp.where(head_at == z, bias_ref[:, rows], 0.0), axis=0, keepdims=True
        )
        extra = jnp.zeros((HEAD_DIM, block_rows), jnp.float32)
        for place, part in enumerate(split_parts(bias)):
            extra = jnp.where(aug_at == place, part, extra)
        stacked = jnp.concatenate([kv_recv[i, :HEAD_DIM, :].astype(jnp.float32), extra], axis=0)
        keys[rows, :] = jnp.transpose(stacked).astype(jnp.bfloat16)

    key_at = lax.broadcasted_iota(jnp.int32, (half, half), 0)
    query_at = lax.broadcasted_iota(jnp.int32, (half, half), 1)
    later = jnp.where(key_at < query_at, 1.0, 0.0).astype(jnp.bfloat16)

    def score(block, queries):
        for sub in range(PAIR):
            rows = pl.ds(pl.multiple_of(block * block_rows + sub * half, half), half)
            scores_buf[sub] = jnp.dot(keys[rows, :], queries, preferred_element_type=jnp.float32)

    def gather_values(block):
        acc[...] += jnp.dot(
            kv_recv[block, HEAD_DIM:, :], weights[...], preferred_element_type=jnp.float32
        )

    def visit(following, queries, running, place):
        firsts, afters = {}, {}
        for sub in range(PAIR - 1, -1, -1):
            scores = scores_buf[sub]
            lost = jnp.maximum(scores, jnp.log(1.0 + jnp.exp(jnp.minimum(scores, 80.0))))
            won[sub] = scores - lost
            if place is not None:
                lost = jnp.where(key_at - query_at < (place - sub) * half, lost, 0.0)
            lost = lost.astype(jnp.bfloat16)
            firsts[sub] = lost[0:1, :].astype(jnp.float32)
            afters[sub] = jnp.dot(later, lost, preferred_element_type=jnp.float32)
        score(following, queries)
        for sub in range(PAIR - 1, -1, -1):
            weight = jnp.exp(won[sub] - (afters[sub] + running))
            if place is not None:
                weight = jnp.where(key_at - query_at < (place - sub) * half, weight, 0.0)
            weights[sub * half : (sub + 1) * half, :] = weight.astype(jnp.bfloat16)
            running = running + afters[sub][0:1, :] + firsts[sub]
        return running

    def send_attended(i, other):
        place = lax.rem(y + i, PAIR)
        return remote(
            att_send.at[i, :, other * quarter : (other + 1) * quarter],
            att_recv.at[
                pl.ds(pl.multiple_of(core * width + z * HEAD_DIM, HEAD_DIM), HEAD_DIM),
                pl.ds(pl.multiple_of(place * quarter, quarter), quarter),
            ],
            att_out,
            att_in,
            (i, PAIR * chip + other),
        )

    def wait_rows(place):
        arrived = rows_recv.at[place]
        remote(arrived, arrived, rows_out, rows_in.at[place], (side, t)).wait_recv()

    def pass_rows(order):
        there = nearest(order)
        place = y * lines + there
        arrived = rows_recv.at[place]
        return remote(arrived, arrived, rows_pass, rows_in.at[place], (side, t))

    def pass_rows_on(order):
        wait_rows(y * lines + nearest(order))
        pass_rows(order).start()

    def pass_copy(index):
        arrived = held(index, over)
        return remote(arrived, arrived, pass_send, pass_recv.at[index], (e, die))

    def pass_on(index):
        arrived = held(index, over)
        remote(arrived, arrived, over_send, over_recv.at[index], (e, over)).wait_recv()
        pass_copy(index).start()

    def one_tile(i, _):
        pair = lax.div(i, PAIR)

        @pl.when(lax.rem(i, PAIR) == 0)
        def _():
            arrived_keys(i + 1 - y).wait_recv()
            ready(i)
            ready(i + 1)

        @pl.when(jnp.logical_and(lax.rem(i, PAIR) == 1, i < ep_count - 1))
        def _():
            pass_keys(pair + 1)

        @pl.when(i == PAIR)
        def _():
            send_own_rows().start()

        @pl.when(i == ep_count - PAIR - 1)
        def _():
            pass_on(0)

        for order in range(lines - 2):

            @pl.when(jnp.logical_and(i == lines + PAIR * order, inner * order == 0))
            def _():
                pass_rows_on(order)

        place = lax.rem(y + i, PAIR)
        queries = q_recv[i]
        acc[...] = jnp.zeros_like(acc)
        score(i, queries)
        running = visit(
            jnp.maximum(i - 1, 0), queries, jnp.zeros((1, half), jnp.float32), place
        )

        def next_block(s, running):
            gather_values(i - s)
            return visit(jnp.maximum(i - 2 - s, 0), queries, running, None)

        lax.fori_loop(0, i, next_block, running)
        gather_values(0)
        att_send[i] = acc[...].astype(jnp.bfloat16)
        for other in range(PAIR):
            here = jnp.logical_and(i == e, core == other)

            @pl.when(jnp.logical_not(here))
            def _():
                send_attended(i, other).start()

            @pl.when(here)
            def _():
                att_recv[
                    pl.ds(pl.multiple_of(core * width + z * HEAD_DIM, HEAD_DIM), HEAD_DIM),
                    pl.ds(pl.multiple_of(place * quarter, quarter), quarter),
                ] = att_send[i, :, other * quarter : (other + 1) * quarter]

        return 0

    pass_keys(0)
    lax.fori_loop(0, ep_count, one_tile, 0)

    def wait_die(index):
        arrived = held(index, die)
        remote(arrived, arrived, die_send, die_recv.at[index], (e, die)).wait_recv()

    def wait_across(index):
        arrived = held(index, across)
        remote(arrived, arrived, pass_send, pass_recv.at[index], (e, die)).wait_recv()

    def serve(owner, first, count):
        hidden_lanes = pl.ds(pl.multiple_of(owner * shard, shard), shard)
        rows = rows_recv[pl.ds(first, count), :, :model].reshape(count * slots, model)
        gate_in = jnp.dot(rows, gate_all[owner], preferred_element_type=jnp.float32)
        up_in = jnp.dot(rows, up_all[owner], preferred_element_type=jnp.float32)
        target = pl.ds(pl.multiple_of(first * slots, slots), count * slots)
        hidden[target, hidden_lanes] = (gate_in / (1.0 + jnp.exp(-gate_in)) * up_in).astype(
            jnp.bfloat16
        )

    def serve_all(first, count, start, stop):
        def one(k, _):
            owner = PAIR * lax.rem(chip + lax.div(k, PAIR), PAIR) + lax.rem(core + k, PAIR)
            serve(owner, first, count)
            return 0

        lax.fori_loop(start, stop, one, 0)

    own_first = y * lines
    early = (1 - y) * lines + PAIR * upper
    late = (1 - y) * lines + PAIR * (1 - upper)

    @pl.when(inner == 1)
    def _():
        pass_rows_on(1)

    pass_rows_on(lines - 2)
    pass_on(1)
    pltpu.make_async_copy(gate_all, gate_all, local_sem).wait()
    wait_die(0)
    wait_die(1)
    for i in range(PAIR):
        wait_rows(early + i)
    serve_all(early, PAIR, 0, PAIR)
    pass_on(2)
    serve_all(own_first, lines, 0, PAIR)
    serve_all(early, PAIR, PAIR, PAIR + 1)
    wait_across(0)
    wait_across(1)
    serve_all(early, PAIR, PAIR + 1, 2 * PAIR)

    def mix():
        pieces_in = att_recv.at[: PAIR * width - HEAD_DIM // PAIR, :]
        remote(pieces_in, pieces_in, att_out, att_in, (side, t)).wait_recv()
        arrived = project.at[die_rows, :]
        remote(arrived, arrived, project_send, project_recv, (e, die)).wait_recv()

        def mixed(which):
            lanes = pl.ds(pl.multiple_of(which * quarter, quarter), quarter)
            attended = jnp.transpose(att_recv[:, lanes].astype(jnp.float32)).astype(jnp.bfloat16)
            return jnp.dot(attended, project[...], preferred_element_type=jnp.float32).astype(
                jnp.bfloat16
            )

        mix_send[...] = mixed(1 - chip)
        remote(mix_send, mix_recv, mix_out, mix_in, (e, over)).start()
        mixer_ref[...] = mixed(chip)

    def share_here(count):
        lane = lax.broadcasted_iota(jnp.int32, (count * slots, 128), 1)
        return jnp.logical_and(lane >= 3 * y, lane < 3 * y + 3)

    def contract(chunk, first, count):
        rows = pl.ds(pl.multiple_of(first * slots, slots), count * slots)
        shares = rows_recv[pl.ds(first, count), :, model:].reshape(count * slots, 128)
        share = jnp.sum(
            jnp.where(share_here(count), shares.astype(jnp.float32), 0.0), axis=1, keepdims=True
        )
        return (
            jnp.dot(hidden[rows, :], down_all[chunk], preferred_element_type=jnp.float32) * share
        )

    def part_copy(chunk, place):
        rows = pl.ds(pl.multiple_of(place * PAIR * slots, PAIR * slots), PAIR * slots)
        return remote(
            part_send.at[chunk, rows],
            part_recv.at[chunk, rows],
            part_out,
            part_in.at[chunk],
            (side, t),
        )

    def send_part(chunk, first, place):
        rows = pl.ds(pl.multiple_of(place * PAIR * slots, PAIR * slots), PAIR * slots)
        part_send[chunk, rows, :] = contract(chunk, first, PAIR).astype(jnp.bfloat16)
        part_copy(chunk, place).start()

    def give_back(chunk):
        arrived = part_recv.at[chunk]
        remote(arrived, arrived, part_out, part_in.at[chunk], (side, t)).wait_recv()
        total = part_own[chunk] + part_recv[chunk].astype(jnp.float32)
        back_send[chunk] = total.astype(jnp.bfloat16).reshape(lines, slots, span)
        for order in range(lines - 2, -1, -1):
            there = nearest(order)
            copy = remote(
                back_send.at[chunk, there],
                back_recv.at[chunk, z],
                back_out,
                back_in.at[chunk],
                (PAIR * there + y, t),
            )
            copy.start()
        back_recv[chunk, z] = back_send[chunk, z]

    def send_early(chunk):
        wait_die(2 + chunk)
        wait_across(2 + chunk)
        send_part(chunk, early, upper)

    def pass_down(chunk):
        if chunk < CHUNKS:
            pass_on(2 + chunk)

    for chunk in range(AHEAD):
        send_early(chunk)
        if chunk == 0:
            mix()
        pass_down(chunk + 1)
    for i in range(PAIR):
        wait_rows(late + i)
    serve_all(late, PAIR, 0, 2 * PAIR)
    for chunk in range(AHEAD):
        send_part(chunk, late, 1 - upper)
    serve_all(own_first, lines, PAIR, 2 * PAIR)
    for chunk in range(CHUNKS):
        if chunk >= AHEAD:
            send_early(chunk)
            send_part(chunk, late, 1 - upper)
            pass_down(chunk + 1)
        part_own[chunk] = contract(chunk, own_first, lines)
        if chunk > 0:
            give_back(chunk - 1)
    give_back(CHUNKS - 1)

    remote(mix_send, mix_recv, mix_out, mix_in, (e, over)).wait_recv()
    mixer_ref[...] = (
        mixer_ref[...].astype(jnp.float32) + mix_recv[...].astype(jnp.float32)
    ).astype(jnp.bfloat16)

    for chunk in range(CHUNKS):
        arrived = back_recv.at[chunk, : lines - 1]
        remote(arrived, arrived, back_out, back_in.at[chunk], (side, t)).wait_recv()
        routed_ref[:, chunk * span : (chunk + 1) * span] = jnp.dot(
            placed[...],
            back_recv[chunk].reshape(groups * slots, span),
            preferred_element_type=jnp.float32,
        ).astype(jnp.bfloat16)

    give_project.wait_send()
    weights_sent = gate_all.at[: PAIR + 1]
    for sem in (over_send, die_send, pass_send):
        remote(weights_sent, weights_sent, sem, over_recv.at[0], (e, die)).wait_send()
    for sent, sem, incoming in (
        (kv_recv.at[: lines - 1], kv_out, kv_in.at[0]),
        (kv_recv.at[:lines], kv_pass, kv_in.at[0]),
        (q_recv.at[: ep_count - 1, :HEAD_DIM, :], q_out, q_in.at[0]),
        (rows_recv.at[: lines - 1], rows_out, rows_in.at[0]),
        (rows_recv.at[:lines], rows_pass, rows_in.at[0]),
        (att_recv.at[: PAIR * width - HEAD_DIM // PAIR, :], att_out, att_in),
        (mix_send, mix_out, mix_in),
        (part_send, part_out, part_in.at[0]),
        (back_send.at[:, : lines - 1], back_out, back_in.at[0]),
    ):
        remote(sent, sent, sem, incoming, (side, t)).wait_send()


def fused(
    query_rows,
    key_rows,
    value_rows,
    key_bias,
    out_weight,
    moe_input,
    moe_gain,
    expert_pick,
    route_weight,
    w_gate,
    w_up,
    w_down,
):
    ep_count = lax.axis_size("ep")
    tp_count = lax.axis_size("tp")
    lines = ep_count // PAIR
    block_rows, width = query_rows.shape
    half = block_rows // PAIR
    quarter = half // PAIR
    tokens, model = moe_input.shape
    slots = GROUPS * tokens // (w_gate.shape[0] * ep_count)
    shard = w_gate.shape[2]
    span = model // CHUNKS
    bf16, f32 = jnp.bfloat16, jnp.float32
    dma = pltpu.SemaphoreType.DMA
    vmem = pltpu.VMEM
    operands = (
        query_rows,
        key_rows,
        value_rows,
        jnp.transpose(key_bias),
        out_weight,
        moe_input,
        moe_gain.reshape(1, model),
        jnp.transpose(expert_pick),
        jnp.transpose(route_weight),
        w_gate,
        w_up,
        w_down,
    )
    fetched = operands[:4] + operands[5:9]
    scratch = [vmem(array.shape, array.dtype) for array in fetched] + [
        vmem((lines, HEAD_DIM, block_rows), bf16),
        vmem((ep_count, 2 * HEAD_DIM, half), bf16),
        vmem((lines, 2 * HEAD_DIM, block_rows), bf16),
        vmem((ep_count, 2 * HEAD_DIM, block_rows), bf16),
        vmem((ep_count * block_rows, 2 * HEAD_DIM), bf16),
        vmem((PAIR, half, half), f32),
        vmem((PAIR, half, half), f32),
        vmem((block_rows, half), bf16),
        vmem((HEAD_DIM, half), f32),
        vmem((ep_count, HEAD_DIM, half), bf16),
        vmem((PAIR * width, half), bf16),
        vmem((PAIR * width, model), bf16),
        vmem((quarter, model), bf16),
        vmem((quarter, model), bf16),
        vmem((lines, slots, model + 128), bf16),
        vmem((ep_count, slots, model + 128), bf16),
        vmem((tokens, lines * slots), bf16),
        vmem((tp_count, model, shard), bf16),
        vmem((tp_count, model, shard), bf16),
        vmem((CHUNKS, tp_count * shard, span), bf16),
        vmem((ep_count * slots, tp_count * shard), bf16),
        vmem((CHUNKS, lines * slots, span), bf16),
        vmem((CHUNKS, lines * slots, span), bf16),
        vmem((CHUNKS, lines * slots, span), f32),
        vmem((CHUNKS, lines, slots, span), bf16),
        vmem((CHUNKS, lines, slots, span), bf16),
        dma,
        dma,
        dma((CHUNKS + 2,)),
        dma,
        dma((CHUNKS + 2,)),
        dma,
        dma((CHUNKS + 2,)),
        dma,
        dma,
        dma,
        dma((ep_count,)),
        dma,
        dma,
        dma((ep_count,)),
        dma,
        dma,
        dma((ep_count,)),
        dma,
        dma,
        dma,
        dma,
        dma,
        dma((CHUNKS,)),
        dma,
        dma((CHUNKS,)),
        dma((len(fetched),)),
    ]
    in_hbm = pl.BlockSpec(memory_space=pltpu.HBM)
    in_vmem = pl.BlockSpec(memory_space=pltpu.VMEM)
    return pl.pallas_call(
        fused_kernel,
        out_shape=(
            vmem((quarter, model), bf16),
            vmem((tokens, model), bf16),
        ),
        in_specs=[in_hbm] * len(operands),
        out_specs=(in_vmem, in_vmem),
        scratch_shapes=scratch,
        compiler_params=pltpu.CompilerParams(
            collective_id=0, has_side_effects=True, vmem_limit_bytes=58 * 1024 * 1024
        ),
    )(*operands)


def fits(query_rows, w_gate):
    ep_count = lax.axis_size("ep")
    return (
        lax.axis_size("tp") == PAIR * PAIR
        and TOPK == PAIR
        and w_gate.shape[0] == 1
        and ep_count == GROUPS * TOPK
        and query_rows.shape[1] == GROUPS * HEAD_DIM == w_gate.shape[2]
    )


def step(*args):
    return (fused if fits(args[0], args[9]) else local)(*args)


def solution(mesh):
    placed = (
        P("ep", "tp"),
        P("ep", "tp"),
        P("ep", "tp"),
        P(None, "tp"),
        P("tp", None),
        P(("ep", "tp"), None),
        P(),
        P(("ep", "tp"), None),
        P(("ep", "tp"), None),
        P("ep", None, "tp"),
        P("ep", None, "tp"),
        P("ep", "tp", None),
    )
    return jax.shard_map(
        step,
        mesh=mesh,
        in_specs=placed,
        out_specs=(P(("ep", "tp"), None), P(("ep", "tp"), None)),
        check_vma=False,
    )
```

```python
import jax
import jax.numpy as jnp
from jax import lax
from jax.experimental import pallas as pl
from jax.experimental.pallas import tpu as pltpu
from jax.sharding import PartitionSpec as P

HEAD_DIM = 64
GROUPS = 4
TOPK = 2
PAIR = 2


norm_eps = 1e-06


def attend_kernel(tops_ref, query_ref, bias_ref, *rest):
    block_refs = rest[:-4]
    out_ref, acc_ref, kv_ref, sems = rest[-4:]

    @pl.when(pl.program_id(0) == 0)
    def _():
        copies = [
            pltpu.make_async_copy(ref, kv_ref.at[slot], sems.at[slot])
            for slot, ref in enumerate(block_refs)
        ]
        for copy in copies:
            copy.start()
        for copy in copies:
            copy.wait()

    tile = query_ref.shape[1]
    width = query_ref.shape[2]
    heads = width // HEAD_DIM
    slots = kv_ref.shape[0]
    per_block = kv_ref.shape[1] // tile
    top = tops_ref[pl.program_id(0)]
    own = tops_ref[2]
    turned = jnp.transpose(query_ref[0].astype(jnp.float32) * HEAD_DIM ** (-0.5))
    row_head = lax.broadcasted_iota(jnp.int32, (width, tile), 0) // HEAD_DIM
    queries = [jnp.where(row_head == h, turned, 0.0).astype(jnp.bfloat16) for h in range(heads)]
    key_at = lax.broadcasted_iota(jnp.int32, (tile, tile), 0)
    query_at = lax.broadcasted_iota(jnp.int32, (tile, tile), 1)
    causal = key_at < query_at
    later = jnp.where(causal, 1.0, 0.0).astype(jnp.bfloat16)
    acc_ref[...] = jnp.zeros_like(acc_ref)

    def visit(index, running, masked):
        block = index // per_block
        away = lax.rem(own // PAIR - block // PAIR + slots // PAIR, slots // PAIR)
        slot = away * PAIR + lax.rem(own + block, PAIR)
        rows = pl.ds(pl.multiple_of((index - block * per_block) * tile, tile), tile)
        first = pl.multiple_of(index * tile, tile)
        keys = kv_ref[slot, rows, :width]
        values = jnp.transpose(kv_ref[slot, rows, width:])
        passed = []
        for h in range(heads):
            scores = jnp.dot(keys, queries[h], preferred_element_type=jnp.float32)
            scores = scores + bias_ref[pl.ds(first, tile), h : h + 1]
            tail = jnp.log(1.0 + jnp.exp(-jnp.abs(scores)))
            lost = jnp.maximum(scores, 0.0) + tail
            won = jnp.minimum(scores, 0.0) - tail
            if masked:
                lost = jnp.where(causal, lost, 0.0)
            lost = lost.astype(jnp.bfloat16)
            after = jnp.dot(later, lost, preferred_element_type=jnp.float32)
            weight = jnp.exp(won - (after + running[h]))
            if masked:
                weight = jnp.where(causal, weight, 0.0)
            span = slice(h * HEAD_DIM, (h + 1) * HEAD_DIM)
            acc_ref[span, :] += jnp.dot(
                values[span, :], weight.astype(jnp.bfloat16), preferred_element_type=jnp.float32
            )
            passed.append(running[h] + after[0:1, :] + lost[0:1, :].astype(jnp.float32))
        return tuple(passed)

    running = tuple(jnp.zeros((1, tile), jnp.float32) for _ in range(heads))
    running = visit(top, running, True)
    lax.fori_loop(0, top, lambda step, carried: visit(top - 1 - step, carried, False), running)
    out_ref[0] = jnp.transpose(acc_ref[...]).astype(jnp.bfloat16)


def attend(tops, queries, blocks, bias):
    parts, tile, width = queries.shape
    held = (len(blocks),) + blocks[0].shape
    pairs = parts * tile * held[0] * held[1] * width // HEAD_DIM // 2
    return pl.pallas_call(
        attend_kernel,
        out_shape=jax.ShapeDtypeStruct(queries.shape, jnp.bfloat16),
        grid_spec=pltpu.PrefetchScalarGridSpec(
            num_scalar_prefetch=1,
            grid=(parts,),
            in_specs=[
                pl.BlockSpec((1, tile, width), lambda c, tops: (c, 0, 0)),
                pl.BlockSpec(memory_space=pltpu.VMEM),
            ]
            + [pl.BlockSpec(memory_space=pl.ANY)] * len(blocks),
            out_specs=pl.BlockSpec((1, tile, width), lambda c, tops: (c, 0, 0)),
            scratch_shapes=[
                pltpu.VMEM((width, tile), jnp.float32),
                pltpu.VMEM(held, blocks[0].dtype),
                pltpu.SemaphoreType.DMA((len(blocks),)),
            ],
        ),
        cost_estimate=pl.CostEstimate(
            flops=pairs * 1000, bytes_accessed=len(blocks) * blocks[0].size * 2, transcendentals=pairs * 3
        ),
        compiler_params=pltpu.CompilerParams(vmem_limit_bytes=58 * 1024 * 1024),
    )(tops, queries, bias, *blocks)


def gather_blocks(own, count):
    ring = count // PAIR
    swap = [(i, i // PAIR * PAIR + (i + 1) % PAIR) for i in range(count)]
    ahead = [(i, (i + PAIR) % count) for i in range(count)]
    behind = [(j, i) for i, j in ahead]
    near = [own, lax.ppermute(own, "ep", swap)]
    far = {}
    for member in range(PAIR):
        reach = (ring - 1 + (member == 0)) // 2
        held = near[member]
        for step in range(1, reach + 1):
            held = lax.ppermute(held, "ep", ahead)
            far[step, member] = held
        held = near[member]
        for step in range(ring - 1, reach, -1):
            held = lax.ppermute(held, "ep", behind)
            far[step, member] = held
    return near + [far[step, member] for step in range(1, ring) for member in range(PAIR)]


def expand(arrived, gate_weights, up_weights):
    gate_in = jnp.einsum(
        "necm,emf->necf", arrived, gate_weights, preferred_element_type=jnp.float32
    )
    up_in = jnp.einsum("necm,emf->necf", arrived, up_weights, preferred_element_type=jnp.float32)
    return (jax.nn.silu(gate_in) * up_in).astype(jnp.bfloat16)


def contract(hidden, down_weights):
    return jnp.einsum("necf,efm->necm", hidden, down_weights, preferred_element_type=jnp.float32)


def local(
    query_rows,
    key_rows,
    value_rows,
    key_bias,
    out_weight,
    moe_input,
    moe_gain,
    expert_pick,
    route_weight,
    w_gate,
    w_up,
    w_down,
):
    block_rows = query_rows.shape[0]
    half_rows = block_rows // 2
    ep_index = lax.axis_index("ep")
    ep_count = lax.axis_size("ep")
    own_kv = jnp.concatenate([key_rows, value_rows], axis=1)
    mirror = [(i, ep_count - 1 - i) for i in range(ep_count)]
    far_query = lax.ppermute(query_rows[half_rows:], "ep", mirror)
    blocks = gather_blocks(own_kv, ep_count)
    tops = jnp.stack(
        [2 * ep_index, 2 * (ep_count - 1 - ep_index) + 1, ep_index]
    ).astype(jnp.int32)
    near, far = attend(
        tops, jnp.stack([query_rows[:half_rows], far_query]), blocks, key_bias
    )
    attended = jnp.concatenate([near, lax.ppermute(far, "ep", mirror)], axis=0)
    mixer_out = lax.psum_scatter(
        jnp.dot(attended, out_weight, preferred_element_type=jnp.float32).astype(jnp.bfloat16),
        "tp",
        scatter_dimension=0,
        tiled=True,
    )
    token_count = moe_input.shape[0]
    widened = moe_input.astype(jnp.float32)
    normed = (
        widened
        * lax.rsqrt(jnp.mean(widened * widened, axis=1, keepdims=True) + norm_eps)
        * moe_gain
    ).astype(jnp.bfloat16)
    local_experts = w_gate.shape[0]
    expert_total = local_experts * ep_count
    capacity = GROUPS * token_count // expert_total
    picks = expert_pick.reshape(-1)
    matches = (picks[:, None] == jnp.arange(expert_total, dtype=jnp.int32)[None, :]).astype(
        jnp.int32
    )
    ranks = jnp.sum((jnp.cumsum(matches, axis=0) - matches) * matches, axis=1)
    slots = picks * capacity + ranks
    owners = jnp.arange(picks.shape[0], dtype=jnp.int32) // TOPK
    table = jnp.full((expert_total * capacity,), token_count, jnp.int32).at[slots].set(owners)
    padded = jnp.concatenate([normed, jnp.zeros((1, normed.shape[1]), jnp.bfloat16)], axis=0)
    outgoing = padded[table].reshape(ep_count, local_experts, capacity, normed.shape[1])
    outgoing = lax.optimization_barrier((outgoing, far_query, *blocks))[0]
    arrived = lax.all_to_all(outgoing, "ep", split_axis=0, concat_axis=0, tiled=True)
    gate_all, up_all, down_all = (
        lax.all_gather(w_gate, "tp", axis=2, tiled=True),
        lax.all_gather(w_up, "tp", axis=2, tiled=True),
        lax.all_gather(w_down, "tp", axis=1, tiled=True),
    )
    served = contract(expand(arrived, gate_all, up_all), down_all).astype(jnp.bfloat16)
    returned = lax.all_to_all(served, "ep", split_axis=0, concat_axis=0, tiled=True)
    flat = returned.reshape(expert_total * capacity, returned.shape[3])
    chosen = flat[slots].reshape(token_count, TOPK, flat.shape[1]).astype(jnp.float32)
    routed_out = jnp.sum(chosen * route_weight[:, :, None], axis=1).astype(jnp.bfloat16)
    return (mixer_out, routed_out)


MESH = pl.DeviceIdType.MESH
CHUNKS = 8
AHEAD = 3


def remote(src, dst, send, recv, device):
    return pltpu.make_async_remote_copy(
        src_ref=src,
        dst_ref=dst,
        send_sem=send,
        recv_sem=recv,
        device_id=device,
        device_id_type=MESH,
    )


def split_parts(values):
    high = values.astype(jnp.bfloat16).astype(jnp.float32)
    rest = values - high
    middle = rest.astype(jnp.bfloat16).astype(jnp.float32)
    return high, middle, rest - middle


def fused_kernel(
    q_hbm,
    k_hbm,
    v_hbm,
    bias_hbm,
    out_weight_ref,
    moe_hbm,
    gain_hbm,
    pick_hbm,
    route_hbm,
    gate_ref,
    up_ref,
    down_ref,
    mixer_ref,
    routed_ref,
    q_ref,
    k_ref,
    v_ref,
    bias_ref,
    moe_ref,
    gain_ref,
    pick_ref,
    route_ref,
    q_send,
    q_recv,
    kv_send,
    kv_recv,
    keys,
    scores_buf,
    won,
    weights,
    acc,
    att_send,
    att_recv,
    project,
    mix_send,
    mix_recv,
    rows_send,
    rows_recv,
    placed,
    gate_all,
    up_all,
    down_all,
    hidden,
    part_send,
    part_recv,
    part_own,
    back_send,
    back_recv,
    local_sem,
    over_send,
    over_recv,
    die_send,
    die_recv,
    pass_send,
    pass_recv,
    project_send,
    project_recv,
    q_out,
    q_in,
    kv_out,
    kv_pass,
    kv_in,
    rows_out,
    rows_pass,
    rows_in,
    att_out,
    att_in,
    mix_out,
    mix_in,
    part_out,
    part_in,
    back_out,
    back_in,
    fetch_sem,
):
    ep_count = q_recv.shape[0]
    lines = ep_count // PAIR
    e, t = lax.axis_index("ep"), lax.axis_index("tp")
    z, y = lax.div(e, PAIR), lax.rem(e, PAIR)
    chip, core = lax.div(t, PAIR), lax.rem(t, PAIR)
    die = PAIR * chip + 1 - core
    over = PAIR * (1 - chip) + core
    across = PAIR * (1 - chip) + 1 - core
    side = PAIR * z + 1 - y
    block_rows, width = q_ref.shape
    half = block_rows // PAIR
    quarter = half // PAIR
    tokens, model = moe_ref.shape
    slots = rows_send.shape[1]
    shard = gate_ref.shape[2]
    span = model // CHUNKS

    upper = lax.div(z, PAIR)
    inner = lax.rem(z + upper, PAIR)

    def nearest(order):
        away = (1 + 2 * inner, 2 - inner, 3 - inner)[order]
        return lax.rem(z + away + upper * (2 * lines - 2 * away), lines)

    def rows_target(order):
        away = (1 + 2 * inner, 2, 3 - 2 * inner)[order]
        return lax.rem(z + away + upper * (2 * lines - 2 * away), lines)

    fetches = [
        pltpu.make_async_copy(src, dst, fetch_sem.at[i])
        for i, (src, dst) in enumerate(
            (
                (k_hbm, k_ref),
                (v_hbm, v_ref),
                (q_hbm, q_ref),
                (moe_hbm, moe_ref),
                (gain_hbm, gain_ref),
                (pick_hbm, pick_ref),
                (route_hbm, route_ref),
                (bias_hbm, bias_ref),
            )
        )
    ]
    for copy in fetches:
        copy.start()

    barrier = pltpu.get_barrier_semaphore()
    for step in range(1, ep_count):
        for other in range(PAIR):
            pl.semaphore_signal(
                barrier,
                inc=1,
                device_id=(lax.rem(e + step, ep_count), PAIR * chip + other),
                device_id_type=MESH,
            )
    for other in (die, over):
        pl.semaphore_signal(barrier, inc=1, device_id=(e, other), device_id_type=MESH)

    pieces = []
    own_rows = pl.ds(pl.multiple_of(t * shard, shard), shard)
    pieces.append((gate_ref.at[0], gate_all.at[t]))
    pieces.append((up_ref.at[0], up_all.at[t]))
    for chunk in range(CHUNKS):
        pieces.append(
            (
                down_ref.at[0, :, chunk * span : (chunk + 1) * span],
                down_all.at[chunk, own_rows, :],
            )
        )

    def held(index, owner):
        if index == 0:
            return gate_all.at[owner]
        if index == 1:
            return up_all.at[owner]
        rows = pl.ds(pl.multiple_of(owner * shard, shard), shard)
        return down_all.at[index - 2, rows, :]

    project_rows = pl.ds(pl.multiple_of(core * width, width), width)
    die_rows = pl.ds(pl.multiple_of((1 - core) * width, width), width)
    locals_ = [
        pltpu.make_async_copy(src, dst, local_sem) for src, dst in pieces
    ]
    locals_.append(
        pltpu.make_async_copy(out_weight_ref, project.at[project_rows, :], local_sem)
    )
    for copy in locals_:
        copy.start()

    pl.semaphore_wait(barrier, PAIR * (ep_count - 1) + 2)

    for i, (src, dst) in enumerate(pieces):
        remote(src, dst, over_send, over_recv.at[i], (e, over)).start()

    for copy in fetches:
        copy.wait()
    keys_turned = jnp.transpose(k_ref[...].astype(jnp.float32)).astype(jnp.bfloat16)
    values_turned = jnp.transpose(v_ref[...].astype(jnp.float32)).astype(jnp.bfloat16)
    for h in range(lines):
        span_h = slice(h * HEAD_DIM, (h + 1) * HEAD_DIM)
        kv_send[h, :HEAD_DIM, :] = keys_turned[span_h, :]
        kv_send[h, HEAD_DIM:, :] = values_turned[span_h, :]
    q_turned = jnp.transpose(q_ref[...].astype(jnp.float32) * HEAD_DIM ** (-0.5))
    for h in range(lines):
        q_send[h] = q_turned[h * HEAD_DIM : (h + 1) * HEAD_DIM, :].astype(jnp.bfloat16)
    copy = remote(kv_send.at[z], kv_recv.at[e], kv_pass, kv_in.at[e], (side, t))
    copy.start()

    def send_queries(head, column):
        lanes = pl.ds(pl.multiple_of(lax.rem(column + e, PAIR) * half, half), half)
        return remote(
            q_send.at[head, :, lanes],
            q_recv.at[e, :HEAD_DIM, :],
            q_out,
            q_in.at[e],
            (PAIR * head + column, t),
        )

    for order in range(lines - 1):
        there = nearest(order)
        copies = [
            remote(
                kv_send.at[there], kv_recv.at[e], kv_out, kv_in.at[e], (PAIR * there + y, t)
            )
        ]
        copies += [send_queries(there, column) for column in range(PAIR)]
        for copy in copies:
            copy.start()
    send_queries(z, 1 - y).start()
    kv_recv[e] = kv_send[z]
    ones_at = lax.broadcasted_iota(jnp.int32, (HEAD_DIM, half), 0) < 3
    ones_rows = jnp.where(ones_at, 1.0, 0.0).astype(jnp.bfloat16)
    for i in range(ep_count):
        q_recv[i, HEAD_DIM:, :] = ones_rows
    own_lanes = pl.ds(pl.multiple_of(lax.rem(y + e, PAIR) * half, half), half)
    q_recv[e, :HEAD_DIM, :] = q_send[z, :, own_lanes]

    for i, (src, dst) in enumerate(pieces):
        remote(src, dst, die_send, die_recv.at[i], (e, die)).start()
    give_project = remote(
        out_weight_ref, project.at[project_rows, :], project_send, project_recv, (e, die)
    )
    give_project.start()

    widened = moe_ref[...].astype(jnp.float32)
    normed = (
        widened
        * lax.rsqrt(jnp.mean(widened * widened, axis=1, keepdims=True) + norm_eps)
        * gain_ref[...]
    ).astype(jnp.bfloat16)
    group_row = lax.shift_right_logical(pick_ref[0:1, :], 1)
    groups = lines
    group_at = lax.broadcasted_iota(jnp.int32, (8, tokens), 0)
    chosen = (group_at == group_row).astype(jnp.float32)
    earlier = (
        lax.broadcasted_iota(jnp.int32, (tokens, tokens), 0)
        < lax.broadcasted_iota(jnp.int32, (tokens, tokens), 1)
    ).astype(jnp.float32)
    ranks = jnp.dot(
        chosen.astype(jnp.bfloat16),
        earlier.astype(jnp.bfloat16),
        preferred_element_type=jnp.float32,
    )
    slot_row = jnp.sum(
        chosen * (ranks + group_at.astype(jnp.float32) * slots), axis=0, keepdims=True
    )
    slot_at = lax.broadcasted_iota(jnp.int32, (groups * slots, tokens), 0)
    picked = (slot_at == slot_row.astype(jnp.int32)).astype(jnp.float32)
    placed[...] = jnp.transpose(picked).astype(jnp.bfloat16)
    first_low = (pick_ref[0:1, :] & 1) == 0
    low_row = jnp.where(first_low, route_ref[0:1, :], route_ref[1:2, :])
    high_row = jnp.where(first_low, route_ref[1:2, :], route_ref[0:1, :])
    low = split_parts(jnp.sum(picked * low_row, axis=1, keepdims=True))
    high = split_parts(jnp.sum(picked * high_row, axis=1, keepdims=True))
    lane = lax.broadcasted_iota(jnp.int32, (groups * slots, 128), 1)
    shares = jnp.zeros((groups * slots, 128), jnp.float32)
    for i, part in enumerate(low + high):
        shares = jnp.where(lane == i, part, shares)
    rows_send[:, :, model:] = shares.astype(jnp.bfloat16).reshape(groups, slots, 128)
    picked = picked.astype(jnp.bfloat16)
    for first in range(0, model, span):
        rows_send[:, :, first : first + span] = (
            jnp.dot(picked, normed[:, first : first + span], preferred_element_type=jnp.float32)
            .astype(jnp.bfloat16)
            .reshape(groups, slots, span)
        )
    home = y * lines + z
    rows_recv[home] = rows_send[z]

    def send_rows(order):
        there = rows_target(order)
        return remote(
            rows_send.at[there],
            rows_recv.at[home],
            rows_out,
            rows_in.at[home],
            (PAIR * there + y, t),
        )

    for order in range(lines - 1):
        send_rows(order).start()

    def send_own_rows():
        return remote(
            rows_send.at[z], rows_recv.at[home], rows_pass, rows_in.at[home], (side, t)
        )

    def arrived_keys(source):
        arrived = kv_recv.at[source]
        return remote(arrived, arrived, kv_pass, kv_in.at[source], (side, t))

    def pass_keys(pair):
        @pl.when(pair != z)
        def _():
            copy = arrived_keys(PAIR * pair + y)
            copy.wait_recv()
            copy.start()

    head_at = lax.broadcasted_iota(jnp.int32, (lines, block_rows), 0)
    aug_at = lax.broadcasted_iota(jnp.int32, (HEAD_DIM, block_rows), 0)

    def ready(i):
        @pl.when(i != e)
        def _():
            arrived = q_recv.at[i, :HEAD_DIM, :]
            remote(arrived, arrived, q_out, q_in.at[i], (side, t)).wait_recv()

        rows = pl.ds(pl.multiple_of(i * block_rows, block_rows), block_rows)
        bias = jnp.sum(
            jnp.where(head_at == z, bias_ref[:, rows], 0.0), axis=0, keepdims=True
        )
        extra = jnp.zeros((HEAD_DIM, block_rows), jnp.float32)
        for place, part in enumerate(split_parts(bias)):
            extra = jnp.where(aug_at == place, part, extra)
        stacked = jnp.concatenate([kv_recv[i, :HEAD_DIM, :].astype(jnp.float32), extra], axis=0)
        keys[rows, :] = jnp.transpose(stacked).astype(jnp.bfloat16)

    key_at = lax.broadcasted_iota(jnp.int32, (half, half), 0)
    query_at = lax.broadcasted_iota(jnp.int32, (half, half), 1)
    later = jnp.where(key_at < query_at, 1.0, 0.0).astype(jnp.bfloat16)

    def score(block, queries):
        for sub in range(PAIR):
            rows = pl.ds(pl.multiple_of(block * block_rows + sub * half, half), half)
            scores_buf[sub] = jnp.dot(keys[rows, :], queries, preferred_element_type=jnp.float32)

    def gather_values(block):
        acc[...] += jnp.dot(
            kv_recv[block, HEAD_DIM:, :], weights[...], preferred_element_type=jnp.float32
        )

    def visit(following, queries, running, place):
        firsts, afters = {}, {}
        for sub in range(PAIR - 1, -1, -1):
            scores = scores_buf[sub]
            lost = jnp.maximum(scores, jnp.log(1.0 + jnp.exp(jnp.minimum(scores, 80.0))))
            won[sub] = scores - lost
            if place is not None:
                lost = jnp.where(key_at - query_at < (place - sub) * half, lost, 0.0)
            lost = lost.astype(jnp.bfloat16)
            firsts[sub] = lost[0:1, :].astype(jnp.float32)
            afters[sub] = jnp.dot(later, lost, preferred_element_type=jnp.float32)
        score(following, queries)
        for sub in range(PAIR - 1, -1, -1):
            weight = jnp.exp(won[sub] - (afters[sub] + running))
            if place is not None:
                weight = jnp.where(key_at - query_at < (place - sub) * half, weight, 0.0)
            weights[sub * half : (sub + 1) * half, :] = weight.astype(jnp.bfloat16)
            running = running + afters[sub][0:1, :] + firsts[sub]
        return running

    def send_attended(i, other):
        place = lax.rem(y + i, PAIR)
        return remote(
            att_send.at[i, :, other * quarter : (other + 1) * quarter],
            att_recv.at[
                pl.ds(pl.multiple_of(core * width + z * HEAD_DIM, HEAD_DIM), HEAD_DIM),
                pl.ds(pl.multiple_of(place * quarter, quarter), quarter),
            ],
            att_out,
            att_in,
            (i, PAIR * chip + other),
        )

    def wait_rows(place):
        arrived = rows_recv.at[place]
        remote(arrived, arrived, rows_out, rows_in.at[place], (side, t)).wait_recv()

    def pass_rows(order):
        there = nearest(order)
        place = y * lines + there
        arrived = rows_recv.at[place]
        return remote(arrived, arrived, rows_pass, rows_in.at[place], (side, t))

    def pass_rows_on(order):
        wait_rows(y * lines + nearest(order))
        pass_rows(order).start()

    def pass_copy(index):
        arrived = held(index, over)
        return remote(arrived, arrived, pass_send, pass_recv.at[index], (e, die))

    def pass_on(index):
        arrived = held(index, over)
        remote(arrived, arrived, over_send, over_recv.at[index], (e, over)).wait_recv()
        pass_copy(index).start()

    def one_tile(i, _):
        pair = lax.div(i, PAIR)

        @pl.when(lax.rem(i, PAIR) == 0)
        def _():
            arrived_keys(i + 1 - y).wait_recv()
            ready(i)
            ready(i + 1)

        @pl.when(jnp.logical_and(lax.rem(i, PAIR) == 1, i < ep_count - 1))
        def _():
            pass_keys(pair + 1)

        @pl.when(i == PAIR)
        def _():
            send_own_rows().start()

        @pl.when(i == ep_count - PAIR - 1)
        def _():
            pass_on(0)

        for order in range(lines - 2):

            @pl.when(jnp.logical_and(i == lines + PAIR * order, inner * order == 0))
            def _():
                pass_rows_on(order)

        place = lax.rem(y + i, PAIR)
        queries = q_recv[i]
        acc[...] = jnp.zeros_like(acc)
        score(i, queries)
        running = visit(
            jnp.maximum(i - 1, 0), queries, jnp.zeros((1, half), jnp.float32), place
        )

        def next_block(s, running):
            gather_values(i - s)
            return visit(jnp.maximum(i - 2 - s, 0), queries, running, None)

        lax.fori_loop(0, i, next_block, running)
        gather_values(0)
        att_send[i] = acc[...].astype(jnp.bfloat16)
        for other in range(PAIR):
            here = jnp.logical_and(i == e, core == other)

            @pl.when(jnp.logical_not(here))
            def _():
                send_attended(i, other).start()

            @pl.when(here)
            def _():
                att_recv[
                    pl.ds(pl.multiple_of(core * width + z * HEAD_DIM, HEAD_DIM), HEAD_DIM),
                    pl.ds(pl.multiple_of(place * quarter, quarter), quarter),
                ] = att_send[i, :, other * quarter : (other + 1) * quarter]

        return 0

    pass_keys(0)
    lax.fori_loop(0, ep_count, one_tile, 0)

    def wait_die(index):
        arrived = held(index, die)
        remote(arrived, arrived, die_send, die_recv.at[index], (e, die)).wait_recv()

    def wait_across(index):
        arrived = held(index, across)
        remote(arrived, arrived, pass_send, pass_recv.at[index], (e, die)).wait_recv()

    def serve(owner, first, count):
        hidden_lanes = pl.ds(pl.multiple_of(owner * shard, shard), shard)
        rows = rows_recv[pl.ds(first, count), :, :model].reshape(count * slots, model)
        gate_in = jnp.dot(rows, gate_all[owner], preferred_element_type=jnp.float32)
        up_in = jnp.dot(rows, up_all[owner], preferred_element_type=jnp.float32)
        target = pl.ds(pl.multiple_of(first * slots, slots), count * slots)
        hidden[target, hidden_lanes] = (gate_in / (1.0 + jnp.exp(-gate_in)) * up_in).astype(
            jnp.bfloat16
        )

    def serve_all(first, count, start, stop):
        def one(k, _):
            owner = PAIR * lax.rem(chip + lax.div(k, PAIR), PAIR) + lax.rem(core + k, PAIR)
            serve(owner, first, count)
            return 0

        lax.fori_loop(start, stop, one, 0)

    own_first = y * lines
    early = (1 - y) * lines + PAIR * upper
    late = (1 - y) * lines + PAIR * (1 - upper)

    @pl.when(inner == 1)
    def _():
        pass_rows_on(1)

    pass_rows_on(lines - 2)
    pass_on(1)
    pltpu.make_async_copy(gate_all, gate_all, local_sem).wait()
    wait_die(0)
    wait_die(1)
    for i in range(PAIR):
        wait_rows(early + i)
    serve_all(early, PAIR, 0, PAIR)
    serve_all(own_first, lines, 0, PAIR)
    pass_on(2)
    serve_all(early, PAIR, PAIR, PAIR + 1)
    wait_across(0)
    wait_across(1)
    serve_all(early, PAIR, PAIR + 1, 2 * PAIR)

    def mix():
        pieces_in = att_recv.at[: PAIR * width - HEAD_DIM // PAIR, :]
        remote(pieces_in, pieces_in, att_out, att_in, (side, t)).wait_recv()
        arrived = project.at[die_rows, :]
        remote(arrived, arrived, project_send, project_recv, (e, die)).wait_recv()

        def mixed(which):
            lanes = pl.ds(pl.multiple_of(which * quarter, quarter), quarter)
            attended = jnp.transpose(att_recv[:, lanes].astype(jnp.float32)).astype(jnp.bfloat16)
            return jnp.dot(attended, project[...], preferred_element_type=jnp.float32).astype(
                jnp.bfloat16
            )

        mix_send[...] = mixed(1 - chip)
        remote(mix_send, mix_recv, mix_out, mix_in, (e, over)).start()
        mixer_ref[...] = mixed(chip)

    def share_here(count):
        lane = lax.broadcasted_iota(jnp.int32, (count * slots, 128), 1)
        return jnp.logical_and(lane >= 3 * y, lane < 3 * y + 3)

    def contract(chunk, first, count):
        rows = pl.ds(pl.multiple_of(first * slots, slots), count * slots)
        shares = rows_recv[pl.ds(first, count), :, model:].reshape(count * slots, 128)
        share = jnp.sum(
            jnp.where(share_here(count), shares.astype(jnp.float32), 0.0), axis=1, keepdims=True
        )
        return (
            jnp.dot(hidden[rows, :], down_all[chunk], preferred_element_type=jnp.float32) * share
        )

    def part_copy(chunk, place):
        rows = pl.ds(pl.multiple_of(place * PAIR * slots, PAIR * slots), PAIR * slots)
        return remote(
            part_send.at[chunk, rows],
            part_recv.at[chunk, rows],
            part_out,
            part_in.at[chunk],
            (side, t),
        )

    def send_part(chunk, first, place):
        rows = pl.ds(pl.multiple_of(place * PAIR * slots, PAIR * slots), PAIR * slots)
        part_send[chunk, rows, :] = contract(chunk, first, PAIR).astype(jnp.bfloat16)
        part_copy(chunk, place).start()

    def give_back(chunk):
        arrived = part_recv.at[chunk]
        remote(arrived, arrived, part_out, part_in.at[chunk], (side, t)).wait_recv()
        total = part_own[chunk] + part_recv[chunk].astype(jnp.float32)
        back_send[chunk] = total.astype(jnp.bfloat16).reshape(lines, slots, span)
        for order in range(lines - 2, -1, -1):
            there = nearest(order)
            copy = remote(
                back_send.at[chunk, there],
                back_recv.at[chunk, z],
                back_out,
                back_in.at[chunk],
                (PAIR * there + y, t),
            )
            copy.start()
        back_recv[chunk, z] = back_send[chunk, z]

    def send_early(chunk):
        wait_die(2 + chunk)
        wait_across(2 + chunk)
        send_part(chunk, early, upper)

    def pass_down(chunk):
        if chunk < CHUNKS:
            pass_on(2 + chunk)

    for chunk in range(AHEAD):
        send_early(chunk)
        if chunk == 0:
            mix()
        pass_down(chunk + 1)
    for i in range(PAIR):
        wait_rows(late + i)
    serve_all(late, PAIR, 0, 2 * PAIR)
    for chunk in range(AHEAD):
        send_part(chunk, late, 1 - upper)
    serve_all(own_first, lines, PAIR, 2 * PAIR)
    for chunk in range(CHUNKS):
        if chunk >= AHEAD:
            send_early(chunk)
            send_part(chunk, late, 1 - upper)
            pass_down(chunk + 1)
        part_own[chunk] = contract(chunk, own_first, lines)
        if chunk > 0:
            give_back(chunk - 1)
    give_back(CHUNKS - 1)

    remote(mix_send, mix_recv, mix_out, mix_in, (e, over)).wait_recv()
    mixer_ref[...] = (
        mixer_ref[...].astype(jnp.float32) + mix_recv[...].astype(jnp.float32)
    ).astype(jnp.bfloat16)

    for chunk in range(CHUNKS):
        arrived = back_recv.at[chunk, : lines - 1]
        remote(arrived, arrived, back_out, back_in.at[chunk], (side, t)).wait_recv()
        routed_ref[:, chunk * span : (chunk + 1) * span] = jnp.dot(
            placed[...],
            back_recv[chunk].reshape(groups * slots, span),
            preferred_element_type=jnp.float32,
        ).astype(jnp.bfloat16)

    give_project.wait_send()
    weights_sent = gate_all.at[: PAIR + 1]
    for sem in (over_send, die_send, pass_send):
        remote(weights_sent, weights_sent, sem, over_recv.at[0], (e, die)).wait_send()
    for sent, sem, incoming in (
        (kv_recv.at[: lines - 1], kv_out, kv_in.at[0]),
        (kv_recv.at[:lines], kv_pass, kv_in.at[0]),
        (q_recv.at[: ep_count - 1, :HEAD_DIM, :], q_out, q_in.at[0]),
        (rows_recv.at[: lines - 1], rows_out, rows_in.at[0]),
        (rows_recv.at[:lines], rows_pass, rows_in.at[0]),
        (att_recv.at[: PAIR * width - HEAD_DIM // PAIR, :], att_out, att_in),
        (mix_send, mix_out, mix_in),
        (part_send, part_out, part_in.at[0]),
        (back_send.at[:, : lines - 1], back_out, back_in.at[0]),
    ):
        remote(sent, sent, sem, incoming, (side, t)).wait_send()


def fused(
    query_rows,
    key_rows,
    value_rows,
    key_bias,
    out_weight,
    moe_input,
    moe_gain,
    expert_pick,
    route_weight,
    w_gate,
    w_up,
    w_down,
):
    ep_count = lax.axis_size("ep")
    tp_count = lax.axis_size("tp")
    lines = ep_count // PAIR
    block_rows, width = query_rows.shape
    half = block_rows // PAIR
    quarter = half // PAIR
    tokens, model = moe_input.shape
    slots = GROUPS * tokens // (w_gate.shape[0] * ep_count)
    shard = w_gate.shape[2]
    span = model // CHUNKS
    bf16, f32 = jnp.bfloat16, jnp.float32
    dma = pltpu.SemaphoreType.DMA
    vmem = pltpu.VMEM
    operands = (
        query_rows,
        key_rows,
        value_rows,
        jnp.transpose(key_bias),
        out_weight,
        moe_input,
        moe_gain.reshape(1, model),
        jnp.transpose(expert_pick),
        jnp.transpose(route_weight),
        w_gate,
        w_up,
        w_down,
    )
    fetched = operands[:4] + operands[5:9]
    scratch = [vmem(array.shape, array.dtype) for array in fetched] + [
        vmem((lines, HEAD_DIM, block_rows), bf16),
        vmem((ep_count, 2 * HEAD_DIM, half), bf16),
        vmem((lines, 2 * HEAD_DIM, block_rows), bf16),
        vmem((ep_count, 2 * HEAD_DIM, block_rows), bf16),
        vmem((ep_count * block_rows, 2 * HEAD_DIM), bf16),
        vmem((PAIR, half, half), f32),
        vmem((PAIR, half, half), f32),
        vmem((block_rows, half), bf16),
        vmem((HEAD_DIM, half), f32),
        vmem((ep_count, HEAD_DIM, half), bf16),
        vmem((PAIR * width, half), bf16),
        vmem((PAIR * width, model), bf16),
        vmem((quarter, model), bf16),
        vmem((quarter, model), bf16),
        vmem((lines, slots, model + 128), bf16),
        vmem((ep_count, slots, model + 128), bf16),
        vmem((tokens, lines * slots), bf16),
        vmem((tp_count, model, shard), bf16),
        vmem((tp_count, model, shard), bf16),
        vmem((CHUNKS, tp_count * shard, span), bf16),
        vmem((ep_count * slots, tp_count * shard), bf16),
        vmem((CHUNKS, lines * slots, span), bf16),
        vmem((CHUNKS, lines * slots, span), bf16),
        vmem((CHUNKS, lines * slots, span), f32),
        vmem((CHUNKS, lines, slots, span), bf16),
        vmem((CHUNKS, lines, slots, span), bf16),
        dma,
        dma,
        dma((CHUNKS + 2,)),
        dma,
        dma((CHUNKS + 2,)),
        dma,
        dma((CHUNKS + 2,)),
        dma,
        dma,
        dma,
        dma((ep_count,)),
        dma,
        dma,
        dma((ep_count,)),
        dma,
        dma,
        dma((ep_count,)),
        dma,
        dma,
        dma,
        dma,
        dma,
        dma((CHUNKS,)),
        dma,
        dma((CHUNKS,)),
        dma((len(fetched),)),
    ]
    in_hbm = pl.BlockSpec(memory_space=pltpu.HBM)
    in_vmem = pl.BlockSpec(memory_space=pltpu.VMEM)
    return pl.pallas_call(
        fused_kernel,
        out_shape=(
            vmem((quarter, model), bf16),
            vmem((tokens, model), bf16),
        ),
        in_specs=[in_hbm] * len(operands),
        out_specs=(in_vmem, in_vmem),
        scratch_shapes=scratch,
        compiler_params=pltpu.CompilerParams(
            collective_id=0, has_side_effects=True, vmem_limit_bytes=58 * 1024 * 1024
        ),
    )(*operands)


def fits(query_rows, w_gate):
    ep_count = lax.axis_size("ep")
    return (
        lax.axis_size("tp") == PAIR * PAIR
        and TOPK == PAIR
        and w_gate.shape[0] == 1
        and ep_count == GROUPS * TOPK
        and query_rows.shape[1] == GROUPS * HEAD_DIM == w_gate.shape[2]
    )


def step(*args):
    return (fused if fits(args[0], args[9]) else local)(*args)


def solution(mesh):
    placed = (
        P("ep", "tp"),
        P("ep", "tp"),
        P("ep", "tp"),
        P(None, "tp"),
        P("tp", None),
        P(("ep", "tp"), None),
        P(),
        P(("ep", "tp"), None),
        P(("ep", "tp"), None),
        P("ep", None, "tp"),
        P("ep", None, "tp"),
        P("ep", "tp", None),
    )
    return jax.shard_map(
        step,
        mesh=mesh,
        in_specs=placed,
        out_specs=(P(("ep", "tp"), None), P(("ep", "tp"), None)),
        check_vma=False,
    )
```
